512 devices in a mesh: sp: 64 (over z, y), fs: 4 (over x), tp: 2 (over core).
Axes of the slice: x: 4, y: 8, z: 8, core: 2. Of those that a mesh axis runs over, the one named last changes fastest.
Arguments:
- tokens: bfloat16 [16384, 2048], P(('sp', 'fs', 'tp')), may hold values from -20 to 20
- norm_gain: float32 [2048], replicated, may hold values from 0.1 to 1.9
- query_weight: bfloat16 [2048, 1024], P(None, ('fs', 'tp')), may hold values from -0.5 to 0.5
- w_key: bfloat16 [2048, 256], P(None, 'tp'), may hold values from -0.5 to 0.5
- w_value: bfloat16 [2048, 256], P(None, 'tp'), may hold values from -0.125 to 0.125
- w_input: bfloat16 [2048, 1024], P(None, ('fs', 'tp')), may hold values from -0.125 to 0.125
- w_gate: bfloat16 [2048, 1024], P(None, ('fs', 'tp')), may hold values from -0.125 to 0.125
- conv_kernel: float32 [4, 1024], P(None, ('fs', 'tp')), may hold values from -3 to 3
- w_recur: bfloat16 [16, 64, 64], P(('fs', 'tp')), may hold values from -0.75 to 0.75
- w_admit: bfloat16 [16, 64, 64], P(('fs', 'tp')), may hold values from -0.75 to 0.75
- decay_param: float32 [1024], P(('fs', 'tp')), may hold values from 4 to 17
- decay_scale: float32 [16384, 1024], P('sp', ('fs', 'tp')), may hold values from 0.5 to 229376
- init_state: float32 [1024], P(('fs', 'tp')), may hold values from -6 to 6
- diff_lambda: float32 [8], P(('fs', 'tp')), may hold values from 0.3 to 0.8
- head_gain: float32 [128], replicated, may hold values from 0.1 to 1.9
- w_out_lru: bfloat16 [1024, 2048], P(('fs', 'tp')), may hold values from -1 to 1
- w_out_attn: bfloat16 [1024, 2048], P(('fs', 'tp')), may hold values from -0.1875 to 0.1875
Outputs:
- mixed: bfloat16 [16384, 2048], P(('sp', 'fs', 'tp'))
The draws below stay inside these ranges and needn't reach their ends.
All inputs are finite; a program needn't handle non-finite values.
Results may differ from the reference program's by a relative error of at most 0.019.
Values may be sent and summed in bfloat16 or wider, within the bound.
No kernel may reach another device: no remote copies, remote signals or barrier semaphores. Data moves between devices by JAX's collectives and lax.ppermute only.
A program may use at most 64 MiB of HBM per device.

```python
import math
import jax
import jax.numpy as jnp
from jax import lax

D = 2048
W = 1024
BD = 64
BLOCKS = 16
HEADS = 8
KV_HEADS = 2
E = 64
V = 128
CONV = 4
TOK_DEV = 256
TOKEN_SPAN = 16384
N_FS = 4
N_TP = 2


def channel_rates(key):
    base = jax.random.fold_in(key, 11)
    key_pick, key_slow, key_fast = jax.random.split(base, 3)
    share = 0.5
    slow = jax.random.uniform(key_pick, (W,), jnp.float32) < share
    slow_rate = jnp.exp(jax.random.uniform(key_slow, (W,), jnp.float32, jnp.log(0.05), jnp.log(0.25))) / (4.0 * TOKEN_SPAN)
    fast_rate = jnp.exp(jax.random.uniform(key_fast, (W,), jnp.float32, jnp.log(0.01), jnp.log(0.033))) / 4.0
    return jnp.where(slow, slow_rate, fast_rate)


def draw_decay_param(key, part):
    rates = channel_rates(key)
    return jnp.clip(-jnp.log(jnp.expm1(rates)), 4.0, 17.0)


def draw_decay_scale(key, part):
    rates = channel_rates(key)
    base = jax.random.fold_in(key, 23)
    key_block, key_spot, key_loss = jax.random.split(base, 3)
    block_count = TOKEN_SPAN // TOK_DEV
    factor = jnp.exp(jax.random.uniform(key_block, (block_count, W), jnp.float32, jnp.log(0.5), jnp.log(2.0)))
    dispersed_numbers = jnp.repeat(factor, TOK_DEV, axis=0)
    spots = jax.random.randint(key_spot, (2,), 0, TOKEN_SPAN)
    losses = jax.random.uniform(key_loss, (2, W), jnp.float32, 0.2, 0.5)
    stride_displacements = -jnp.log1p(-losses) / (4.0 * rates[None, :])
    selected_members = (jnp.arange(TOKEN_SPAN)[:, None] == spots[None, :]).astype(jnp.float32)
    clustered_numbers = jnp.dot(selected_members, stride_displacements)
    masked_elements = jnp.sum(selected_members, axis=1) > 0.0
    return jnp.clip(jnp.where(masked_elements[:, None], clustered_numbers, dispersed_numbers), 0.5, 14.0 * TOKEN_SPAN)


def first_block_lean(key, values, row_scale):
    lean_key = jax.random.fold_in(key, 43)
    common = jax.random.normal(lean_key, (D,), jnp.float32)
    common = common / jnp.sqrt(jnp.sum(common * common))
    leaning = (jnp.arange(TOKEN_SPAN) < TOK_DEV)[:, None]
    blended = 0.71 * values + 0.7 * D ** 0.5 * row_scale * common[None, :]
    return jnp.where(leaning, blended, values)


def draw_tokens(key, part):
    base = jax.random.fold_in(key, 41)
    key_body, key_rows = jax.random.split(base, 2)
    row_scale = jnp.exp(jax.random.uniform(key_rows, (TOKEN_SPAN, 1), jnp.float32, jnp.log(0.3), jnp.log(3.0)))
    values = jax.random.normal(key_body, (TOKEN_SPAN, D), jnp.float32) * row_scale
    values = first_block_lean(key, values, row_scale)
    return jnp.clip(values, -20.0, 20.0).astype(jnp.bfloat16)


def draw_query_weight(key, part):
    base = jax.random.fold_in(key, 31)
    dispersed_numbers = (2.0 / D) ** 0.5
    values = jax.random.normal(base, (D, HEADS * 2 * E), jnp.float32) * dispersed_numbers
    return jnp.clip(values, -0.5, 0.5).astype(jnp.bfloat16)


def draw_w_key(key, part):
    base = jax.random.fold_in(key, 37)
    dispersed_numbers = (1.5 / D) ** 0.5
    values = jax.random.normal(base, (D, KV_HEADS * 2 * E), jnp.float32) * dispersed_numbers
    return jnp.clip(values, -0.5, 0.5).astype(jnp.bfloat16)


def block_levels(rng, dims, pieces, least, high):
    loudness = 1.0
    for axis_at, parts in pieces:
        heights = jax.random.uniform(jax.random.fold_in(jax.random.fold_in(rng, 6), axis_at), (parts,), jnp.float32, least / len(pieces), high / len(pieces))
        loudness = loudness * jnp.repeat(jnp.exp(heights), dims[axis_at] // parts).reshape((-1,) + (1,) * (len(dims) - 1 - axis_at))
    return loudness


def scatter_about(stream_key, dims, scale, most, cuts=(), kind=jnp.bfloat16):
    drawn = jax.random.normal(stream_key, dims, jnp.float32) * scale
    if len(cuts) > 0:
        drawn = block_levels(stream_key, dims, cuts, -0.22, 0.18) * drawn
    return jnp.clip(drawn, min=-most, max=most).astype(kind)


def setup_inputs(seed: int = 0) -> dict:
    arg_keys = jax.random.split(jax.random.key(seed), 18)
    return {
        "tokens": draw_tokens(jax.random.fold_in(arg_keys[17], 71), 0),
        "norm_gain": jnp.clip(1.0 + 0.18 * jax.random.normal(arg_keys[1], (D,), jnp.float32), 0.1, 1.9),
        "query_weight": draw_query_weight(jax.random.fold_in(arg_keys[17], 71), 0),
        "w_key": draw_w_key(jax.random.fold_in(arg_keys[17], 71), 0),
        "w_value": scatter_about(arg_keys[4], (D, V * KV_HEADS), D ** -0.5, 0.125, ((1, 2),)),
        "w_input": scatter_about(arg_keys[5], (D, W), D ** -0.5, 0.125, ((1, 8),)),
        "w_gate": scatter_about(arg_keys[6], (D, W), D ** -0.5, 0.125, ((1, 8),)),
        "conv_kernel": scatter_about(arg_keys[7], (CONV, W), CONV ** -0.5, 3.0, ((1, 8),), jnp.float32),
        "w_recur": scatter_about(arg_keys[8], (BLOCKS, BD, BD), BD ** -0.5, 0.75, ((0, 8),)),
        "w_admit": scatter_about(arg_keys[9], (BLOCKS, BD, BD), BD ** -0.5, 0.75, ((0, 8),)),
        "decay_param": draw_decay_param(jax.random.fold_in(arg_keys[17], 71), 0),
        "decay_scale": draw_decay_scale(jax.random.fold_in(arg_keys[17], 71), 0),
        "init_state": scatter_about(arg_keys[12], (W,), 1.0, 6.0, ((0, 8),), jnp.float32),
        "diff_lambda": jnp.clip(0.3 + 0.5 * jax.random.uniform(arg_keys[13], (HEADS,), jnp.float32) ** block_levels(arg_keys[13], (HEADS,), ((0, 8),), -0.2, 0.2), 0.3, 0.8),
        "head_gain": jnp.clip(1.0 + 0.18 * jax.random.normal(arg_keys[14], (V,), jnp.float32), 0.1, 1.9),
        "w_out_lru": scatter_about(arg_keys[15], (W, D), (W // 32) ** -0.5, 1.0, ((0, 8),)),
        "w_out_attn": scatter_about(arg_keys[16], (HEADS * V, D), (HEADS * V) ** -0.5, 0.1875, ((0, 8),)),
    }


gate_scale = 8.0
input_eps = 1e-06
head_eps = 1e-05

def pair_combine(earlier, later):
    decay_early, state_early = earlier
    decay_late, state_late = later
    return (decay_early * decay_late, decay_late * state_early + state_late)

def project(normed, weight):
    return jnp.dot(normed, weight, preferred_element_type=jnp.float32).astype(jnp.bfloat16)

def reference(tokens, norm_gain, query_weight, w_key, w_value, w_input, w_gate, conv_kernel, w_recur, w_admit, decay_param, decay_scale, init_state, diff_lambda, head_gain, w_out_lru, w_out_attn):
    floats = tokens.astype(jnp.float32)
    normed = (floats * lax.rsqrt(lax.optimization_barrier(jnp.mean(floats * floats, axis=1, keepdims=True)) + input_eps) * norm_gain).astype(jnp.bfloat16)
    query = project(normed, query_weight)
    keys_all = project(normed, w_key)
    values_all = project(normed, w_value)
    lru_in = project(normed, w_input)
    gate_proj = project(normed, w_gate)
    padded = jnp.concatenate([jnp.zeros((CONV - 1, W), jnp.bfloat16), lru_in], axis=0).astype(jnp.float32)
    conv_sum = jnp.zeros((TOKEN_SPAN, W), jnp.float32)
    for offset in range(CONV):
        conv_sum = conv_sum + conv_kernel[offset] * padded[offset:offset + TOKEN_SPAN]
    conv_out = conv_sum.astype(jnp.bfloat16)
    grouped = conv_out.astype(jnp.float32).reshape(TOKEN_SPAN, BLOCKS, BD)
    recur = jax.nn.sigmoid(jnp.einsum('tni,nij->tnj', grouped, w_recur.astype(jnp.float32)).reshape(TOKEN_SPAN, W))
    admit = jax.nn.sigmoid(jnp.einsum('tni,nij->tnj', grouped, w_admit.astype(jnp.float32)).reshape(TOKEN_SPAN, W))
    log_decay = -gate_scale * recur * jax.nn.softplus(-decay_param) * decay_scale
    decay = jnp.exp(log_decay)
    drive = jnp.sqrt(-jnp.expm1(2.0 * log_decay)) * admit * conv_out.astype(jnp.float32)
    drive = jnp.concatenate([drive[:1] + decay[:1] * init_state[None, :], drive[1:]], axis=0)
    _, states = lax.associative_scan(pair_combine, (decay, drive), axis=0)
    lru_out = (states * jax.nn.gelu(gate_proj.astype(jnp.float32))).astype(jnp.bfloat16)
    query_heads = query.reshape(TOKEN_SPAN, HEADS, 2, E).astype(jnp.float32)
    head_owner = (jnp.arange(HEADS) % KV_HEADS).astype(jnp.int32)
    key_heads = keys_all.reshape(TOKEN_SPAN, KV_HEADS, 2, E).astype(jnp.float32)[:, head_owner]
    value_heads = values_all.reshape(TOKEN_SPAN, KV_HEADS, V).astype(jnp.float32)[:, head_owner]
    query_rows = math.gcd(TOKEN_SPAN, 256)
    key_index = jnp.arange(TOKEN_SPAN).astype(jnp.int32)

    def attend_block(block_index):
        first_row = (block_index * query_rows).astype(jnp.int32)
        block = lax.dynamic_slice_in_dim(query_heads, first_row, query_rows, 0)
        scores = jnp.einsum('qhme,khme->hmqk', block, key_heads) * E ** (-0.5)
        query_index = first_row + jnp.arange(query_rows).astype(jnp.int32)
        visible = key_index[None, :] <= query_index[:, None]
        scores = jnp.where(visible, scores, -jnp.inf)
        peak = lax.optimization_barrier(jnp.max(scores, axis=-1, keepdims=True))
        expos = jnp.where(visible, jnp.exp(scores - peak), 0.0)
        total = lax.optimization_barrier(jnp.sum(expos, axis=-1))
        weights = lax.optimization_barrier(expos.astype(jnp.bfloat16)).astype(jnp.float32)
        heads_values = jnp.einsum('hmqk,khv->hmqv', weights, value_heads)
        lam = diff_lambda[:, None, None]
        diff = heads_values[:, 0] / total[:, 0, :, None] - lam * heads_values[:, 1] / total[:, 1, :, None]
        scaled = diff * lax.rsqrt(lax.optimization_barrier(jnp.mean(diff * diff, axis=-1, keepdims=True)) + head_eps) * head_gain
        return jnp.transpose(scaled, (1, 0, 2)).reshape(query_rows, HEADS * V).astype(jnp.bfloat16)
    attn_out = lax.map(attend_block, jnp.arange(TOKEN_SPAN // query_rows).astype(jnp.int32))
    attn_out = attn_out.reshape(TOKEN_SPAN, HEADS * V)
    group_count = N_FS * N_TP
    lru_cols = W // group_count
    head_cols = HEADS * V // group_count
    mixed = jnp.zeros((TOKEN_SPAN, D), jnp.float32)
    for group_index in range(group_count):
        low = group_index * lru_cols
        high = group_index * head_cols
        partial_sum = jnp.dot(lru_out[:, low:low + lru_cols], w_out_lru[low:low + lru_cols], preferred_element_type=jnp.float32)
        partial_sum = partial_sum + jnp.dot(attn_out[:, high:high + head_cols], w_out_attn[high:high + head_cols], preferred_element_type=jnp.float32)
        rounded = lax.optimization_barrier(partial_sum.astype(jnp.bfloat16))
        mixed = mixed + rounded.astype(jnp.float32)
    return mixed.astype(jnp.bfloat16)
```

```python
import functools

import jax
import jax.numpy as jnp
from jax import lax
from jax.experimental import pallas as pl
from jax.experimental.pallas import tpu as pltpu
from jax.sharding import Mesh
from jax.sharding import PartitionSpec as P


SP = ("sp_0", "sp_1")
SP_FS_TP = ("sp_0", "sp_1", "fs", "tp")


gate_scale = 8.0
input_eps = 1e-06
head_eps = 1e-05
far_below = -1e30
log2_e = 1.4426950408889634


def from_everyone(value, axis):
    copies = jnp.broadcast_to(value, (lax.axis_size(axis), *value.shape))
    return lax.all_to_all(copies, axis, split_axis=0, concat_axis=0, tiled=True)


def passed_along(value, axis, by):
    devices = lax.axis_size(axis)
    pairs = [(i, i + by) for i in range(devices) if 0 <= i + by < devices]
    return lax.ppermute(value, axis, pairs)


def pair_combine(earlier, later):
    decay_early, state_early = earlier
    decay_late, state_late = later
    return (decay_early * decay_late, decay_late * state_early + state_late)


def prefix_by_axis(pair, axes):
    start = (jnp.ones_like(pair[0]), jnp.zeros_like(pair[1]))
    before = start
    total = (pair[0], pair[1])
    for axis in reversed(axes):
        devices, here = (lax.axis_size(axis), lax.axis_index(axis))
        gather = lax.all_gather if axis == axes[-1] else from_everyone
        pieces = gather(jnp.stack(total), axis)
        inside, total = (start, start)
        for k in range(devices):
            passed = k < here
            total = pair_combine(total, (pieces[k, 0], pieces[k, 1]))
            inside = jax.tree.map(lambda new, old: jnp.where(passed, new, old), total, inside)
        before = pair_combine(inside, before)
    return before


def attention_kernel(
    place, group, kv, packed, query, peak, total, values, value_t, *, block_rows, part_rows
):
    heads, size, rows = group.shape
    chunk_keys = kv.shape[1]
    z, y, member = (place[0], place[1], place[2])
    scale = (size // 2) ** (-0.5) * log2_e
    line = lax.broadcasted_iota(jnp.int32, (size, rows), 0)
    for h in range(heads):
        whole = group[h]
        zero = jnp.zeros_like(whole)
        query[2 * h] = jnp.where(line < size // 2, whole, zero)
        query[2 * h + 1] = jnp.where(line < size // 2, zero, whole)
    peak[...] = jnp.full(peak.shape, far_below, jnp.float32)
    total[...] = jnp.zeros(total.shape, jnp.float32)
    values[...] = jnp.zeros(values.shape, jnp.float32)

    def visible_keys():
        row = lax.broadcasted_iota(jnp.int32, (chunk_keys, rows), 0)
        lane = lax.broadcasted_iota(jnp.int32, (chunk_keys, rows), 1)
        key_pos = (row // part_rows) * block_rows + member * part_rows + row % part_rows
        half, piece = (rows // 2, part_rows // 2)
        inside = (lane % half) // piece * part_rows + lane // half * piece + lane % piece
        return key_pos <= inside + y * block_rows

    def one_chunk(at, masked):
        both = kv[at]
        keys = both[:, :size]
        value_t[...] = both[:, size:].T
        visible = visible_keys() if masked else None

        def scores_of(i):
            found = jnp.dot(keys, query[i], preferred_element_type=jnp.float32) * scale
            return jnp.where(visible, found, far_below) if masked else found

        scores = scores_of(0)
        for i in range(2 * heads):
            following = scores_of(i + 1) if i + 1 < 2 * heads else None
            old = peak[i]
            now = jnp.maximum(old, jnp.max(scores, axis=0, keepdims=True))
            expos = jnp.exp2(scores - now)
            if masked:
                expos = jnp.where(visible, expos, 0.0)
            fade = jnp.exp2(old - now)
            peak[i] = now
            total[i] = total[i] * fade + jnp.sum(expos, axis=0, keepdims=True)
            values[i] = values[i] * fade + jnp.dot(
                value_t[...], expos.astype(jnp.bfloat16), preferred_element_type=jnp.float32
            )
            scores = following

    one_chunk(z, True)

    def earlier(at, _):
        one_chunk(at, False)
        return 0

    lax.fori_loop(0, z, earlier, 0)

    half = rows // 2
    line = lax.broadcasted_iota(jnp.int32, (16, rows), 0)
    for h in range(heads):
        tail = jnp.zeros((16, rows), jnp.float32)
        for m in range(2):
            amount = total[2 * h + m]
            some = amount > 0.0
            safe = jnp.where(some, amount, 1.0)
            shares = (values[2 * h + m] * jnp.where(some, 1.0 / safe, 0.0)).astype(jnp.bfloat16)
            level = jnp.where(some, peak[2 * h + m] + jnp.log2(safe), far_below)
            coarse = level.astype(jnp.bfloat16).astype(jnp.float32)
            tail = jnp.where(line == 2 * m, coarse, tail)
            tail = jnp.where(line == 2 * m + 1, level - coarse, tail)
            for t in range(2):
                packed[h, t, m * size : (m + 1) * size, :] = shares[:, t * half : (t + 1) * half]
        rounded = tail.astype(jnp.bfloat16)
        for t in range(2):
            packed[h, t, 2 * size : 2 * size + 16, :] = rounded[:, t * half : (t + 1) * half]


def vmem():
    return pl.BlockSpec(memory_space=pltpu.VMEM)


def smem():
    return pl.BlockSpec(memory_space=pltpu.SMEM)


def attention(place, group, kv, block_rows, part_rows):
    heads, size, rows = group.shape
    z_count, chunk_keys, _ = kv.shape
    keys = chunk_keys * z_count
    return pl.pallas_call(
        functools.partial(attention_kernel, block_rows=block_rows, part_rows=part_rows),
        out_shape=jax.ShapeDtypeStruct((heads, 2, 2 * size + 16, rows // 2), jnp.bfloat16),
        in_specs=[smem(), vmem(), vmem()],
        out_specs=vmem(),
        scratch_shapes=[
            pltpu.VMEM((2 * heads, size, rows), jnp.bfloat16),
            pltpu.VMEM((2 * heads, 1, rows), jnp.float32),
            pltpu.VMEM((2 * heads, 1, rows), jnp.float32),
            pltpu.VMEM((2 * heads, size, rows), jnp.float32),
            pltpu.VMEM((size, chunk_keys), jnp.bfloat16),
        ],
        cost_estimate=pl.CostEstimate(
            flops=4 * 2 * heads * rows * keys * size,
            bytes_accessed=4 << 20,
            transcendentals=2 * heads * rows * keys,
        ),
        name="attention",
    )(place, group, kv)


def finish_kernel(place, lams, parts, gain, lru_mine, lru_theirs, w_mine, w_theirs, out):
    count, _, lines, _ = parts.shape
    size = (lines - 16) // 2
    core = place[0]

    def head_output(owner):
        joined = []
        for m in range(2):
            tails = [parts[i, owner, 2 * size :, :].astype(jnp.float32) for i in range(count)]
            levels = [t[2 * m : 2 * m + 1] + t[2 * m + 1 : 2 * m + 2] for t in tails]
            top = functools.reduce(jnp.maximum, levels)
            shares = [jnp.exp2(level - top) for level in levels]
            inverse = 1.0 / functools.reduce(jnp.add, shares)
            weighted = [
                parts[i, owner, m * size : (m + 1) * size, :].astype(jnp.float32)
                * (shares[i] * inverse)
                for i in range(count)
            ]
            joined.append(functools.reduce(jnp.add, weighted))
        diff = joined[0] - lams[owner] * joined[1]
        level = lax.rsqrt(jnp.mean(diff * diff, axis=0, keepdims=True) + head_eps)
        return (diff * level * gain[...]).T.astype(jnp.bfloat16)

    mine = jnp.concatenate([lru_mine[...], head_output(core)], axis=1)
    theirs = jnp.concatenate([lru_theirs[...], head_output(1 - core)], axis=1)
    result = jnp.dot(mine, w_mine[...], preferred_element_type=jnp.float32)
    result = result + jnp.dot(theirs, w_theirs[...], preferred_element_type=jnp.float32)
    out[...] = result.astype(jnp.bfloat16)


def finish(place, lams, parts, gain, lru_mine, lru_theirs, w_mine, w_theirs):
    rows, wide = (lru_mine.shape[0], w_mine.shape[1])
    return pl.pallas_call(
        finish_kernel,
        out_shape=jax.ShapeDtypeStruct((rows, wide), jnp.bfloat16),
        in_specs=[smem(), smem()] + [vmem()] * 6,
        out_specs=vmem(),
        cost_estimate=pl.CostEstimate(
            flops=2 * rows * wide * 512, bytes_accessed=3 << 20, transcendentals=rows * 16
        ),
        name="finish",
    )(place, lams, parts, gain, lru_mine, lru_theirs, w_mine, w_theirs)


def body(
    tokens,
    norm_gain,
    query_weight,
    w_key,
    w_value,
    w_input,
    w_gate,
    conv_kernel,
    w_recur,
    w_admit,
    decay_param,
    decay_scale,
    init_state,
    diff_lambda,
    head_gain,
    w_out_lru,
    w_out_attn,
):
    member_rows, wide = tokens.shape
    fs_count = lax.axis_size("fs")
    tp_count = lax.axis_size("tp")
    row_count = member_rows * fs_count * tp_count
    share_rows = member_rows * tp_count
    member = lax.axis_index("fs")
    core = lax.axis_index("tp")
    z_count, z = (lax.axis_size("sp_0"), lax.axis_index("sp_0"))
    y_count, y = (lax.axis_size("sp_1"), lax.axis_index("sp_1"))

    floats = tokens.astype(jnp.float32)
    normed = (
        floats * lax.rsqrt(jnp.mean(floats * floats, axis=1, keepdims=True) + input_eps) * norm_gain
    ).astype(jnp.bfloat16)

    taps = conv_kernel.shape[0]
    margin = 8
    before_rows = passed_along(normed[member_rows - margin :], SP, 1)

    chip_rows = lax.all_gather(normed, "tp", axis=0, tiled=True)
    kv_here = jnp.concatenate(
        [
            jnp.dot(chip_rows, weight, preferred_element_type=jnp.float32).astype(jnp.bfloat16)
            for weight in (w_key, w_value)
        ],
        axis=1,
    )
    kv_here, normed, before_rows = lax.optimization_barrier((kv_here, normed, before_rows))
    everyone = from_everyone(kv_here, SP)
    everyone = everyone.reshape(z_count, y_count * share_rows, kv_here.shape[1])

    sent = jnp.concatenate([normed, before_rows], axis=0)
    sent_rows = sent.shape[0]
    mine = lax.all_gather(sent, "fs", axis=0, tiled=True)
    swap = [(0, 1), (1, 0)]
    theirs = lax.ppermute(mine, "tp", swap)

    def projected(weight):
        a, b = [
            jnp.dot(piece, weight, preferred_element_type=jnp.float32).astype(jnp.bfloat16)
            for piece in (mine, theirs)
        ]
        both = jnp.stack([jnp.where(core == 0, a, b), jnp.where(core == 0, b, a)], axis=0)
        return both.reshape(tp_count, fs_count, sent_rows, weight.shape[1])

    def in_order(both):
        return jnp.moveaxis(both[:, :, :member_rows], 0, 1).reshape(row_count, both.shape[3])

    query = projected(query_weight)[:, :, :member_rows].reshape(row_count, query_weight.shape[1])
    lru_all = projected(w_input)
    lru_in = in_order(lru_all)
    earlier_rows = lru_all[tp_count - 1, fs_count - 1, sent_rows - (taps - 1) :]
    gate_proj = in_order(projected(w_gate))

    group = lax.all_gather(query.T, "fs")

    w_mine = jnp.concatenate([w_out_lru, w_out_attn], axis=0)
    w_theirs = lax.ppermute(w_mine, "tp", swap)
    lams = lax.all_gather(diff_lambda, "tp", axis=0, tiled=True)

    channels = lru_in.shape[1]
    padded = jnp.concatenate([earlier_rows, lru_in], axis=0).astype(jnp.float32)
    conv_sum = jnp.zeros((row_count, channels), jnp.float32)
    for offset in range(taps):
        conv_sum = conv_sum + conv_kernel[offset] * padded[offset : offset + row_count]
    conv_out = conv_sum.astype(jnp.bfloat16)
    grouped = conv_out.reshape(row_count, w_recur.shape[0], w_recur.shape[1])
    recur = jax.nn.sigmoid(
        jnp.einsum("tni,nij->tnj", grouped, w_recur, preferred_element_type=jnp.float32).reshape(
            row_count, channels
        )
    )
    admit = jax.nn.sigmoid(
        jnp.einsum("tni,nij->tnj", grouped, w_admit, preferred_element_type=jnp.float32).reshape(
            row_count, channels
        )
    )
    log_decay = -gate_scale * recur * jax.nn.softplus(-decay_param) * decay_scale
    decay = jnp.exp(log_decay)
    drive = jnp.sqrt(-jnp.expm1(2.0 * log_decay)) * admit * conv_out.astype(jnp.float32)
    decay_run, local_states = lax.associative_scan(pair_combine, (decay, drive), axis=0)
    before_decay, before_state = prefix_by_axis(
        jnp.stack([decay_run[-1], local_states[-1]]), SP
    )
    entering = before_decay * init_state + before_state
    states = local_states + decay_run * entering[None, :]
    lru_out = (states * jax.nn.gelu(gate_proj.astype(jnp.float32))).astype(jnp.bfloat16)

    place = jnp.stack([z, y, member]).astype(jnp.int32)
    carried = attention(place, group, everyone, row_count, share_rows)
    lru_split = lru_out.reshape(fs_count, tp_count, member_rows, channels)
    lru_mine = lax.dynamic_index_in_dim(lru_split, core, 1, keepdims=False)
    lru_other = lax.dynamic_index_in_dim(lru_split, 1 - core, 1, keepdims=False)
    half_rows = fs_count * member_rows
    lru_theirs = lax.ppermute(lru_other.reshape(half_rows, channels), "tp", swap)

    lines = carried.shape[2]
    carried = carried.reshape(fs_count * tp_count, lines, half_rows)
    packed = lax.all_to_all(carried, ("fs", "tp"), split_axis=0, concat_axis=0, tiled=True)
    packed = packed.reshape(fs_count, tp_count, lines, half_rows)

    gain = jnp.broadcast_to(head_gain[:, None], (head_gain.shape[0], half_rows))
    partial = finish(
        core[None].astype(jnp.int32),
        lams,
        packed,
        gain,
        lru_mine.reshape(half_rows, channels),
        lru_theirs,
        w_mine,
        w_theirs,
    )
    partial = partial.reshape(fs_count, member_rows, wide)
    arrived = lax.all_to_all(partial, "fs", split_axis=0, concat_axis=0, tiled=True)
    return arrived.astype(jnp.float32).sum(axis=0).astype(jnp.bfloat16)


def solution(mesh):
    torus = Mesh(
        mesh.devices.reshape(8, 8, mesh.shape["fs"], mesh.shape["tp"]), ("sp_0", "sp_1", "fs", "tp")
    )

    return jax.shard_map(
        body,
        mesh=torus,
        in_specs=(
            P(SP_FS_TP, None),
            P(),
            P(None, ("fs", "tp")),
            P(None, "tp"),
            P(None, "tp"),
            P(None, ("fs", "tp")),
            P(None, ("fs", "tp")),
            P(None, ("fs", "tp")),
            P(("fs", "tp"), None, None),
            P(("fs", "tp"), None, None),
            P(("fs", "tp")),
            P(SP, ("fs", "tp")),
            P(("fs", "tp")),
            P(("fs", "tp")),
            P(),
            P(("fs", "tp"), None),
            P(("fs", "tp"), None),
        ),
        out_specs=P(SP_FS_TP, None),
        check_vma=False,
    )
```

```python
import functools

import jax
import jax.numpy as jnp
from jax import lax
from jax.experimental import pallas as pl
from jax.experimental.pallas import tpu as pltpu
from jax.sharding import Mesh
from jax.sharding import PartitionSpec as P


SP = ("sp_0", "sp_1")
SP_FS_TP = ("sp_0", "sp_1", "fs", "tp")


gate_scale = 8.0
input_eps = 1e-06
head_eps = 1e-05
far_below = -1e30
log2_e = 1.4426950408889634


def from_everyone(value, axis):
    copies = jnp.broadcast_to(value, (lax.axis_size(axis), *value.shape))
    return lax.all_to_all(copies, axis, split_axis=0, concat_axis=0, tiled=True)


def passed_along(value, axis, by):
    devices = lax.axis_size(axis)
    pairs = [(i, i + by) for i in range(devices) if 0 <= i + by < devices]
    return lax.ppermute(value, axis, pairs)


def pair_combine(earlier, later):
    decay_early, state_early = earlier
    decay_late, state_late = later
    return (decay_early * decay_late, decay_late * state_early + state_late)


def vmem():
    return pl.BlockSpec(memory_space=pltpu.VMEM)


def smem():
    return pl.BlockSpec(memory_space=pltpu.SMEM)


def one_minus_exp(x):
    series = jnp.full_like(x, 1.0)
    for k in range(7, 1, -1):
        series = 1.0 - series * x * (1.0 / k)
    return jnp.where(x < 0.35, x * series, 1.0 - jnp.exp(-x))


def project_kernel(
    place, mine, theirs, w_query, w_input, w_gate, taps, w_recur, w_admit, rate, scale,
    query_t, decays, states, gates, ends, *, fs_count, member_rows,
):
    core = place[3]
    sent_rows = mine.shape[0] // fs_count
    first = jnp.where(core == 0, mine[...], theirs[...])
    second = jnp.where(core == 0, theirs[...], mine[...])
    rows = jnp.concatenate([first, second], axis=0)

    def project(weight):
        return jnp.dot(rows, weight[...], preferred_element_type=jnp.float32)

    def piece(value, t, f):
        at = (t * fs_count + f) * sent_rows
        return value[at : at + member_rows]

    def in_order(value):
        pieces = [piece(value, t, f) for f in range(fs_count) for t in range(2)]
        return jnp.concatenate(pieces, axis=0)

    query = project(w_query)
    query = jnp.concatenate([piece(query, t, f) for t in range(2) for f in range(fs_count)], axis=0)
    query_t[...] = query.astype(jnp.bfloat16).T

    gate = in_order(project(w_gate).astype(jnp.bfloat16)).astype(jnp.float32)
    gates[...] = jax.nn.gelu(gate)

    lru_all = project(w_input).astype(jnp.bfloat16).astype(jnp.float32)
    margin = sent_rows - member_rows
    before = lru_all[2 * fs_count * sent_rows - margin :]
    padded = jnp.concatenate([before, in_order(lru_all)], axis=0)
    count = taps.shape[0]
    conv_sum = padded[margin:] * taps[count - 1 : count, :]
    for back in range(1, count):
        moved = pltpu.roll(padded, back, 0)[margin:]
        conv_sum = conv_sum + moved * taps[count - 1 - back : count - back, :]
    conv_out = conv_sum.astype(jnp.bfloat16)

    def gate_of(weight):
        zero = jnp.zeros(weight.shape[1:], weight.dtype)
        whole = jnp.concatenate(
            [
                jnp.concatenate([weight[0], zero], axis=1),
                jnp.concatenate([zero, weight[1]], axis=1),
            ],
            axis=0,
        )
        return jax.nn.sigmoid(jnp.dot(conv_out, whole, preferred_element_type=jnp.float32))

    log_decay = -gate_of(w_recur) * rate[...] * scale[...]
    decay = jnp.exp(log_decay)
    drive = jnp.sqrt(one_minus_exp(-2.0 * log_decay)) * gate_of(w_admit) * conv_out.astype(jnp.float32)

    row = lax.broadcasted_iota(jnp.int32, decay.shape, 0)
    by = 1
    while by < decay.shape[0]:
        inside = row >= by
        decay_before = jnp.where(inside, pltpu.roll(decay, by, 0), 1.0)
        state_before = jnp.where(inside, pltpu.roll(drive, by, 0), 0.0)
        drive = decay * state_before + drive
        decay = decay * decay_before
        by *= 2
    decays[...] = decay
    states[...] = drive
    last = decay.shape[0] - 1
    ends[0:1, :] = decay[last:]
    ends[1:2, :] = drive[last:]


def project(place, mine, theirs, weights, taps, w_recur, w_admit, rate, scale, fs_count, rows):
    channels = scale.shape[1]
    block = jax.ShapeDtypeStruct(scale.shape, jnp.float32)
    return pl.pallas_call(
        functools.partial(project_kernel, fs_count=fs_count, member_rows=rows),
        out_shape=(
            jax.ShapeDtypeStruct((channels, scale.shape[0]), jnp.bfloat16),
            block,
            block,
            block,
            jax.ShapeDtypeStruct((2, channels), jnp.float32),
        ),
        in_specs=[smem()] + [vmem()] * 10,
        out_specs=(vmem(),) * 5,
        cost_estimate=pl.CostEstimate(
            flops=2 * scale.shape[0] * mine.shape[1] * 3 * channels,
            bytes_accessed=4 << 20,
            transcendentals=1 << 18,
        ),
        name="project",
    )(place, mine, theirs, *weights, taps, w_recur, w_admit, rate, scale)


def states_kernel(
    place, near, far, start, decays, states, gates, mine, theirs, *, fs_count, member_rows
):
    z, y, core = (place[0], place[1], place[3])

    def before(pieces, here):
        decay, state = (jnp.ones_like(pieces[0, 0:1]), jnp.zeros_like(pieces[0, 1:2]))
        for k in range(pieces.shape[0]):
            passed = k < here
            new_decay, new_state = pair_combine((decay, state), (pieces[k, 0:1], pieces[k, 1:2]))
            decay = jnp.where(passed, new_decay, decay)
            state = jnp.where(passed, new_state, state)
        return decay, state

    decay, state = pair_combine(before(far, z), before(near, y))
    entering = decay * start[...] + state
    out = ((states[...] + decays[...] * entering) * gates[...]).astype(jnp.bfloat16)
    for f in range(fs_count):
        at = 2 * f * member_rows
        even = out[at : at + member_rows]
        odd = out[at + member_rows : at + 2 * member_rows]
        mine[f * member_rows : (f + 1) * member_rows] = jnp.where(core == 0, even, odd)
        theirs[f * member_rows : (f + 1) * member_rows] = jnp.where(core == 0, odd, even)


def final_states(place, near, far, start, decays, states, gates, fs_count, member_rows):
    half = jax.ShapeDtypeStruct((fs_count * member_rows, decays.shape[1]), jnp.bfloat16)
    return pl.pallas_call(
        functools.partial(states_kernel, fs_count=fs_count, member_rows=member_rows),
        out_shape=(half, half),
        in_specs=[smem()] + [vmem()] * 6,
        out_specs=(vmem(), vmem()),
        cost_estimate=pl.CostEstimate(
            flops=1 << 20, bytes_accessed=1 << 19, transcendentals=0
        ),
        name="final_states",
    )(place, near, far, start, decays, states, gates)


def attention_kernel(
    place, group, kv, packed, query, peak, total, values, value_t, *, block_rows, part_rows
):
    heads, size, rows = group.shape
    chunk_keys = kv.shape[1]
    z, y, member = (place[0], place[1], place[2])
    scale = (size // 2) ** (-0.5) * log2_e
    line = lax.broadcasted_iota(jnp.int32, (size, rows), 0)
    for h in range(heads):
        whole = group[h]
        zero = jnp.zeros_like(whole)
        query[2 * h] = jnp.where(line < size // 2, whole, zero)
        query[2 * h + 1] = jnp.where(line < size // 2, zero, whole)
    peak[...] = jnp.full(peak.shape, far_below, jnp.float32)
    total[...] = jnp.zeros(total.shape, jnp.float32)
    values[...] = jnp.zeros(values.shape, jnp.float32)

    def visible_keys():
        row = lax.broadcasted_iota(jnp.int32, (chunk_keys, rows), 0)
        lane = lax.broadcasted_iota(jnp.int32, (chunk_keys, rows), 1)
        key_pos = (row // part_rows) * block_rows + member * part_rows + row % part_rows
        half, piece = (rows // 2, part_rows // 2)
        inside = (lane % half) // piece * part_rows + lane // half * piece + lane % piece
        return key_pos <= inside + y * block_rows

    def one_chunk(at, masked):
        both = kv[at]
        keys = both[:, :size]
        value_t[...] = both[:, size:].T
        visible = visible_keys() if masked else None

        def scores_of(i):
            found = jnp.dot(keys, query[i], preferred_element_type=jnp.float32) * scale
            return jnp.where(visible, found, far_below) if masked else found

        scores = scores_of(0)
        for i in range(2 * heads):
            following = scores_of(i + 1) if i + 1 < 2 * heads else None
            old = peak[i]
            now = jnp.maximum(old, jnp.max(scores, axis=0, keepdims=True))
            expos = jnp.exp2(scores - now)
            if masked:
                expos = jnp.where(visible, expos, 0.0)
            fade = jnp.exp2(old - now)
            peak[i] = now
            total[i] = total[i] * fade + jnp.sum(expos, axis=0, keepdims=True)
            values[i] = values[i] * fade + jnp.dot(
                value_t[...], expos.astype(jnp.bfloat16), preferred_element_type=jnp.float32
            )
            scores = following

    one_chunk(z, True)

    def earlier(at, _):
        one_chunk(at, False)
        return 0

    lax.fori_loop(0, z, earlier, 0)

    half = rows // 2
    line = lax.broadcasted_iota(jnp.int32, (16, rows), 0)
    for h in range(heads):
        tail = jnp.zeros((16, rows), jnp.float32)
        for m in range(2):
            amount = total[2 * h + m]
            some = amount > 0.0
            safe = jnp.where(some, amount, 1.0)
            shares = (values[2 * h + m] * jnp.where(some, 1.0 / safe, 0.0)).astype(jnp.bfloat16)
            level = jnp.where(some, peak[2 * h + m] + jnp.log2(safe), far_below)
            coarse = level.astype(jnp.bfloat16).astype(jnp.float32)
            tail = jnp.where(line == 2 * m, coarse, tail)
            tail = jnp.where(line == 2 * m + 1, level - coarse, tail)
            for t in range(2):
                packed[h, t, m * size : (m + 1) * size, :] = shares[:, t * half : (t + 1) * half]
        rounded = tail.astype(jnp.bfloat16)
        for t in range(2):
            packed[h, t, 2 * size : 2 * size + 16, :] = rounded[:, t * half : (t + 1) * half]


def attention(place, group, kv, block_rows, part_rows):
    heads, size, rows = group.shape
    z_count, chunk_keys, _ = kv.shape
    keys = chunk_keys * z_count
    return pl.pallas_call(
        functools.partial(attention_kernel, block_rows=block_rows, part_rows=part_rows),
        out_shape=jax.ShapeDtypeStruct((heads, 2, 2 * size + 16, rows // 2), jnp.bfloat16),
        in_specs=[smem(), vmem(), vmem()],
        out_specs=vmem(),
        scratch_shapes=[
            pltpu.VMEM((2 * heads, size, rows), jnp.bfloat16),
            pltpu.VMEM((2 * heads, 1, rows), jnp.float32),
            pltpu.VMEM((2 * heads, 1, rows), jnp.float32),
            pltpu.VMEM((2 * heads, size, rows), jnp.float32),
            pltpu.VMEM((size, chunk_keys), jnp.bfloat16),
        ],
        cost_estimate=pl.CostEstimate(
            flops=4 * 2 * heads * rows * keys * size,
            bytes_accessed=4 << 20,
            transcendentals=2 * heads * rows * keys,
        ),
        name="attention",
    )(place, group, kv)


def finish_kernel(place, lam, lam_theirs, parts, gain, lru_mine, lru_theirs, w_mine, w_theirs, out):
    count, _, lines, _ = parts.shape
    size = (lines - 16) // 2
    core = place[3]

    def head_output(owner, factor):
        joined = []
        for m in range(2):
            tails = [parts[i, owner, 2 * size :, :].astype(jnp.float32) for i in range(count)]
            levels = [t[2 * m : 2 * m + 1] + t[2 * m + 1 : 2 * m + 2] for t in tails]
            top = functools.reduce(jnp.maximum, levels)
            shares = [jnp.exp2(level - top) for level in levels]
            inverse = 1.0 / functools.reduce(jnp.add, shares)
            weighted = [
                parts[i, owner, m * size : (m + 1) * size, :].astype(jnp.float32)
                * (shares[i] * inverse)
                for i in range(count)
            ]
            joined.append(functools.reduce(jnp.add, weighted))
        diff = joined[0] - factor * joined[1]
        level = lax.rsqrt(jnp.mean(diff * diff, axis=0, keepdims=True) + head_eps)
        return ((diff * level).T * gain[...]).astype(jnp.bfloat16)

    mine = jnp.concatenate([lru_mine[...], head_output(core, lam[0])], axis=1)
    theirs = jnp.concatenate([lru_theirs[...], head_output(1 - core, lam_theirs[0])], axis=1)
    result = jnp.dot(mine, w_mine[...], preferred_element_type=jnp.float32)
    result = result + jnp.dot(theirs, w_theirs[...], preferred_element_type=jnp.float32)
    out[...] = result.astype(jnp.bfloat16)


def finish(place, lam, lam_theirs, parts, gain, lru_mine, lru_theirs, w_mine, w_theirs):
    rows, wide = (lru_mine.shape[0], w_mine.shape[1])
    return pl.pallas_call(
        finish_kernel,
        out_shape=jax.ShapeDtypeStruct((rows, wide), jnp.bfloat16),
        in_specs=[smem()] * 3 + [vmem()] * 6,
        out_specs=vmem(),
        cost_estimate=pl.CostEstimate(
            flops=2 * rows * wide * 512, bytes_accessed=3 << 20, transcendentals=rows * 16
        ),
        name="finish",
    )(place, lam, lam_theirs, parts, gain, lru_mine, lru_theirs, w_mine, w_theirs)


def body(
    tokens,
    norm_gain,
    query_weight,
    w_key,
    w_value,
    w_input,
    w_gate,
    conv_kernel,
    w_recur,
    w_admit,
    decay_param,
    decay_scale,
    init_state,
    diff_lambda,
    head_gain,
    w_out_lru,
    w_out_attn,
):
    member_rows, wide = tokens.shape
    fs_count = lax.axis_size("fs")
    tp_count = lax.axis_size("tp")
    row_count = member_rows * fs_count * tp_count
    share_rows = member_rows * tp_count
    member = lax.axis_index("fs")
    core = lax.axis_index("tp")
    z_count, z = (lax.axis_size("sp_0"), lax.axis_index("sp_0"))
    y_count, y = (lax.axis_size("sp_1"), lax.axis_index("sp_1"))

    floats = tokens.astype(jnp.float32)
    normed = (
        floats * lax.rsqrt(jnp.mean(floats * floats, axis=1, keepdims=True) + input_eps) * norm_gain
    ).astype(jnp.bfloat16)

    margin = 8
    before_rows = passed_along(normed[member_rows - margin :], SP, 1)

    chip_rows = lax.all_gather(normed, "tp", axis=0, tiled=True)
    kv_here = jnp.concatenate(
        [
            jnp.dot(chip_rows, weight, preferred_element_type=jnp.float32).astype(jnp.bfloat16)
            for weight in (w_key, w_value)
        ],
        axis=1,
    )
    kv_here, normed, before_rows = lax.optimization_barrier((kv_here, normed, before_rows))
    everyone = from_everyone(kv_here, SP)
    everyone = everyone.reshape(z_count, y_count * share_rows, kv_here.shape[1])

    sent = jnp.concatenate([normed, before_rows], axis=0)
    mine = lax.all_gather(sent, "fs", axis=0, tiled=True)
    swap = [(0, 1), (1, 0)]
    theirs = lax.ppermute(mine, "tp", swap)

    place = jnp.stack([z, y, member, core]).astype(jnp.int32)
    rate = gate_scale * jax.nn.softplus(-decay_param)
    query_t, decays, states, gates, ends = project(
        place,
        mine,
        theirs,
        (query_weight, w_input, w_gate),
        conv_kernel,
        w_recur,
        w_admit,
        rate[None],
        decay_scale,
        fs_count,
        member_rows,
    )

    group = lax.all_gather(query_t, "fs")

    near = lax.all_gather(ends, "sp_1")
    row = (near[0, 0], near[0, 1])
    for k in range(1, y_count):
        row = pair_combine(row, (near[k, 0], near[k, 1]))
    far = from_everyone(jnp.stack(row), "sp_0")

    w_mine = jnp.concatenate([w_out_lru, w_out_attn], axis=0)
    w_theirs = lax.ppermute(w_mine, "tp", swap)
    lam_theirs = lax.ppermute(diff_lambda, "tp", swap)

    carried = attention(place, group, everyone, row_count, share_rows)
    lines, half_rows = carried.shape[2:]
    carried = carried.reshape(fs_count * tp_count, lines, half_rows)
    packed = lax.all_to_all(carried, ("fs", "tp"), split_axis=0, concat_axis=0, tiled=True)
    packed = packed.reshape(fs_count, tp_count, lines, half_rows)

    lru_mine, lru_other = final_states(
        place, near, far, init_state[None], decays, states, gates, fs_count, member_rows
    )
    lru_theirs = lax.ppermute(lru_other, "tp", swap)

    partial = finish(
        place,
        diff_lambda,
        lam_theirs,
        packed,
        head_gain[None],
        lru_mine,
        lru_theirs,
        w_mine,
        w_theirs,
    )
    partial = partial.reshape(fs_count, member_rows, wide)
    arrived = lax.all_to_all(partial, "fs", split_axis=0, concat_axis=0, tiled=True)
    return arrived.astype(jnp.float32).sum(axis=0).astype(jnp.bfloat16)


def solution(mesh):
    torus = Mesh(
        mesh.devices.reshape(8, 8, mesh.shape["fs"], mesh.shape["tp"]), ("sp_0", "sp_1", "fs", "tp")
    )

    return jax.shard_map(
        body,
        mesh=torus,
        in_specs=(
            P(SP_FS_TP, None),
            P(),
            P(None, ("fs", "tp")),
            P(None, "tp"),
            P(None, "tp"),
            P(None, ("fs", "tp")),
            P(None, ("fs", "tp")),
            P(None, ("fs", "tp")),
            P(("fs", "tp"), None, None),
            P(("fs", "tp"), None, None),
            P(("fs", "tp")),
            P(SP, ("fs", "tp")),
            P(("fs", "tp")),
            P(("fs", "tp")),
            P(),
            P(("fs", "tp"), None),
            P(("fs", "tp"), None),
        ),
        out_specs=P(SP_FS_TP, None),
        check_vma=False,
    )
```

```python
import functools

import jax
import jax.numpy as jnp
from jax import lax
from jax.experimental import pallas as pl
from jax.experimental.pallas import tpu as pltpu
from jax.sharding import Mesh
from jax.sharding import PartitionSpec as P


SP = ("sp_0", "sp_1")
SP_FS_TP = ("sp_0", "sp_1", "fs", "tp")


gate_scale = 8.0
input_eps = 1e-06
head_eps = 1e-05
far_below = -1e30
log2_e = 1.4426950408889634


def from_everyone(value, axis):
    copies = jnp.broadcast_to(value, (lax.axis_size(axis), *value.shape))
    return lax.all_to_all(copies, axis, split_axis=0, concat_axis=0, tiled=True)


def passed_along(value, axis, by):
    devices = lax.axis_size(axis)
    pairs = [(i, i + by) for i in range(devices) if 0 <= i + by < devices]
    return lax.ppermute(value, axis, pairs)


def pair_combine(earlier, later):
    decay_early, state_early = earlier
    decay_late, state_late = later
    return (decay_early * decay_late, decay_late * state_early + state_late)


def vmem():
    return pl.BlockSpec(memory_space=pltpu.VMEM)


def smem():
    return pl.BlockSpec(memory_space=pltpu.SMEM)


def one_minus_exp(x):
    series = jnp.full_like(x, 1.0)
    for k in range(7, 1, -1):
        series = 1.0 - series * x * (1.0 / k)
    return jnp.where(x < 0.35, x * series, 1.0 - jnp.exp(-x))


def project_kernel(
    place, mine, theirs, w_query, w_input, w_gate, taps, w_recur, w_admit, rate, scale,
    query_t, decays, states, gates, ends, *, fs_count, member_rows,
):
    core = place[3]
    sent_rows = mine.shape[0] // fs_count
    first = jnp.where(core == 0, mine[...], theirs[...])
    second = jnp.where(core == 0, theirs[...], mine[...])
    rows = jnp.concatenate([first, second], axis=0)

    def project(weight):
        return jnp.dot(rows, weight[...], preferred_element_type=jnp.float32)

    def piece(value, t, f):
        at = (t * fs_count + f) * sent_rows
        return value[at : at + member_rows]

    def in_order(value):
        pieces = [piece(value, t, f) for f in range(fs_count) for t in range(2)]
        return jnp.concatenate(pieces, axis=0)

    query = project(w_query)
    query = jnp.concatenate([piece(query, t, f) for t in range(2) for f in range(fs_count)], axis=0)
    query_t[...] = query.astype(jnp.bfloat16).T

    gate = in_order(project(w_gate).astype(jnp.bfloat16)).astype(jnp.float32)
    gates[...] = jax.nn.gelu(gate)

    lru_all = project(w_input).astype(jnp.bfloat16).astype(jnp.float32)
    margin = sent_rows - member_rows
    before = lru_all[2 * fs_count * sent_rows - margin :]
    padded = jnp.concatenate([before, in_order(lru_all)], axis=0)
    count = taps.shape[0]
    conv_sum = padded[margin:] * taps[count - 1 : count, :]
    for back in range(1, count):
        moved = pltpu.roll(padded, back, 0)[margin:]
        conv_sum = conv_sum + moved * taps[count - 1 - back : count - back, :]
    conv_out = conv_sum.astype(jnp.bfloat16)

    def gate_of(weight):
        zero = jnp.zeros(weight.shape[1:], weight.dtype)
        whole = jnp.concatenate(
            [
                jnp.concatenate([weight[0], zero], axis=1),
                jnp.concatenate([zero, weight[1]], axis=1),
            ],
            axis=0,
        )
        return jax.nn.sigmoid(jnp.dot(conv_out, whole, preferred_element_type=jnp.float32))

    log_decay = -gate_of(w_recur) * rate[...] * scale[...]
    decay = jnp.exp(log_decay)
    drive = jnp.sqrt(one_minus_exp(-2.0 * log_decay)) * gate_of(w_admit) * conv_out.astype(jnp.float32)

    row = lax.broadcasted_iota(jnp.int32, decay.shape, 0)
    by = 1
    while by < decay.shape[0]:
        inside = row >= by
        decay_before = jnp.where(inside, pltpu.roll(decay, by, 0), 1.0)
        state_before = jnp.where(inside, pltpu.roll(drive, by, 0), 0.0)
        drive = decay * state_before + drive
        decay = decay * decay_before
        by *= 2
    decays[...] = decay
    states[...] = drive
    last = decay.shape[0] - 1
    ends[0:1, :] = decay[last:]
    ends[1:2, :] = drive[last:]


def project(place, mine, theirs, weights, taps, w_recur, w_admit, rate, scale, fs_count, rows):
    channels = scale.shape[1]
    block = jax.ShapeDtypeStruct(scale.shape, jnp.float32)
    return pl.pallas_call(
        functools.partial(project_kernel, fs_count=fs_count, member_rows=rows),
        out_shape=(
            jax.ShapeDtypeStruct((channels, scale.shape[0]), jnp.bfloat16),
            block,
            block,
            block,
            jax.ShapeDtypeStruct((2, channels), jnp.float32),
        ),
        in_specs=[smem()] + [vmem()] * 10,
        out_specs=(vmem(),) * 5,
        cost_estimate=pl.CostEstimate(
            flops=2 * scale.shape[0] * mine.shape[1] * 3 * channels,
            bytes_accessed=4 << 20,
            transcendentals=1 << 18,
        ),
        name="project",
    )(place, mine, theirs, *weights, taps, w_recur, w_admit, rate, scale)


def states_kernel(
    place, near, far, start, decays, states, gates, mine, theirs, *, fs_count, member_rows
):
    z, y, core = (place[0], place[1], place[3])

    def before(pieces, here):
        decay, state = (jnp.ones_like(pieces[0, 0:1]), jnp.zeros_like(pieces[0, 1:2]))
        for k in range(pieces.shape[0]):
            passed = k < here
            new_decay, new_state = pair_combine((decay, state), (pieces[k, 0:1], pieces[k, 1:2]))
            decay = jnp.where(passed, new_decay, decay)
            state = jnp.where(passed, new_state, state)
        return decay, state

    decay, state = pair_combine(before(far, z), before(near, y))
    entering = decay * start[...] + state
    out = ((states[...] + decays[...] * entering) * gates[...]).astype(jnp.bfloat16)
    for f in range(fs_count):
        at = 2 * f * member_rows
        even = out[at : at + member_rows]
        odd = out[at + member_rows : at + 2 * member_rows]
        mine[f * member_rows : (f + 1) * member_rows] = jnp.where(core == 0, even, odd)
        theirs[f * member_rows : (f + 1) * member_rows] = jnp.where(core == 0, odd, even)


def final_states(place, near, far, start, decays, states, gates, fs_count, member_rows):
    half = jax.ShapeDtypeStruct((fs_count * member_rows, decays.shape[1]), jnp.bfloat16)
    return pl.pallas_call(
        functools.partial(states_kernel, fs_count=fs_count, member_rows=member_rows),
        out_shape=(half, half),
        in_specs=[smem()] + [vmem()] * 6,
        out_specs=(vmem(), vmem()),
        cost_estimate=pl.CostEstimate(
            flops=1 << 20, bytes_accessed=1 << 19, transcendentals=0
        ),
        name="final_states",
    )(place, near, far, start, decays, states, gates)


def attention_kernel(*refs, chunks, block_rows, part_rows, first, last):
    place, flags, group = refs[:3]
    kvs = refs[3 : 3 + chunks]
    at = 3 + chunks
    if not first:
        before = refs[at : at + 3]
        at += 3
    if last:
        packed = refs[at]
        peak, total, values, query, value_t = refs[at + 1 :]
    else:
        peak, total, values, query, value_t = refs[at:]
    heads, size, rows = group.shape
    chunk_keys = kvs[0].shape[0]
    y, member = (place[1], place[2])
    scale = (size // 2) ** (-0.5) * log2_e
    line = lax.broadcasted_iota(jnp.int32, (size, rows), 0)
    for h in range(heads):
        whole = group[h]
        zero = jnp.zeros_like(whole)
        query[2 * h] = jnp.where(line < size // 2, whole, zero)
        query[2 * h + 1] = jnp.where(line < size // 2, zero, whole)
    if first:
        peak[...] = jnp.full(peak.shape, far_below, jnp.float32)
        total[...] = jnp.zeros(total.shape, jnp.float32)
        values[...] = jnp.zeros(values.shape, jnp.float32)
    else:
        peak[...] = before[0][...]
        total[...] = before[1][...]
        values[...] = before[2][...]

    def visible_keys():
        row = lax.broadcasted_iota(jnp.int32, (chunk_keys, rows), 0)
        lane = lax.broadcasted_iota(jnp.int32, (chunk_keys, rows), 1)
        key_pos = (row // part_rows) * block_rows + member * part_rows + row % part_rows
        half, piece = (rows // 2, part_rows // 2)
        inside = (lane % half) // piece * part_rows + lane // half * piece + lane % piece
        return key_pos <= inside + y * block_rows

    def one_chunk(kv, masked):
        keys = kv[:, :size]
        value_t[...] = kv[:, size:].T
        visible = visible_keys() if masked else None

        def scores_of(i):
            found = jnp.dot(keys, query[i], preferred_element_type=jnp.float32) * scale
            return jnp.where(visible, found, far_below) if masked else found

        scores = scores_of(0)
        for i in range(2 * heads):
            following = scores_of(i + 1) if i + 1 < 2 * heads else None
            old = peak[i]
            now = jnp.maximum(old, jnp.max(scores, axis=0, keepdims=True))
            expos = jnp.exp2(scores - now)
            if masked:
                expos = jnp.where(visible, expos, 0.0)
            fade = jnp.exp2(old - now)
            peak[i] = now
            total[i] = total[i] * fade + jnp.sum(expos, axis=0, keepdims=True)
            values[i] = values[i] * fade + jnp.dot(
                value_t[...], expos.astype(jnp.bfloat16), preferred_element_type=jnp.float32
            )
            scores = following

    for c in range(chunks):
        if first and c == 0:
            one_chunk(kvs[c], True)
        else:

            @pl.when(flags[c] > 0)
            def _(c=c):
                one_chunk(kvs[c], False)

    if not last:
        return
    half = rows // 2
    line = lax.broadcasted_iota(jnp.int32, (16, rows), 0)
    for h in range(heads):
        tail = jnp.zeros((16, rows), jnp.float32)
        for m in range(2):
            amount = total[2 * h + m]
            some = amount > 0.0
            safe = jnp.where(some, amount, 1.0)
            shares = (values[2 * h + m] * jnp.where(some, 1.0 / safe, 0.0)).astype(jnp.bfloat16)
            level = jnp.where(some, peak[2 * h + m] + jnp.log2(safe), far_below)
            coarse = level.astype(jnp.bfloat16).astype(jnp.float32)
            tail = jnp.where(line == 2 * m, coarse, tail)
            tail = jnp.where(line == 2 * m + 1, level - coarse, tail)
            for t in range(2):
                packed[h, t, m * size : (m + 1) * size, :] = shares[:, t * half : (t + 1) * half]
        rounded = tail.astype(jnp.bfloat16)
        for t in range(2):
            packed[h, t, 2 * size : 2 * size + 16, :] = rounded[:, t * half : (t + 1) * half]


def attention(place, flags, group, kvs, before, last, block_rows, part_rows):
    heads, size, rows = group.shape
    chunk_keys = kvs[0].shape[0]
    chunks = len(kvs)
    first = before is None
    small = jax.ShapeDtypeStruct((2 * heads, 1, rows), jnp.float32)
    state = (small, small, jax.ShapeDtypeStruct((2 * heads, size, rows), jnp.float32))
    scratch = [
        pltpu.VMEM((2 * heads, size, rows), jnp.bfloat16),
        pltpu.VMEM((size, chunk_keys), jnp.bfloat16),
    ]
    if last:
        outs = jax.ShapeDtypeStruct((heads, 2, 2 * size + 16, rows // 2), jnp.bfloat16)
        specs = vmem()
        scratch = [pltpu.VMEM(s.shape, s.dtype) for s in state] + scratch
    else:
        outs = state
        specs = (vmem(),) * 3
    carried = () if first else tuple(before)
    return pl.pallas_call(
        functools.partial(
            attention_kernel,
            chunks=chunks,
            block_rows=block_rows,
            part_rows=part_rows,
            first=first,
            last=last,
        ),
        out_shape=outs,
        in_specs=[smem(), smem()] + [vmem()] * (1 + chunks + len(carried)),
        out_specs=specs,
        scratch_shapes=scratch,
        cost_estimate=pl.CostEstimate(
            flops=4 * 2 * heads * rows * chunk_keys * chunks * size,
            bytes_accessed=4 << 20,
            transcendentals=2 * heads * rows * chunk_keys * chunks,
        ),
        name="attention",
    )(place, flags, group, *kvs, *carried)


def finish_kernel(place, lam, lam_theirs, parts, gain, lru_mine, lru_theirs, w_mine, w_theirs, out):
    count, _, lines, _ = parts.shape
    size = (lines - 16) // 2
    core = place[3]

    def head_output(owner, factor):
        joined = []
        for m in range(2):
            tails = [parts[i, owner, 2 * size :, :].astype(jnp.float32) for i in range(count)]
            levels = [t[2 * m : 2 * m + 1] + t[2 * m + 1 : 2 * m + 2] for t in tails]
            top = functools.reduce(jnp.maximum, levels)
            shares = [jnp.exp2(level - top) for level in levels]
            inverse = 1.0 / functools.reduce(jnp.add, shares)
            weighted = [
                parts[i, owner, m * size : (m + 1) * size, :].astype(jnp.float32)
                * (shares[i] * inverse)
                for i in range(count)
            ]
            joined.append(functools.reduce(jnp.add, weighted))
        diff = joined[0] - factor * joined[1]
        level = lax.rsqrt(jnp.mean(diff * diff, axis=0, keepdims=True) + head_eps)
        return ((diff * level).T * gain[...]).astype(jnp.bfloat16)

    mine = jnp.concatenate([lru_mine[...], head_output(core, lam[0])], axis=1)
    theirs = jnp.concatenate([lru_theirs[...], head_output(1 - core, lam_theirs[0])], axis=1)
    result = jnp.dot(mine, w_mine[...], preferred_element_type=jnp.float32)
    result = result + jnp.dot(theirs, w_theirs[...], preferred_element_type=jnp.float32)
    out[...] = result.astype(jnp.bfloat16)


def finish(place, lam, lam_theirs, parts, gain, lru_mine, lru_theirs, w_mine, w_theirs):
    rows, wide = (lru_mine.shape[0], w_mine.shape[1])
    return pl.pallas_call(
        finish_kernel,
        out_shape=jax.ShapeDtypeStruct((rows, wide), jnp.bfloat16),
        in_specs=[smem()] * 3 + [vmem()] * 6,
        out_specs=vmem(),
        cost_estimate=pl.CostEstimate(
            flops=2 * rows * wide * 512, bytes_accessed=3 << 20, transcendentals=rows * 16
        ),
        name="finish",
    )(place, lam, lam_theirs, parts, gain, lru_mine, lru_theirs, w_mine, w_theirs)


def body(
    tokens,
    norm_gain,
    query_weight,
    w_key,
    w_value,
    w_input,
    w_gate,
    conv_kernel,
    w_recur,
    w_admit,
    decay_param,
    decay_scale,
    init_state,
    diff_lambda,
    head_gain,
    w_out_lru,
    w_out_attn,
):
    member_rows, wide = tokens.shape
    fs_count = lax.axis_size("fs")
    tp_count = lax.axis_size("tp")
    row_count = member_rows * fs_count * tp_count
    share_rows = member_rows * tp_count
    member = lax.axis_index("fs")
    core = lax.axis_index("tp")
    z_count, z = (lax.axis_size("sp_0"), lax.axis_index("sp_0"))
    y_count, y = (lax.axis_size("sp_1"), lax.axis_index("sp_1"))

    floats = tokens.astype(jnp.float32)
    normed = (
        floats * lax.rsqrt(jnp.mean(floats * floats, axis=1, keepdims=True) + input_eps) * norm_gain
    ).astype(jnp.bfloat16)

    margin = 8
    before_rows = passed_along(normed[member_rows - margin :], SP, 1)

    chip_rows = lax.all_gather(normed, "tp", axis=0, tiled=True)
    kv_here = jnp.concatenate(
        [
            jnp.dot(chip_rows, weight, preferred_element_type=jnp.float32).astype(jnp.bfloat16)
            for weight in (w_key, w_value)
        ],
        axis=1,
    )
    kv_here, normed, before_rows = lax.optimization_barrier((kv_here, normed, before_rows))
    own = from_everyone(kv_here, "sp_1").reshape(y_count * share_rows, kv_here.shape[1])

    steps = z_count // 2
    up_pairs = [(i, i + 1) for i in range(z_count - 1)]
    down_pairs = [
        [(i, (i - 1) % z_count) for i in (2, 1, 0)],
        [(i, (i - 1) % z_count) for i in (1, 0, z_count - 1)],
        [(i, (i - 1) % z_count) for i in (0, z_count - 1, z_count - 2)],
    ]
    rising, falling = ([own], [own])
    for step in range(1, steps + 1):
        rising.append(lax.ppermute(rising[-1], "sp_0", up_pairs))
        if step < steps:
            falling.append(lax.ppermute(falling[-1], "sp_0", down_pairs[step - 1]))

    sent = jnp.concatenate([normed, before_rows], axis=0)
    mine = lax.all_gather(sent, "fs", axis=0, tiled=True)
    swap = [(0, 1), (1, 0)]
    theirs = lax.ppermute(mine, "tp", swap)

    place = jnp.stack([z, y, member, core]).astype(jnp.int32)
    rate = gate_scale * jax.nn.softplus(-decay_param)
    query_t, decays, states, gates, ends = project(
        place,
        mine,
        theirs,
        (query_weight, w_input, w_gate),
        conv_kernel,
        w_recur,
        w_admit,
        rate[None],
        decay_scale,
        fs_count,
        member_rows,
    )

    group = lax.all_gather(query_t, "fs")

    near = from_everyone(ends, "sp_1")
    row = (near[0, 0], near[0, 1])
    for k in range(1, y_count):
        row = pair_combine(row, (near[k, 0], near[k, 1]))
    far = from_everyone(jnp.stack(row), "sp_0")

    w_mine = jnp.concatenate([w_out_lru, w_out_attn], axis=0)
    w_theirs = lax.ppermute(w_mine, "tp", swap)
    lam_theirs = lax.ppermute(diff_lambda, "tp", swap)

    steps_of = jnp.arange(steps + 1)
    ups = (z >= steps_of).astype(jnp.int32)
    downs = (z + steps_of >= z_count).astype(jnp.int32)
    flags = jnp.concatenate([ups, downs])

    def pick(*at):
        return jnp.stack([flags[i] for i in at])

    n = steps + 1
    kvs = (own, rising[1], falling[1])
    carried = attention(place, pick(0, 1, n + 1), group, kvs, None, False, row_count, share_rows)
    kvs = (rising[2], falling[2], rising[3], falling[3])
    chosen = pick(2, n + 2, 3, n + 3)
    carried = attention(place, chosen, group, kvs, carried, False, row_count, share_rows)
    kvs = (rising[4],)
    carried = attention(place, pick(4), group, kvs, carried, True, row_count, share_rows)
    lines, half_rows = carried.shape[2:]
    carried = carried.reshape(fs_count * tp_count, lines, half_rows)
    packed = lax.all_to_all(carried, ("fs", "tp"), split_axis=0, concat_axis=0, tiled=True)
    packed = packed.reshape(fs_count, tp_count, lines, half_rows)

    lru_mine, lru_other = final_states(
        place, near, far, init_state[None], decays, states, gates, fs_count, member_rows
    )
    lru_theirs = lax.ppermute(lru_other, "tp", swap)

    partial = finish(
        place,
        diff_lambda,
        lam_theirs,
        packed,
        head_gain[None],
        lru_mine,
        lru_theirs,
        w_mine,
        w_theirs,
    )
    partial = partial.reshape(fs_count, member_rows, wide)
    arrived = lax.all_to_all(partial, "fs", split_axis=0, concat_axis=0, tiled=True)
    return arrived.astype(jnp.float32).sum(axis=0).astype(jnp.bfloat16)


def solution(mesh):
    torus = Mesh(
        mesh.devices.reshape(8, 8, mesh.shape["fs"], mesh.shape["tp"]), ("sp_0", "sp_1", "fs", "tp")
    )

    return jax.shard_map(
        body,
        mesh=torus,
        in_specs=(
            P(SP_FS_TP, None),
            P(),
            P(None, ("fs", "tp")),
            P(None, "tp"),
            P(None, "tp"),
            P(None, ("fs", "tp")),
            P(None, ("fs", "tp")),
            P(None, ("fs", "tp")),
            P(("fs", "tp"), None, None),
            P(("fs", "tp"), None, None),
            P(("fs", "tp")),
            P(SP, ("fs", "tp")),
            P(("fs", "tp")),
            P(("fs", "tp")),
            P(),
            P(("fs", "tp"), None),
            P(("fs", "tp"), None),
        ),
        out_specs=P(SP_FS_TP, None),
        check_vma=False,
    )
```

```python
import functools

import jax
import jax.numpy as jnp
from jax import lax
from jax.experimental import pallas as pl
from jax.experimental.pallas import tpu as pltpu
from jax.sharding import Mesh
from jax.sharding import PartitionSpec as P


SP = ("sp_0", "sp_1")
SP_FS_TP = ("sp_0", "sp_1", "fs", "tp")


gate_scale = 8.0
input_eps = 1e-06
head_eps = 1e-05
far_below = -1e30
log2_e = 1.4426950408889634


def from_everyone(value, axis):
    copies = jnp.broadcast_to(value, (lax.axis_size(axis), *value.shape))
    return lax.all_to_all(copies, axis, split_axis=0, concat_axis=0, tiled=True)


def passed_along(value, axis, by):
    devices = lax.axis_size(axis)
    pairs = [(i, i + by) for i in range(devices) if 0 <= i + by < devices]
    return lax.ppermute(value, axis, pairs)


def vmem():
    return pl.BlockSpec(memory_space=pltpu.VMEM)


def smem():
    return pl.BlockSpec(memory_space=pltpu.SMEM)


def one_minus_exp(x):
    series = jnp.full_like(x, 1.0)
    for k in range(7, 1, -1):
        series = 1.0 - series * x * (1.0 / k)
    return jnp.where(x < 0.35, x * series, 1.0 - jnp.exp(-x))


def project_kernel(
    place, mine, theirs, w_query, w_input, w_gate, taps, w_recur, w_admit, rate, scale,
    query_t, decays, states, gates, ends, *, fs_count, member_rows,
):
    core = place[3]
    sent_rows = mine.shape[0] // fs_count
    first = jnp.where(core == 0, mine[...], theirs[...])
    second = jnp.where(core == 0, theirs[...], mine[...])
    rows = jnp.concatenate([first, second], axis=0)

    def project(weight):
        return jnp.dot(rows, weight[...], preferred_element_type=jnp.float32)

    def piece(value, t, f):
        at = (t * fs_count + f) * sent_rows
        return value[at : at + member_rows]

    def in_order(value):
        pieces = [piece(value, t, f) for f in range(fs_count) for t in range(2)]
        return jnp.concatenate(pieces, axis=0)

    query = project(w_query)
    query = jnp.concatenate([piece(query, t, f) for t in range(2) for f in range(fs_count)], axis=0)
    query_t[...] = query.astype(jnp.bfloat16).T

    gate = in_order(project(w_gate).astype(jnp.bfloat16)).astype(jnp.float32)
    gates[...] = jax.nn.gelu(gate)

    lru_all = project(w_input).astype(jnp.bfloat16).astype(jnp.float32)
    margin = sent_rows - member_rows
    before = lru_all[2 * fs_count * sent_rows - margin :]
    padded = jnp.concatenate([before, in_order(lru_all)], axis=0)
    count = taps.shape[0]
    conv_sum = padded[margin:] * taps[count - 1 : count, :]
    for back in range(1, count):
        moved = pltpu.roll(padded, back, 0)[margin:]
        conv_sum = conv_sum + moved * taps[count - 1 - back : count - back, :]
    conv_out = conv_sum.astype(jnp.bfloat16)

    def gate_of(weight):
        zero = jnp.zeros(weight.shape[1:], weight.dtype)
        whole = jnp.concatenate(
            [
                jnp.concatenate([weight[0], zero], axis=1),
                jnp.concatenate([zero, weight[1]], axis=1),
            ],
            axis=0,
        )
        return jax.nn.sigmoid(jnp.dot(conv_out, whole, preferred_element_type=jnp.float32))

    log_decay = -gate_of(w_recur) * rate[...] * scale[...]
    decay = jnp.exp(log_decay)
    drive = jnp.sqrt(one_minus_exp(-2.0 * log_decay)) * gate_of(w_admit) * conv_out.astype(jnp.float32)

    row = lax.broadcasted_iota(jnp.int32, decay.shape, 0)
    by = 1
    while by < decay.shape[0]:
        inside = row >= by
        decay_before = jnp.where(inside, pltpu.roll(decay, by, 0), 1.0)
        state_before = jnp.where(inside, pltpu.roll(drive, by, 0), 0.0)
        drive = decay * state_before + drive
        decay = decay * decay_before
        by *= 2
    decays[...] = decay
    states[...] = drive
    last = decay.shape[0] - 1
    ends[0:1, :] = decay[last:]
    ends[1:2, :] = drive[last:]


def project(place, mine, theirs, weights, taps, w_recur, w_admit, rate, scale, fs_count, rows):
    channels = scale.shape[1]
    block = jax.ShapeDtypeStruct(scale.shape, jnp.float32)
    return pl.pallas_call(
        functools.partial(project_kernel, fs_count=fs_count, member_rows=rows),
        out_shape=(
            jax.ShapeDtypeStruct((channels, scale.shape[0]), jnp.bfloat16),
            block,
            block,
            block,
            jax.ShapeDtypeStruct((2, channels), jnp.float32),
        ),
        in_specs=[smem()] + [vmem()] * 10,
        out_specs=(vmem(),) * 5,
        cost_estimate=pl.CostEstimate(
            flops=2 * scale.shape[0] * mine.shape[1] * 3 * channels,
            bytes_accessed=4 << 20,
            transcendentals=1 << 18,
        ),
        name="project",
    )(place, mine, theirs, *weights, taps, w_recur, w_admit, rate, scale)


def states_kernel(
    place, pieces, start, decays, states, gates, mine, theirs, *, y_count, fs_count, member_rows
):
    here, core = (place[0] * y_count + place[1], place[3])

    count = pieces.shape[0]
    decay, state = (pieces[:, 0, :], pieces[:, 1, :])
    row = lax.broadcasted_iota(jnp.int32, decay.shape, 0)
    decay = jnp.where(row < here, decay, 1.0)
    state = jnp.where(row < here, state, 0.0)
    by = 1
    while by < count:
        inside = row >= by
        decay_before = jnp.where(inside, pltpu.roll(decay, by, 0), 1.0)
        state_before = jnp.where(inside, pltpu.roll(state, by, 0), 0.0)
        state = decay * state_before + state
        decay = decay * decay_before
        by *= 2
    entering = decay[count - 1 :] * start[...] + state[count - 1 :]
    out = ((states[...] + decays[...] * entering) * gates[...]).astype(jnp.bfloat16)
    for f in range(fs_count):
        at = 2 * f * member_rows
        even = out[at : at + member_rows]
        odd = out[at + member_rows : at + 2 * member_rows]
        mine[f * member_rows : (f + 1) * member_rows] = jnp.where(core == 0, even, odd)
        theirs[f * member_rows : (f + 1) * member_rows] = jnp.where(core == 0, odd, even)


def final_states(place, pieces, start, decays, states, gates, y_count, fs_count, member_rows):
    half = jax.ShapeDtypeStruct((fs_count * member_rows, decays.shape[1]), jnp.bfloat16)
    return pl.pallas_call(
        functools.partial(
            states_kernel, y_count=y_count, fs_count=fs_count, member_rows=member_rows
        ),
        out_shape=(half, half),
        in_specs=[smem()] + [vmem()] * 5,
        out_specs=(vmem(), vmem()),
        cost_estimate=pl.CostEstimate(
            flops=1 << 20, bytes_accessed=1 << 19, transcendentals=0
        ),
        name="final_states",
    )(place, pieces, start, decays, states, gates)


def attention_kernel(
    place, group, kv, packed, query, peak, total, values, value_t, *, block_rows, part_rows
):
    heads, size, rows = group.shape
    chunk_keys = kv.shape[1]
    z, y, member = (place[0], place[1], place[2])
    scale = (size // 2) ** (-0.5) * log2_e
    line = lax.broadcasted_iota(jnp.int32, (size, rows), 0)
    for h in range(heads):
        whole = group[h]
        zero = jnp.zeros_like(whole)
        query[2 * h] = jnp.where(line < size // 2, whole, zero)
        query[2 * h + 1] = jnp.where(line < size // 2, zero, whole)
    peak[...] = jnp.full(peak.shape, far_below, jnp.float32)
    total[...] = jnp.zeros(total.shape, jnp.float32)
    values[...] = jnp.zeros(values.shape, jnp.float32)

    def visible_keys():
        row = lax.broadcasted_iota(jnp.int32, (chunk_keys, rows), 0)
        lane = lax.broadcasted_iota(jnp.int32, (chunk_keys, rows), 1)
        key_pos = (row // part_rows) * block_rows + member * part_rows + row % part_rows
        half, piece = (rows // 2, part_rows // 2)
        inside = (lane % half) // piece * part_rows + lane // half * piece + lane % piece
        return key_pos <= inside + y * block_rows

    def one_chunk(at, masked):
        both = kv[at]
        keys = both[:, :size]
        value_t[...] = both[:, size:].T
        visible = visible_keys() if masked else None

        def scores_of(i):
            found = jnp.dot(keys, query[i], preferred_element_type=jnp.float32) * scale
            return jnp.where(visible, found, far_below) if masked else found

        scores = scores_of(0)
        for i in range(2 * heads):
            following = scores_of(i + 1) if i + 1 < 2 * heads else None
            old = peak[i]
            now = jnp.maximum(old, jnp.max(scores, axis=0, keepdims=True))
            expos = jnp.exp2(scores - now)
            if masked:
                expos = jnp.where(visible, expos, 0.0)
            fade = jnp.exp2(old - now)
            peak[i] = now
            total[i] = total[i] * fade + jnp.sum(expos, axis=0, keepdims=True)
            values[i] = values[i] * fade + jnp.dot(
                value_t[...], expos.astype(jnp.bfloat16), preferred_element_type=jnp.float32
            )
            scores = following

    one_chunk(z, True)

    def earlier(at, _):
        one_chunk(at, False)
        return 0

    lax.fori_loop(0, z, earlier, 0)

    half = rows // 2
    line = lax.broadcasted_iota(jnp.int32, (16, rows), 0)
    for h in range(heads):
        tail = jnp.zeros((16, rows), jnp.float32)
        for m in range(2):
            amount = total[2 * h + m]
            some = amount > 0.0
            safe = jnp.where(some, amount, 1.0)
            shares = (values[2 * h + m] * jnp.where(some, 1.0 / safe, 0.0)).astype(jnp.bfloat16)
            level = jnp.where(some, peak[2 * h + m] + jnp.log2(safe), far_below)
            coarse = level.astype(jnp.bfloat16).astype(jnp.float32)
            tail = jnp.where(line == 2 * m, coarse, tail)
            tail = jnp.where(line == 2 * m + 1, level - coarse, tail)
            for t in range(2):
                packed[h, t, m * size : (m + 1) * size, :] = shares[:, t * half : (t + 1) * half]
        rounded = tail.astype(jnp.bfloat16)
        for t in range(2):
            packed[h, t, 2 * size : 2 * size + 16, :] = rounded[:, t * half : (t + 1) * half]


def attention(place, group, kv, block_rows, part_rows):
    heads, size, rows = group.shape
    z_count, chunk_keys, _ = kv.shape
    keys = chunk_keys * z_count
    return pl.pallas_call(
        functools.partial(attention_kernel, block_rows=block_rows, part_rows=part_rows),
        out_shape=jax.ShapeDtypeStruct((heads, 2, 2 * size + 16, rows // 2), jnp.bfloat16),
        in_specs=[smem(), vmem(), vmem()],
        out_specs=vmem(),
        scratch_shapes=[
            pltpu.VMEM((2 * heads, size, rows), jnp.bfloat16),
            pltpu.VMEM((2 * heads, 1, rows), jnp.float32),
            pltpu.VMEM((2 * heads, 1, rows), jnp.float32),
            pltpu.VMEM((2 * heads, size, rows), jnp.float32),
            pltpu.VMEM((size, chunk_keys), jnp.bfloat16),
        ],
        cost_estimate=pl.CostEstimate(
            flops=4 * 2 * heads * rows * keys * size,
            bytes_accessed=4 << 20,
            transcendentals=2 * heads * rows * keys,
        ),
        name="attention",
    )(place, group, kv)


def finish_kernel(place, lam, lam_theirs, parts, gain, lru_mine, lru_theirs, w_mine, w_theirs, out):
    count, _, lines, _ = parts.shape
    size = (lines - 16) // 2
    core = place[3]

    def head_output(owner, factor):
        joined = []
        for m in range(2):
            tails = [parts[i, owner, 2 * size :, :].astype(jnp.float32) for i in range(count)]
            levels = [t[2 * m : 2 * m + 1] + t[2 * m + 1 : 2 * m + 2] for t in tails]
            top = functools.reduce(jnp.maximum, levels)
            shares = [jnp.exp2(level - top) for level in levels]
            inverse = 1.0 / functools.reduce(jnp.add, shares)
            weighted = [
                parts[i, owner, m * size : (m + 1) * size, :].astype(jnp.float32)
                * (shares[i] * inverse)
                for i in range(count)
            ]
            joined.append(functools.reduce(jnp.add, weighted))
        diff = joined[0] - factor * joined[1]
        level = lax.rsqrt(jnp.mean(diff * diff, axis=0, keepdims=True) + head_eps)
        return ((diff * level).T * gain[...]).astype(jnp.bfloat16)

    mine = jnp.concatenate([lru_mine[...], head_output(core, lam[0])], axis=1)
    theirs = jnp.concatenate([lru_theirs[...], head_output(1 - core, lam_theirs[0])], axis=1)
    result = jnp.dot(mine, w_mine[...], preferred_element_type=jnp.float32)
    result = result + jnp.dot(theirs, w_theirs[...], preferred_element_type=jnp.float32)
    out[...] = result.astype(jnp.bfloat16)


def finish(place, lam, lam_theirs, parts, gain, lru_mine, lru_theirs, w_mine, w_theirs):
    rows, wide = (lru_mine.shape[0], w_mine.shape[1])
    return pl.pallas_call(
        finish_kernel,
        out_shape=jax.ShapeDtypeStruct((rows, wide), jnp.bfloat16),
        in_specs=[smem()] * 3 + [vmem()] * 6,
        out_specs=vmem(),
        cost_estimate=pl.CostEstimate(
            flops=2 * rows * wide * 512, bytes_accessed=3 << 20, transcendentals=rows * 16
        ),
        name="finish",
    )(place, lam, lam_theirs, parts, gain, lru_mine, lru_theirs, w_mine, w_theirs)


def body(
    tokens,
    norm_gain,
    query_weight,
    w_key,
    w_value,
    w_input,
    w_gate,
    conv_kernel,
    w_recur,
    w_admit,
    decay_param,
    decay_scale,
    init_state,
    diff_lambda,
    head_gain,
    w_out_lru,
    w_out_attn,
):
    member_rows, wide = tokens.shape
    fs_count = lax.axis_size("fs")
    tp_count = lax.axis_size("tp")
    row_count = member_rows * fs_count * tp_count
    share_rows = member_rows * tp_count
    member = lax.axis_index("fs")
    core = lax.axis_index("tp")
    z_count, z = (lax.axis_size("sp_0"), lax.axis_index("sp_0"))
    y_count, y = (lax.axis_size("sp_1"), lax.axis_index("sp_1"))

    floats = tokens.astype(jnp.float32)
    normed = (
        floats * lax.rsqrt(jnp.mean(floats * floats, axis=1, keepdims=True) + input_eps) * norm_gain
    ).astype(jnp.bfloat16)

    margin = 8
    before_rows = passed_along(normed[member_rows - margin :], SP, 1)

    chip_rows = lax.all_gather(normed, "tp", axis=0, tiled=True)
    kv_here = jnp.concatenate(
        [
            jnp.dot(chip_rows, weight, preferred_element_type=jnp.float32).astype(jnp.bfloat16)
            for weight in (w_key, w_value)
        ],
        axis=1,
    )
    kv_here, normed, before_rows = lax.optimization_barrier((kv_here, normed, before_rows))
    everyone = from_everyone(kv_here, SP)
    everyone = everyone.reshape(z_count, y_count * share_rows, kv_here.shape[1])

    sent = jnp.concatenate([normed, before_rows], axis=0)
    mine = lax.all_gather(sent, "fs", axis=0, tiled=True)
    swap = [(0, 1), (1, 0)]
    theirs = lax.ppermute(mine, "tp", swap)

    place = jnp.stack([z, y, member, core]).astype(jnp.int32)
    rate = gate_scale * jax.nn.softplus(-decay_param)
    query_t, decays, states, gates, ends = project(
        place,
        mine,
        theirs,
        (query_weight, w_input, w_gate),
        conv_kernel,
        w_recur,
        w_admit,
        rate[None],
        decay_scale,
        fs_count,
        member_rows,
    )

    group = lax.all_gather(query_t, "fs")

    everywhere = from_everyone(ends, SP)

    w_mine = jnp.concatenate([w_out_lru, w_out_attn], axis=0)
    w_theirs = lax.ppermute(w_mine, "tp", swap)
    lam_theirs = lax.ppermute(diff_lambda, "tp", swap)

    carried = attention(place, group, everyone, row_count, share_rows)
    lines, half_rows = carried.shape[2:]
    carried = carried.reshape(fs_count * tp_count, lines, half_rows)
    packed = lax.all_to_all(carried, ("fs", "tp"), split_axis=0, concat_axis=0, tiled=True)
    packed = packed.reshape(fs_count, tp_count, lines, half_rows)

    lru_mine, lru_other = final_states(
        place, everywhere, init_state[None], decays, states, gates, y_count, fs_count, member_rows
    )
    lru_theirs = lax.ppermute(lru_other, "tp", swap)

    partial = finish(
        place,
        diff_lambda,
        lam_theirs,
        packed,
        head_gain[None],
        lru_mine,
        lru_theirs,
        w_mine,
        w_theirs,
    )
    partial = partial.reshape(fs_count, member_rows, wide)
    arrived = lax.all_to_all(partial, "fs", split_axis=0, concat_axis=0, tiled=True)
    return arrived.astype(jnp.float32).sum(axis=0).astype(jnp.bfloat16)


def solution(mesh):
    torus = Mesh(
        mesh.devices.reshape(8, 8, mesh.shape["fs"], mesh.shape["tp"]), ("sp_0", "sp_1", "fs", "tp")
    )

    return jax.shard_map(
        body,
        mesh=torus,
        in_specs=(
            P(SP_FS_TP, None),
            P(),
            P(None, ("fs", "tp")),
            P(None, "tp"),
            P(None, "tp"),
            P(None, ("fs", "tp")),
            P(None, ("fs", "tp")),
            P(None, ("fs", "tp")),
            P(("fs", "tp"), None, None),
            P(("fs", "tp"), None, None),
            P(("fs", "tp")),
            P(SP, ("fs", "tp")),
            P(("fs", "tp")),
            P(("fs", "tp")),
            P(),
            P(("fs", "tp"), None),
            P(("fs", "tp"), None),
        ),
        out_specs=P(SP_FS_TP, None),
        check_vma=False,
    )
```

```python
import functools

import jax
import jax.numpy as jnp
from jax import lax
from jax.experimental import pallas as pl
from jax.experimental.pallas import tpu as pltpu
from jax.sharding import Mesh
from jax.sharding import PartitionSpec as P


SP = ("sp_0", "sp_1")
SP_FS_TP = ("sp_0", "sp_1", "fs", "tp")


gate_scale = 8.0
input_eps = 1e-06
head_eps = 1e-05
far_below = -1e30
log2_e = 1.4426950408889634


def from_everyone(value, axis):
    copies = jnp.broadcast_to(value, (lax.axis_size(axis), *value.shape))
    return lax.all_to_all(copies, axis, split_axis=0, concat_axis=0, tiled=True)


def passed_along(value, axis, by):
    devices = lax.axis_size(axis)
    pairs = [(i, i + by) for i in range(devices) if 0 <= i + by < devices]
    return lax.ppermute(value, axis, pairs)


def pair_combine(earlier, later):
    decay_early, state_early = earlier
    decay_late, state_late = later
    return (decay_early * decay_late, decay_late * state_early + state_late)


def vmem():
    return pl.BlockSpec(memory_space=pltpu.VMEM)


def smem():
    return pl.BlockSpec(memory_space=pltpu.SMEM)


def one_minus_exp(x):
    series = jnp.full_like(x, 1.0)
    for k in range(7, 1, -1):
        series = 1.0 - series * x * (1.0 / k)
    return jnp.where(x < 0.35, x * series, 1.0 - jnp.exp(-x))


def project_kernel(
    place, mine, theirs, w_query, w_input, w_gate, taps, w_recur, w_admit, rate, scale,
    query_t, decays, states, gates, ends, *, fs_count, member_rows,
):
    core = place[3]
    sent_rows = mine.shape[0] // fs_count
    first = jnp.where(core == 0, mine[...], theirs[...])
    second = jnp.where(core == 0, theirs[...], mine[...])
    rows = jnp.concatenate([first, second], axis=0)

    def project(weight):
        return jnp.dot(rows, weight[...], preferred_element_type=jnp.float32)

    def piece(value, t, f):
        at = (t * fs_count + f) * sent_rows
        return value[at : at + member_rows]

    def in_order(value):
        pieces = [piece(value, t, f) for f in range(fs_count) for t in range(2)]
        return jnp.concatenate(pieces, axis=0)

    query = project(w_query)
    query = jnp.concatenate([piece(query, t, f) for t in range(2) for f in range(fs_count)], axis=0)
    query_t[...] = query.astype(jnp.bfloat16).T

    gate = in_order(project(w_gate).astype(jnp.bfloat16)).astype(jnp.float32)
    gates[...] = jax.nn.gelu(gate)

    lru_all = project(w_input).astype(jnp.bfloat16).astype(jnp.float32)
    margin = sent_rows - member_rows
    before = lru_all[2 * fs_count * sent_rows - margin :]
    padded = jnp.concatenate([before, in_order(lru_all)], axis=0)
    count = taps.shape[0]
    conv_sum = padded[margin:] * taps[count - 1 : count, :]
    for back in range(1, count):
        moved = pltpu.roll(padded, back, 0)[margin:]
        conv_sum = conv_sum + moved * taps[count - 1 - back : count - back, :]
    conv_out = conv_sum.astype(jnp.bfloat16)

    def gate_of(weight):
        zero = jnp.zeros(weight.shape[1:], weight.dtype)
        whole = jnp.concatenate(
            [
                jnp.concatenate([weight[0], zero], axis=1),
                jnp.concatenate([zero, weight[1]], axis=1),
            ],
            axis=0,
        )
        return jax.nn.sigmoid(jnp.dot(conv_out, whole, preferred_element_type=jnp.float32))

    log_decay = -gate_of(w_recur) * rate[...] * scale[...]
    decay = jnp.exp(log_decay)
    drive = jnp.sqrt(one_minus_exp(-2.0 * log_decay)) * gate_of(w_admit) * conv_out.astype(jnp.float32)

    row = lax.broadcasted_iota(jnp.int32, decay.shape, 0)
    by = 1
    while by < decay.shape[0]:
        inside = row >= by
        decay_before = jnp.where(inside, pltpu.roll(decay, by, 0), 1.0)
        state_before = jnp.where(inside, pltpu.roll(drive, by, 0), 0.0)
        drive = decay * state_before + drive
        decay = decay * decay_before
        by *= 2
    decays[...] = decay
    states[...] = drive
    last = decay.shape[0] - 1
    ends[0:1, :] = decay[last:]
    ends[1:2, :] = drive[last:]


def project(place, mine, theirs, weights, taps, w_recur, w_admit, rate, scale, fs_count, rows):
    channels = scale.shape[1]
    block = jax.ShapeDtypeStruct(scale.shape, jnp.float32)
    return pl.pallas_call(
        functools.partial(project_kernel, fs_count=fs_count, member_rows=rows),
        out_shape=(
            jax.ShapeDtypeStruct((channels, scale.shape[0]), jnp.bfloat16),
            block,
            block,
            block,
            jax.ShapeDtypeStruct((2, channels), jnp.float32),
        ),
        in_specs=[smem()] + [vmem()] * 10,
        out_specs=(vmem(),) * 5,
        cost_estimate=pl.CostEstimate(
            flops=2 * scale.shape[0] * mine.shape[1] * 3 * channels,
            bytes_accessed=4 << 20,
            transcendentals=1 << 18,
        ),
        name="project",
    )(place, mine, theirs, *weights, taps, w_recur, w_admit, rate, scale)


def states_kernel(
    place, near, far, start, decays, states, gates, mine, theirs, *, fs_count, member_rows
):
    z, y, core = (place[0], place[1], place[3])

    def before(pieces, here):
        decay, state = (jnp.ones_like(pieces[0, 0:1]), jnp.zeros_like(pieces[0, 1:2]))
        for k in range(pieces.shape[0]):
            passed = k < here
            new_decay, new_state = pair_combine((decay, state), (pieces[k, 0:1], pieces[k, 1:2]))
            decay = jnp.where(passed, new_decay, decay)
            state = jnp.where(passed, new_state, state)
        return decay, state

    decay, state = pair_combine(before(far, z), before(near, y))
    entering = decay * start[...] + state
    out = ((states[...] + decays[...] * entering) * gates[...]).astype(jnp.bfloat16)
    for f in range(fs_count):
        at = 2 * f * member_rows
        even = out[at : at + member_rows]
        odd = out[at + member_rows : at + 2 * member_rows]
        mine[f * member_rows : (f + 1) * member_rows] = jnp.where(core == 0, even, odd)
        theirs[f * member_rows : (f + 1) * member_rows] = jnp.where(core == 0, odd, even)


def final_states(place, near, far, start, decays, states, gates, fs_count, member_rows):
    half = jax.ShapeDtypeStruct((fs_count * member_rows, decays.shape[1]), jnp.bfloat16)
    return pl.pallas_call(
        functools.partial(states_kernel, fs_count=fs_count, member_rows=member_rows),
        out_shape=(half, half),
        in_specs=[smem()] + [vmem()] * 6,
        out_specs=(vmem(), vmem()),
        cost_estimate=pl.CostEstimate(
            flops=1 << 20, bytes_accessed=1 << 19, transcendentals=0
        ),
        name="final_states",
    )(place, near, far, start, decays, states, gates)


def attention_kernel(
    place, *refs, block_rows, part_rows
):
    group = refs[:-7]
    kv, packed, query, peak, total, values, value_t = refs[-7:]
    heads = len(group)
    size, rows = group[0].shape
    chunk_keys = kv.shape[1]
    z, y, member = (place[0], place[1], place[2])
    scale = (size // 2) ** (-0.5) * log2_e
    line = lax.broadcasted_iota(jnp.int32, (size, rows), 0)
    for h in range(heads):
        whole = group[h][...]
        zero = jnp.zeros_like(whole)
        query[2 * h] = jnp.where(line < size // 2, whole, zero)
        query[2 * h + 1] = jnp.where(line < size // 2, zero, whole)
    peak[...] = jnp.full(peak.shape, far_below, jnp.float32)
    total[...] = jnp.zeros(total.shape, jnp.float32)
    values[...] = jnp.zeros(values.shape, jnp.float32)

    def visible_keys():
        row = lax.broadcasted_iota(jnp.int32, (chunk_keys, rows), 0)
        lane = lax.broadcasted_iota(jnp.int32, (chunk_keys, rows), 1)
        key_pos = (row // part_rows) * block_rows + member * part_rows + row % part_rows
        half, piece = (rows // 2, part_rows // 2)
        inside = (lane % half) // piece * part_rows + lane // half * piece + lane % piece
        return key_pos <= inside + y * block_rows

    def one_chunk(at, masked):
        both = kv[at]
        keys = both[:, :size]
        value_t[...] = both[:, size:].T
        visible = visible_keys() if masked else None

        def scores_of(i):
            found = jnp.dot(keys, query[i], preferred_element_type=jnp.float32) * scale
            return jnp.where(visible, found, far_below) if masked else found

        scores = scores_of(0)
        for i in range(2 * heads):
            following = scores_of(i + 1) if i + 1 < 2 * heads else None
            old = peak[i]
            now = jnp.maximum(old, jnp.max(scores, axis=0, keepdims=True))
            expos = jnp.exp2(scores - now)
            if masked:
                expos = jnp.where(visible, expos, 0.0)
            fade = jnp.exp2(old - now)
            peak[i] = now
            total[i] = total[i] * fade + jnp.sum(expos, axis=0, keepdims=True)
            values[i] = values[i] * fade + jnp.dot(
                value_t[...], expos.astype(jnp.bfloat16), preferred_element_type=jnp.float32
            )
            scores = following

    one_chunk(z, True)

    def earlier(at, _):
        one_chunk(at, False)
        return 0

    lax.fori_loop(0, z, earlier, 0)

    half = rows // 2
    line = lax.broadcasted_iota(jnp.int32, (16, rows), 0)
    for h in range(heads):
        tail = jnp.zeros((16, rows), jnp.float32)
        for m in range(2):
            amount = total[2 * h + m]
            some = amount > 0.0
            safe = jnp.where(some, amount, 1.0)
            shares = (values[2 * h + m] * jnp.where(some, 1.0 / safe, 0.0)).astype(jnp.bfloat16)
            level = jnp.where(some, peak[2 * h + m] + jnp.log2(safe), far_below)
            coarse = level.astype(jnp.bfloat16).astype(jnp.float32)
            tail = jnp.where(line == 2 * m, coarse, tail)
            tail = jnp.where(line == 2 * m + 1, level - coarse, tail)
            for t in range(2):
                packed[member ^ h, t, m * size : (m + 1) * size, :] = shares[:, t * half : (t + 1) * half]
        rounded = tail.astype(jnp.bfloat16)
        for t in range(2):
            packed[member ^ h, t, 2 * size : 2 * size + 16, :] = rounded[:, t * half : (t + 1) * half]


def attention(place, group, kv, block_rows, part_rows):
    heads = len(group)
    size, rows = group[0].shape
    z_count, chunk_keys, _ = kv.shape
    keys = chunk_keys * z_count
    return pl.pallas_call(
        functools.partial(attention_kernel, block_rows=block_rows, part_rows=part_rows),
        out_shape=jax.ShapeDtypeStruct((heads, 2, 2 * size + 16, rows // 2), jnp.bfloat16),
        in_specs=[smem()] + [vmem()] * (heads + 1),
        out_specs=vmem(),
        scratch_shapes=[
            pltpu.VMEM((2 * heads, size, rows), jnp.bfloat16),
            pltpu.VMEM((2 * heads, 1, rows), jnp.float32),
            pltpu.VMEM((2 * heads, 1, rows), jnp.float32),
            pltpu.VMEM((2 * heads, size, rows), jnp.float32),
            pltpu.VMEM((size, chunk_keys), jnp.bfloat16),
        ],
        cost_estimate=pl.CostEstimate(
            flops=4 * 2 * heads * rows * keys * size,
            bytes_accessed=4 << 20,
            transcendentals=2 * heads * rows * keys,
        ),
        name="attention",
    )(place, *group, kv)


def finish_kernel(place, lam, lam_theirs, parts, gain, lru_mine, lru_theirs, w_mine, w_theirs, out):
    count, _, lines, _ = parts.shape
    size = (lines - 16) // 2
    core = place[3]

    def head_output(owner, factor):
        joined = []
        for m in range(2):
            tails = [parts[i, owner, 2 * size :, :].astype(jnp.float32) for i in range(count)]
            levels = [t[2 * m : 2 * m + 1] + t[2 * m + 1 : 2 * m + 2] for t in tails]
            top = functools.reduce(jnp.maximum, levels)
            shares = [jnp.exp2(level - top) for level in levels]
            inverse = 1.0 / functools.reduce(jnp.add, shares)
            weighted = [
                parts[i, owner, m * size : (m + 1) * size, :].astype(jnp.float32)
                * (shares[i] * inverse)
                for i in range(count)
            ]
            joined.append(functools.reduce(jnp.add, weighted))
        diff = joined[0] - factor * joined[1]
        level = lax.rsqrt(jnp.mean(diff * diff, axis=0, keepdims=True) + head_eps)
        return ((diff * level).T * gain[...]).astype(jnp.bfloat16)

    mine = jnp.concatenate([lru_mine[...], head_output(core, lam[0])], axis=1)
    theirs = jnp.concatenate([lru_theirs[...], head_output(1 - core, lam_theirs[0])], axis=1)
    result = jnp.dot(mine, w_mine[...], preferred_element_type=jnp.float32)
    result = result + jnp.dot(theirs, w_theirs[...], preferred_element_type=jnp.float32)
    out[...] = result.astype(jnp.bfloat16)


def finish(place, lam, lam_theirs, parts, gain, lru_mine, lru_theirs, w_mine, w_theirs):
    rows, wide = (lru_mine.shape[0], w_mine.shape[1])
    return pl.pallas_call(
        finish_kernel,
        out_shape=jax.ShapeDtypeStruct((rows, wide), jnp.bfloat16),
        in_specs=[smem()] * 3 + [vmem()] * 6,
        out_specs=vmem(),
        cost_estimate=pl.CostEstimate(
            flops=2 * rows * wide * 512, bytes_accessed=3 << 20, transcendentals=rows * 16
        ),
        name="finish",
    )(place, lam, lam_theirs, parts, gain, lru_mine, lru_theirs, w_mine, w_theirs)


def body(
    tokens,
    norm_gain,
    query_weight,
    w_key,
    w_value,
    w_input,
    w_gate,
    conv_kernel,
    w_recur,
    w_admit,
    decay_param,
    decay_scale,
    init_state,
    diff_lambda,
    head_gain,
    w_out_lru,
    w_out_attn,
):
    member_rows, wide = tokens.shape
    fs_count = lax.axis_size("fs")
    tp_count = lax.axis_size("tp")
    row_count = member_rows * fs_count * tp_count
    share_rows = member_rows * tp_count
    member = lax.axis_index("fs")
    core = lax.axis_index("tp")
    z = lax.axis_index("sp_0")
    y_count, y = (lax.axis_size("sp_1"), lax.axis_index("sp_1"))

    floats = tokens.astype(jnp.float32)
    normed = (
        floats * lax.rsqrt(jnp.mean(floats * floats, axis=1, keepdims=True) + input_eps) * norm_gain
    ).astype(jnp.bfloat16)

    margin = 8
    before_rows = passed_along(normed[member_rows - margin :], SP, 1)

    chip_rows = lax.all_gather(normed, "tp", axis=0, tiled=True)
    kv_here = jnp.concatenate(
        [
            jnp.dot(chip_rows, weight, preferred_element_type=jnp.float32).astype(jnp.bfloat16)
            for weight in (w_key, w_value)
        ],
        axis=1,
    )
    kv_here, normed, before_rows = lax.optimization_barrier((kv_here, normed, before_rows))
    chunk = from_everyone(kv_here, "sp_1").reshape(y_count * share_rows, kv_here.shape[1])
    everyone = from_everyone(chunk, "sp_0")

    sent = jnp.concatenate([normed, before_rows], axis=0)
    mine = lax.all_gather(sent, "fs", axis=0, tiled=True)
    swap = [(0, 1), (1, 0)]
    theirs = lax.ppermute(mine, "tp", swap)

    place = jnp.stack([z, y, member, core]).astype(jnp.int32)
    rate = gate_scale * jax.nn.softplus(-decay_param)
    query_t, decays, states, gates, ends = project(
        place,
        mine,
        theirs,
        (query_weight, w_input, w_gate),
        conv_kernel,
        w_recur,
        w_admit,
        rate[None],
        decay_scale,
        fs_count,
        member_rows,
    )

    group = [query_t]
    for by in range(1, fs_count):
        group.append(lax.ppermute(query_t, "fs", [(i, i ^ by) for i in range(fs_count)]))

    near = lax.all_gather(ends, "sp_1")
    row = (near[0, 0], near[0, 1])
    for k in range(1, y_count):
        row = pair_combine(row, (near[k, 0], near[k, 1]))
    far = from_everyone(jnp.stack(row), "sp_0")

    w_mine = jnp.concatenate([w_out_lru, w_out_attn], axis=0)
    w_theirs = lax.ppermute(w_mine, "tp", swap)
    lam_theirs = lax.ppermute(diff_lambda, "tp", swap)

    carried = attention(place, group, everyone, row_count, share_rows)
    lines, half_rows = carried.shape[2:]
    carried = carried.reshape(fs_count * tp_count, lines, half_rows)
    packed = lax.all_to_all(carried, ("fs", "tp"), split_axis=0, concat_axis=0, tiled=True)
    packed = packed.reshape(fs_count, tp_count, lines, half_rows)

    lru_mine, lru_other = final_states(
        place, near, far, init_state[None], decays, states, gates, fs_count, member_rows
    )
    lru_theirs = lax.ppermute(lru_other, "tp", swap)

    partial = finish(
        place,
        diff_lambda,
        lam_theirs,
        packed,
        head_gain[None],
        lru_mine,
        lru_theirs,
        w_mine,
        w_theirs,
    )
    partial = partial.reshape(fs_count, member_rows, wide)
    arrived = lax.all_to_all(partial, "fs", split_axis=0, concat_axis=0, tiled=True)
    return arrived.astype(jnp.float32).sum(axis=0).astype(jnp.bfloat16)


def solution(mesh):
    torus = Mesh(
        mesh.devices.reshape(8, 8, mesh.shape["fs"], mesh.shape["tp"]), ("sp_0", "sp_1", "fs", "tp")
    )

    return jax.shard_map(
        body,
        mesh=torus,
        in_specs=(
            P(SP_FS_TP, None),
            P(),
            P(None, ("fs", "tp")),
            P(None, "tp"),
            P(None, "tp"),
            P(None, ("fs", "tp")),
            P(None, ("fs", "tp")),
            P(None, ("fs", "tp")),
            P(("fs", "tp"), None, None),
            P(("fs", "tp"), None, None),
            P(("fs", "tp")),
            P(SP, ("fs", "tp")),
            P(("fs", "tp")),
            P(("fs", "tp")),
            P(),
            P(("fs", "tp"), None),
            P(("fs", "tp"), None),
        ),
        out_specs=P(SP_FS_TP, None),
        check_vma=False,
    )
```

```python
import functools

import jax
import jax.numpy as jnp
from jax import lax
from jax.experimental import pallas as pl
from jax.experimental.pallas import tpu as pltpu
from jax.sharding import Mesh
from jax.sharding import PartitionSpec as P


SP = ("sp_0", "sp_1")
SP_FS_TP = ("sp_0", "sp_1", "fs", "tp")


gate_scale = 8.0
input_eps = 1e-06
head_eps = 1e-05
far_below = -1e30
log2_e = 1.4426950408889634


def from_everyone(value, axis):
    copies = jnp.broadcast_to(value, (lax.axis_size(axis), *value.shape))
    return lax.all_to_all(copies, axis, split_axis=0, concat_axis=0, tiled=True)


def passed_along(value, axis, by):
    devices = lax.axis_size(axis)
    pairs = [(i, i + by) for i in range(devices) if 0 <= i + by < devices]
    return lax.ppermute(value, axis, pairs)


def vmem():
    return pl.BlockSpec(memory_space=pltpu.VMEM)


def anywhere():
    return pl.BlockSpec(memory_space=pl.ANY)


def smem():
    return pl.BlockSpec(memory_space=pltpu.SMEM)


def norm_kernel(tokens, gain, out):
    floats = tokens[...].astype(jnp.float32)
    level = lax.rsqrt(jnp.mean(floats * floats, axis=1, keepdims=True) + input_eps)
    out[...] = (floats * level * gain[...]).astype(jnp.bfloat16)


def normalized(tokens, gain):
    return pl.pallas_call(
        norm_kernel,
        out_shape=jax.ShapeDtypeStruct(tokens.shape, jnp.bfloat16),
        in_specs=[vmem(), vmem()],
        out_specs=vmem(),
        cost_estimate=pl.CostEstimate(
            flops=4 * tokens.size, bytes_accessed=1 << 18, transcendentals=0
        ),
        name="normalized",
    )(tokens, gain)


def one_minus_exp(x):
    series = jnp.full_like(x, 1.0)
    for k in range(7, 1, -1):
        series = 1.0 - series * x * (1.0 / k)
    return jnp.where(x < 0.35, x * series, 1.0 - jnp.exp(-x))


def project_kernel(
    place, mine, theirs, w_query, w_input, w_gate, taps, w_recur, w_admit, rate, scale,
    query_t, decays, states, gates, ends, *, fs_count, member_rows,
):
    core = place[3]
    sent_rows = mine.shape[0] // fs_count
    first = jnp.where(core == 0, mine[...], theirs[...])
    second = jnp.where(core == 0, theirs[...], mine[...])
    rows = jnp.concatenate([first, second], axis=0)

    def project(weight):
        return jnp.dot(rows, weight[...], preferred_element_type=jnp.float32)

    def piece(value, t, f):
        at = (t * fs_count + f) * sent_rows
        return value[at : at + member_rows]

    def in_order(value):
        pieces = [piece(value, t, f) for f in range(fs_count) for t in range(2)]
        return jnp.concatenate(pieces, axis=0)

    query = project(w_query)
    query = jnp.concatenate([piece(query, t, f) for t in range(2) for f in range(fs_count)], axis=0)
    score_scale = (query.shape[1] // 2) ** (-0.5) * log2_e
    query_t[...] = (query * score_scale).astype(jnp.bfloat16).T

    gate = in_order(project(w_gate).astype(jnp.bfloat16)).astype(jnp.float32)
    gates[...] = jax.nn.gelu(gate)

    lru_all = project(w_input).astype(jnp.bfloat16).astype(jnp.float32)
    margin = sent_rows - member_rows
    before = lru_all[2 * fs_count * sent_rows - margin :]
    padded = jnp.concatenate([before, in_order(lru_all)], axis=0)
    count = taps.shape[0]
    conv_sum = padded[margin:] * taps[count - 1 : count, :]
    for back in range(1, count):
        moved = pltpu.roll(padded, back, 0)[margin:]
        conv_sum = conv_sum + moved * taps[count - 1 - back : count - back, :]
    conv_out = conv_sum.astype(jnp.bfloat16)

    def gate_of(weight):
        zero = jnp.zeros(weight.shape[1:], weight.dtype)
        whole = jnp.concatenate(
            [
                jnp.concatenate([weight[0], zero], axis=1),
                jnp.concatenate([zero, weight[1]], axis=1),
            ],
            axis=0,
        )
        return jax.nn.sigmoid(jnp.dot(conv_out, whole, preferred_element_type=jnp.float32))

    log_decay = -gate_of(w_recur) * rate[...] * scale[...]
    decay = jnp.exp(log_decay)
    drive = jnp.sqrt(one_minus_exp(-2.0 * log_decay)) * gate_of(w_admit) * conv_out.astype(jnp.float32)

    row = lax.broadcasted_iota(jnp.int32, decay.shape, 0)
    by = 1
    while by < decay.shape[0]:
        inside = row >= by
        decay_before = jnp.where(inside, pltpu.roll(decay, by, 0), 1.0)
        state_before = jnp.where(inside, pltpu.roll(drive, by, 0), 0.0)
        drive = decay * state_before + drive
        decay = decay * decay_before
        by *= 2
    decays[...] = decay
    states[...] = drive
    last = decay.shape[0] - 1
    ends[0:1, :] = decay[last:]
    ends[1:2, :] = drive[last:]


def project(place, mine, theirs, weights, taps, w_recur, w_admit, rate, scale, fs_count, rows):
    channels = scale.shape[1]
    block = jax.ShapeDtypeStruct(scale.shape, jnp.float32)
    return pl.pallas_call(
        functools.partial(project_kernel, fs_count=fs_count, member_rows=rows),
        out_shape=(
            jax.ShapeDtypeStruct((channels, scale.shape[0]), jnp.bfloat16),
            block,
            block,
            block,
            jax.ShapeDtypeStruct((2, channels), jnp.float32),
        ),
        in_specs=[smem()] + [vmem()] * 10,
        out_specs=(vmem(),) * 5,
        cost_estimate=pl.CostEstimate(
            flops=2 * scale.shape[0] * mine.shape[1] * 3 * channels,
            bytes_accessed=4 << 20,
            transcendentals=1 << 18,
        ),
        name="project",
    )(place, mine, theirs, *weights, taps, w_recur, w_admit, rate, scale)


def states_kernel(
    place, pieces, start, decays, states, gates, mine, theirs, *, y_count, fs_count, member_rows
):
    here, core = (place[0] * y_count + place[1], place[3])

    count = pieces.shape[0]
    decay, state = (pieces[:, 0, :], pieces[:, 1, :])
    row = lax.broadcasted_iota(jnp.int32, decay.shape, 0)
    decay = jnp.where(row < here, decay, 1.0)
    state = jnp.where(row < here, state, 0.0)
    by = 1
    while by < count:
        inside = row >= by
        decay_before = jnp.where(inside, pltpu.roll(decay, by, 0), 1.0)
        state_before = jnp.where(inside, pltpu.roll(state, by, 0), 0.0)
        state = decay * state_before + state
        decay = decay * decay_before
        by *= 2
    entering = decay[count - 1 :] * start[...] + state[count - 1 :]
    out = ((states[...] + decays[...] * entering) * gates[...]).astype(jnp.bfloat16)
    for f in range(fs_count):
        at = 2 * f * member_rows
        even = out[at : at + member_rows]
        odd = out[at + member_rows : at + 2 * member_rows]
        mine[f * member_rows : (f + 1) * member_rows] = jnp.where(core == 0, even, odd)
        theirs[f * member_rows : (f + 1) * member_rows] = jnp.where(core == 0, odd, even)


def final_states(place, pieces, start, decays, states, gates, y_count, fs_count, member_rows):
    half = jax.ShapeDtypeStruct((fs_count * member_rows, decays.shape[1]), jnp.bfloat16)
    return pl.pallas_call(
        functools.partial(
            states_kernel, y_count=y_count, fs_count=fs_count, member_rows=member_rows
        ),
        out_shape=(half, half),
        in_specs=[smem()] + [vmem()] * 5,
        out_specs=(vmem(), vmem()),
        cost_estimate=pl.CostEstimate(
            flops=1 << 20, bytes_accessed=1 << 19, transcendentals=0
        ),
        name="final_states",
    )(place, pieces, start, decays, states, gates)


def attention_kernel(
    place, group, kv_far, packed, query, peak, values, value_t, kv, arrivals,
    *, block_rows, part_rows,
):
    heads, size, rows = group.shape
    chunk_keys = kv.shape[1]
    z, y, member = (place[0], place[1], place[2])

    def arrival(at):
        return pltpu.make_async_copy(kv_far.at[at], kv.at[at], arrivals.at[at])

    arrival(z).start()

    def begin(at, _):
        arrival(at).start()
        return 0

    lax.fori_loop(0, z, begin, 0)
    line = lax.broadcasted_iota(jnp.int32, (size, rows), 0)
    for h in range(heads):
        whole = group[h]
        zero = jnp.zeros_like(whole)
        query[2 * h] = jnp.where(line < size // 2, whole, zero)
        query[2 * h + 1] = jnp.where(line < size // 2, zero, whole)
    peak[...] = jnp.full(peak.shape, far_below, jnp.float32)
    value_t[size:, :] = jnp.ones((16, chunk_keys), jnp.bfloat16)
    values[...] = jnp.zeros(values.shape, jnp.float32)

    def visible_keys():
        row = lax.broadcasted_iota(jnp.int32, (chunk_keys, rows), 0)
        lane = lax.broadcasted_iota(jnp.int32, (chunk_keys, rows), 1)
        key_pos = (row // part_rows) * block_rows + member * part_rows + row % part_rows
        half, piece = (rows // 2, part_rows // 2)
        inside = (lane % half) // piece * part_rows + lane // half * piece + lane % piece
        return key_pos <= inside + y * block_rows

    def one_chunk(at, masked):
        arrival(at).wait()
        both = kv[at]
        keys = both[:, :size]
        value_t[:size, :] = both[:, size:].T
        visible = visible_keys() if masked else None

        def scores_of(i):
            found = jnp.dot(keys, query[i], preferred_element_type=jnp.float32)
            return jnp.where(visible, found, far_below) if masked else found

        scores = scores_of(0)
        for i in range(2 * heads):
            following = scores_of(i + 1) if i + 1 < 2 * heads else None
            old = peak[i]
            now = jnp.maximum(old, jnp.max(scores, axis=0, keepdims=True))
            expos = jnp.exp2(scores - now)
            if masked:
                expos = jnp.where(visible, expos, 0.0)
            fade = jnp.exp2(old - now)
            peak[i] = now
            values[i] = values[i] * fade + jnp.dot(
                value_t[...], expos.astype(jnp.bfloat16), preferred_element_type=jnp.float32
            )
            scores = following

    one_chunk(z, True)

    def earlier(at, _):
        one_chunk(at, False)
        return 0

    lax.fori_loop(0, z, earlier, 0)

    half = rows // 2
    line = lax.broadcasted_iota(jnp.int32, (16, rows), 0)
    for h in range(heads):
        tail = jnp.zeros((16, rows), jnp.float32)
        for m in range(2):
            amount = values[2 * h + m, size : size + 1, :]
            some = amount > 0.0
            safe = jnp.where(some, amount, 1.0)
            shares = (values[2 * h + m, :size, :] * jnp.where(some, 1.0 / safe, 0.0)).astype(jnp.bfloat16)
            level = jnp.where(some, peak[2 * h + m] + jnp.log2(safe), far_below)
            coarse = level.astype(jnp.bfloat16).astype(jnp.float32)
            tail = jnp.where(line == 2 * m, coarse, tail)
            tail = jnp.where(line == 2 * m + 1, level - coarse, tail)
            for t in range(2):
                packed[h, t, m * size : (m + 1) * size, :] = shares[:, t * half : (t + 1) * half]
        rounded = tail.astype(jnp.bfloat16)
        for t in range(2):
            packed[h, t, 2 * size : 2 * size + 16, :] = rounded[:, t * half : (t + 1) * half]


def attention(place, group, kv, block_rows, part_rows):
    heads, size, rows = group.shape
    z_count, chunk_keys, _ = kv.shape
    keys = chunk_keys * z_count
    return pl.pallas_call(
        functools.partial(attention_kernel, block_rows=block_rows, part_rows=part_rows),
        out_shape=jax.ShapeDtypeStruct((heads, 2, 2 * size + 16, rows // 2), jnp.bfloat16),
        in_specs=[smem(), vmem(), anywhere()],
        out_specs=vmem(),
        scratch_shapes=[
            pltpu.VMEM((2 * heads, size, rows), jnp.bfloat16),
            pltpu.VMEM((2 * heads, 1, rows), jnp.float32),
            pltpu.VMEM((2 * heads, size + 16, rows), jnp.float32),
            pltpu.VMEM((size + 16, chunk_keys), jnp.bfloat16),
            pltpu.VMEM(kv.shape, kv.dtype),
            pltpu.SemaphoreType.DMA((z_count,)),
        ],
        cost_estimate=pl.CostEstimate(
            flops=4 * 2 * heads * rows * keys * size,
            bytes_accessed=4 << 20,
            transcendentals=2 * heads * rows * keys,
        ),
        name="attention",
    )(place, group, kv)


def finish_kernel(
    place, lam, lam_theirs, parts, gain, lru_mine, lru_theirs, w_mine_far, w_theirs_far, *refs,
):
    outs = refs[:-4]
    w_mine, w_theirs, whole, arrivals = refs[-4:]
    copies = [
        pltpu.make_async_copy(w_mine_far, w_mine, arrivals.at[0]),
        pltpu.make_async_copy(w_theirs_far, w_theirs, arrivals.at[1]),
    ]
    for copy in copies:
        copy.start()
    count, _, lines, _ = parts.shape
    size = (lines - 16) // 2
    core = place[3]

    def head_output(owner, factor):
        joined = []
        for m in range(2):
            tails = [parts[i, owner, 2 * size :, :].astype(jnp.float32) for i in range(count)]
            levels = [t[2 * m : 2 * m + 1] + t[2 * m + 1 : 2 * m + 2] for t in tails]
            top = functools.reduce(jnp.maximum, levels)
            shares = [jnp.exp2(level - top) for level in levels]
            inverse = 1.0 / functools.reduce(jnp.add, shares)
            weighted = [
                parts[i, owner, m * size : (m + 1) * size, :].astype(jnp.float32)
                * (shares[i] * inverse)
                for i in range(count)
            ]
            joined.append(functools.reduce(jnp.add, weighted))
        diff = joined[0] - factor * joined[1]
        level = lax.rsqrt(jnp.mean(diff * diff, axis=0, keepdims=True) + head_eps)
        return ((diff * level).T * gain[...]).astype(jnp.bfloat16)

    mine = jnp.concatenate([lru_mine[...], head_output(core, lam[0])], axis=1)
    theirs = jnp.concatenate([lru_theirs[...], head_output(1 - core, lam_theirs[0])], axis=1)
    for copy in copies:
        copy.wait()
    result = jnp.dot(mine, w_mine[...], preferred_element_type=jnp.float32)
    result = result + jnp.dot(theirs, w_theirs[...], preferred_element_type=jnp.float32)
    whole[...] = result.astype(jnp.bfloat16).reshape(whole.shape)
    for by, out in enumerate(outs):
        out[...] = whole[place[2] ^ by]


def finish(place, lam, lam_theirs, parts, gain, lru_mine, lru_theirs, w_mine, w_theirs, slots):
    rows, wide = (lru_mine.shape[0], w_mine.shape[1])
    return pl.pallas_call(
        finish_kernel,
        out_shape=(jax.ShapeDtypeStruct((rows // slots, wide), jnp.bfloat16),) * slots,
        in_specs=[smem()] * 3 + [vmem()] * 4 + [anywhere()] * 2,
        out_specs=(vmem(),) * slots,
        scratch_shapes=[
            pltpu.VMEM(w_mine.shape, w_mine.dtype),
            pltpu.VMEM(w_theirs.shape, w_theirs.dtype),
            pltpu.VMEM((slots, rows // slots, wide), jnp.bfloat16),
            pltpu.SemaphoreType.DMA((2,)),
        ],
        cost_estimate=pl.CostEstimate(
            flops=2 * rows * wide * 512, bytes_accessed=3 << 20, transcendentals=rows * 16
        ),
        name="finish",
    )(place, lam, lam_theirs, parts, gain, lru_mine, lru_theirs, w_mine, w_theirs)


def body(
    tokens,
    norm_gain,
    query_weight,
    w_key,
    w_value,
    w_input,
    w_gate,
    conv_kernel,
    w_recur,
    w_admit,
    decay_param,
    decay_scale,
    init_state,
    diff_lambda,
    head_gain,
    w_out_lru,
    w_out_attn,
):
    member_rows, _ = tokens.shape
    fs_count = lax.axis_size("fs")
    tp_count = lax.axis_size("tp")
    row_count = member_rows * fs_count * tp_count
    share_rows = member_rows * tp_count
    member = lax.axis_index("fs")
    core = lax.axis_index("tp")
    z_count, z = (lax.axis_size("sp_0"), lax.axis_index("sp_0"))
    y_count, y = (lax.axis_size("sp_1"), lax.axis_index("sp_1"))

    normed = normalized(tokens, norm_gain[None])

    margin = 8
    before_rows = passed_along(normed[member_rows - margin :], SP, 1)

    chip_rows = lax.all_gather(normed, "tp", axis=0, tiled=True)
    kv_here = jnp.concatenate(
        [
            jnp.dot(chip_rows, weight, preferred_element_type=jnp.float32).astype(jnp.bfloat16)
            for weight in (w_key, w_value)
        ],
        axis=1,
    )
    kv_here, normed = lax.optimization_barrier((kv_here, normed))
    everyone = from_everyone(kv_here, SP)
    everyone = everyone.reshape(z_count, y_count * share_rows, kv_here.shape[1])

    sent = jnp.concatenate([normed, before_rows], axis=0)
    mine = lax.all_gather(sent, "fs", axis=0, tiled=True)
    swap = [(0, 1), (1, 0)]
    theirs = lax.ppermute(mine, "tp", swap)

    place = jnp.stack([z, y, member, core]).astype(jnp.int32)
    rate = gate_scale * jax.nn.softplus(-decay_param)
    query_t, decays, states, gates, ends = project(
        place,
        mine,
        theirs,
        (query_weight, w_input, w_gate),
        conv_kernel,
        w_recur,
        w_admit,
        rate[None],
        decay_scale,
        fs_count,
        member_rows,
    )

    group = lax.all_gather(query_t, "fs")

    everywhere = from_everyone(ends, SP)

    w_mine = jnp.concatenate([w_out_lru, w_out_attn], axis=0)
    w_theirs = lax.ppermute(w_mine, "tp", swap)
    lam_theirs = lax.ppermute(diff_lambda, "tp", swap)

    carried = attention(place, group, everyone, row_count, share_rows)
    lines, half_rows = carried.shape[2:]
    carried = carried.reshape(fs_count * tp_count, lines, half_rows)
    packed = lax.all_to_all(carried, ("fs", "tp"), split_axis=0, concat_axis=0, tiled=True)
    packed = packed.reshape(fs_count, tp_count, lines, half_rows)

    lru_mine, lru_other = final_states(
        place, everywhere, init_state[None], decays, states, gates, y_count, fs_count, member_rows
    )
    lru_theirs = lax.ppermute(lru_other, "tp", swap)

    partial = finish(
        place,
        diff_lambda,
        lam_theirs,
        packed,
        head_gain[None],
        lru_mine,
        lru_theirs,
        w_mine,
        w_theirs,
        fs_count,
    )
    mixed = partial[0].astype(jnp.float32)
    for by in (2, 1, 3):
        pairs = [(i, i ^ by) for i in range(fs_count)]
        mixed = mixed + lax.ppermute(partial[by], "fs", pairs).astype(jnp.float32)
    return mixed.astype(jnp.bfloat16)


def solution(mesh):
    torus = Mesh(
        mesh.devices.reshape(8, 8, mesh.shape["fs"], mesh.shape["tp"]), ("sp_0", "sp_1", "fs", "tp")
    )

    return jax.shard_map(
        body,
        mesh=torus,
        in_specs=(
            P(SP_FS_TP, None),
            P(),
            P(None, ("fs", "tp")),
            P(None, "tp"),
            P(None, "tp"),
            P(None, ("fs", "tp")),
            P(None, ("fs", "tp")),
            P(None, ("fs", "tp")),
            P(("fs", "tp"), None, None),
            P(("fs", "tp"), None, None),
            P(("fs", "tp")),
            P(SP, ("fs", "tp")),
            P(("fs", "tp")),
            P(("fs", "tp")),
            P(),
            P(("fs", "tp"), None),
            P(("fs", "tp"), None),
        ),
        out_specs=P(SP_FS_TP, None),
        check_vma=False,
    )
```

```python
import functools

import jax
import jax.numpy as jnp
from jax import lax
from jax.experimental import pallas as pl
from jax.experimental.pallas import tpu as pltpu
from jax.sharding import Mesh
from jax.sharding import PartitionSpec as P


SP = ("sp_0", "sp_1")
SP_FS_TP = ("sp_0", "sp_1", "fs", "tp")


gate_scale = 8.0
input_eps = 1e-06
head_eps = 1e-05
far_below = -1e30
log2_e = 1.4426950408889634


def from_everyone(value, axis):
    copies = jnp.broadcast_to(value, (lax.axis_size(axis), *value.shape))
    return lax.all_to_all(copies, axis, split_axis=0, concat_axis=0, tiled=True)


def passed_along(value, axis, by):
    devices = lax.axis_size(axis)
    pairs = [(i, i + by) for i in range(devices) if 0 <= i + by < devices]
    return lax.ppermute(value, axis, pairs)


def vmem():
    return pl.BlockSpec(memory_space=pltpu.VMEM)


def anywhere():
    return pl.BlockSpec(memory_space=pl.ANY)


def smem():
    return pl.BlockSpec(memory_space=pltpu.SMEM)


def norm_kernel(tokens, gain, out, last):
    floats = tokens[...].astype(jnp.float32)
    level = lax.rsqrt(jnp.mean(floats * floats, axis=1, keepdims=True) + input_eps)
    out[...] = (floats * level * gain[...]).astype(jnp.bfloat16)
    last[...] = out[out.shape[0] - last.shape[0] :, :]


def normalized(tokens, gain, margin):
    return pl.pallas_call(
        norm_kernel,
        out_shape=(
            jax.ShapeDtypeStruct(tokens.shape, jnp.bfloat16),
            jax.ShapeDtypeStruct((margin, tokens.shape[1]), jnp.bfloat16),
        ),
        in_specs=[vmem(), vmem()],
        out_specs=(vmem(), vmem()),
        cost_estimate=pl.CostEstimate(
            flops=4 * tokens.size, bytes_accessed=1 << 18, transcendentals=0
        ),
        name="normalized",
    )(tokens, gain)


def one_minus_exp(x):
    series = jnp.full_like(x, 1.0)
    for k in range(7, 1, -1):
        series = 1.0 - series * x * (1.0 / k)
    return jnp.where(x < 0.35, x * series, 1.0 - jnp.exp(-x))


def project_kernel(
    place, mine, theirs, w_query, w_input, w_gate, taps, w_recur, w_admit, rate, scale,
    query_t, decays, states, gates, ends, *, fs_count, member_rows,
):
    core = place[3]
    sent_rows = mine.shape[0] // fs_count
    first = jnp.where(core == 0, mine[...], theirs[...])
    second = jnp.where(core == 0, theirs[...], mine[...])
    rows = jnp.concatenate([first, second], axis=0)

    def project(weight):
        return jnp.dot(rows, weight[...], preferred_element_type=jnp.float32)

    def piece(value, t, f):
        at = (t * fs_count + f) * sent_rows
        return value[at : at + member_rows]

    def in_order(value):
        pieces = [piece(value, t, f) for f in range(fs_count) for t in range(2)]
        return jnp.concatenate(pieces, axis=0)

    query = project(w_query)
    query = jnp.concatenate([piece(query, t, f) for t in range(2) for f in range(fs_count)], axis=0)
    score_scale = (query.shape[1] // 2) ** (-0.5) * log2_e
    query_t[...] = (query * score_scale).astype(jnp.bfloat16).T

    gate = in_order(project(w_gate).astype(jnp.bfloat16)).astype(jnp.float32)
    gates[...] = jax.nn.gelu(gate)

    lru_all = project(w_input).astype(jnp.bfloat16).astype(jnp.float32)
    margin = sent_rows - member_rows
    before = lru_all[2 * fs_count * sent_rows - margin :]
    padded = jnp.concatenate([before, in_order(lru_all)], axis=0)
    count = taps.shape[0]
    conv_sum = padded[margin:] * taps[count - 1 : count, :]
    for back in range(1, count):
        moved = pltpu.roll(padded, back, 0)[margin:]
        conv_sum = conv_sum + moved * taps[count - 1 - back : count - back, :]
    conv_out = conv_sum.astype(jnp.bfloat16)

    def gate_of(weight):
        zero = jnp.zeros(weight.shape[1:], weight.dtype)
        whole = jnp.concatenate(
            [
                jnp.concatenate([weight[0], zero], axis=1),
                jnp.concatenate([zero, weight[1]], axis=1),
            ],
            axis=0,
        )
        return jax.nn.sigmoid(jnp.dot(conv_out, whole, preferred_element_type=jnp.float32))

    log_decay = -gate_of(w_recur) * rate[...] * scale[...]
    decay = jnp.exp(log_decay)
    drive = jnp.sqrt(one_minus_exp(-2.0 * log_decay)) * gate_of(w_admit) * conv_out.astype(jnp.float32)

    row = lax.broadcasted_iota(jnp.int32, decay.shape, 0)
    by = 1
    while by < decay.shape[0]:
        inside = row >= by
        decay_before = jnp.where(inside, pltpu.roll(decay, by, 0), 1.0)
        state_before = jnp.where(inside, pltpu.roll(drive, by, 0), 0.0)
        drive = decay * state_before + drive
        decay = decay * decay_before
        by *= 2
    decays[...] = decay
    states[...] = drive
    last = decay.shape[0] - 1
    both = jnp.concatenate([decay[last:], drive[last:]], axis=0)
    ends[...] = jnp.broadcast_to(both[None], ends.shape)


def project(
    place, mine, theirs, weights, taps, w_recur, w_admit, rate, scale, blocks, fs_count, rows
):
    channels = scale.shape[1]
    block = jax.ShapeDtypeStruct(scale.shape, jnp.float32)
    return pl.pallas_call(
        functools.partial(project_kernel, fs_count=fs_count, member_rows=rows),
        out_shape=(
            jax.ShapeDtypeStruct((channels, scale.shape[0]), jnp.bfloat16),
            block,
            block,
            block,
            jax.ShapeDtypeStruct((blocks, 2, channels), jnp.float32),
        ),
        in_specs=[smem()] + [vmem()] * 10,
        out_specs=(vmem(),) * 5,
        cost_estimate=pl.CostEstimate(
            flops=2 * scale.shape[0] * mine.shape[1] * 3 * channels,
            bytes_accessed=4 << 20,
            transcendentals=1 << 18,
        ),
        name="project",
    )(place, mine, theirs, *weights, taps, w_recur, w_admit, rate, scale)


def states_kernel(
    place, pieces, start, decays, states, gates, mine, theirs, *, y_count, fs_count, member_rows
):
    here, core = (place[0] * y_count + place[1], place[3])

    count = pieces.shape[0]
    decay, state = (pieces[:, 0, :], pieces[:, 1, :])
    row = lax.broadcasted_iota(jnp.int32, decay.shape, 0)
    decay = jnp.where(row < here, decay, 1.0)
    state = jnp.where(row < here, state, 0.0)
    by = 1
    while by < count:
        inside = row >= by
        decay_before = jnp.where(inside, pltpu.roll(decay, by, 0), 1.0)
        state_before = jnp.where(inside, pltpu.roll(state, by, 0), 0.0)
        state = decay * state_before + state
        decay = decay * decay_before
        by *= 2
    entering = decay[count - 1 :] * start[...] + state[count - 1 :]
    out = ((states[...] + decays[...] * entering) * gates[...]).astype(jnp.bfloat16)
    for f in range(fs_count):
        at = 2 * f * member_rows
        even = out[at : at + member_rows]
        odd = out[at + member_rows : at + 2 * member_rows]
        mine[f * member_rows : (f + 1) * member_rows] = jnp.where(core == 0, even, odd)
        theirs[f * member_rows : (f + 1) * member_rows] = jnp.where(core == 0, odd, even)


def final_states(place, pieces, start, decays, states, gates, y_count, fs_count, member_rows):
    half = jax.ShapeDtypeStruct((fs_count * member_rows, decays.shape[1]), jnp.bfloat16)
    return pl.pallas_call(
        functools.partial(
            states_kernel, y_count=y_count, fs_count=fs_count, member_rows=member_rows
        ),
        out_shape=(half, half),
        in_specs=[smem()] + [vmem()] * 5,
        out_specs=(vmem(), vmem()),
        cost_estimate=pl.CostEstimate(
            flops=1 << 20, bytes_accessed=1 << 19, transcendentals=0
        ),
        name="final_states",
    )(place, pieces, start, decays, states, gates)


def attention_kernel(
    place, group, kv_far, *refs, block_rows, part_rows, start, stop
):
    packed, query, peak, values, value_t, kv, arrivals = refs[-7:]
    heads = stop - start
    _, size, rows = group.shape
    chunk_keys = kv.shape[1]
    z, y, member = (place[0], place[1], place[2])

    def arrival(at):
        return pltpu.make_async_copy(kv_far.at[at], kv.at[at], arrivals.at[at])

    arrival(z).start()

    def begin(at, _):
        arrival(at).start()
        return 0

    lax.fori_loop(0, z, begin, 0)
    line = lax.broadcasted_iota(jnp.int32, (size, rows), 0)
    for h in range(heads):
        whole = group[start + h]
        zero = jnp.zeros_like(whole)
        query[2 * h] = jnp.where(line < size // 2, whole, zero)
        query[2 * h + 1] = jnp.where(line < size // 2, zero, whole)
    peak[...] = jnp.full(peak.shape, far_below, jnp.float32)
    value_t[size:, :] = jnp.ones((16, chunk_keys), jnp.bfloat16)
    values[...] = jnp.zeros(values.shape, jnp.float32)

    def visible_keys():
        row = lax.broadcasted_iota(jnp.int32, (chunk_keys, rows), 0)
        lane = lax.broadcasted_iota(jnp.int32, (chunk_keys, rows), 1)
        key_pos = (row // part_rows) * block_rows + member * part_rows + row % part_rows
        half, piece = (rows // 2, part_rows // 2)
        inside = (lane % half) // piece * part_rows + lane // half * piece + lane % piece
        return key_pos <= inside + y * block_rows

    def one_chunk(at, masked):
        arrival(at).wait()
        both = kv[at]
        keys = both[:, :size]
        value_t[:size, :] = both[:, size:].T
        visible = visible_keys() if masked else None

        def scores_of(i):
            found = jnp.dot(keys, query[i], preferred_element_type=jnp.float32)
            return jnp.where(visible, found, far_below) if masked else found

        scores = scores_of(0)
        for i in range(2 * heads):
            following = scores_of(i + 1) if i + 1 < 2 * heads else None
            old = peak[i]
            now = jnp.maximum(old, jnp.max(scores, axis=0, keepdims=True))
            expos = jnp.exp2(scores - now)
            if masked:
                expos = jnp.where(visible, expos, 0.0)
            fade = jnp.exp2(old - now)
            peak[i] = now
            values[i] = values[i] * fade + jnp.dot(
                value_t[...], expos.astype(jnp.bfloat16), preferred_element_type=jnp.float32
            )
            scores = following

    one_chunk(z, True)

    def earlier(at, _):
        one_chunk(at, False)
        return 0

    lax.fori_loop(0, z, earlier, 0)

    if start:
        packed[:start] = refs[0][...]
    half = rows // 2
    line = lax.broadcasted_iota(jnp.int32, (16, rows), 0)
    for h in range(heads):
        tail = jnp.zeros((16, rows), jnp.float32)
        for m in range(2):
            amount = values[2 * h + m, size : size + 1, :]
            some = amount > 0.0
            safe = jnp.where(some, amount, 1.0)
            shares = (values[2 * h + m, :size, :] * jnp.where(some, 1.0 / safe, 0.0)).astype(jnp.bfloat16)
            level = jnp.where(some, peak[2 * h + m] + jnp.log2(safe), far_below)
            coarse = level.astype(jnp.bfloat16).astype(jnp.float32)
            tail = jnp.where(line == 2 * m, coarse, tail)
            tail = jnp.where(line == 2 * m + 1, level - coarse, tail)
            for t in range(2):
                packed[start + h, t, m * size : (m + 1) * size, :] = shares[:, t * half : (t + 1) * half]
        rounded = tail.astype(jnp.bfloat16)
        for t in range(2):
            packed[start + h, t, 2 * size : 2 * size + 16, :] = rounded[:, t * half : (t + 1) * half]


def attention(place, group, kv, earlier, stop, block_rows, part_rows):
    start = 0 if earlier is None else earlier.shape[0]
    heads = stop - start
    _, size, rows = group.shape
    z_count, chunk_keys, _ = kv.shape
    keys = chunk_keys * z_count
    return pl.pallas_call(
        functools.partial(
            attention_kernel, block_rows=block_rows, part_rows=part_rows, start=start, stop=stop
        ),
        out_shape=jax.ShapeDtypeStruct((stop, 2, 2 * size + 16, rows // 2), jnp.bfloat16),
        in_specs=[smem(), vmem(), anywhere()] + [vmem()] * (start > 0),
        out_specs=vmem(),
        scratch_shapes=[
            pltpu.VMEM((2 * heads, size, rows), jnp.bfloat16),
            pltpu.VMEM((2 * heads, 1, rows), jnp.float32),
            pltpu.VMEM((2 * heads, size + 16, rows), jnp.float32),
            pltpu.VMEM((size + 16, chunk_keys), jnp.bfloat16),
            pltpu.VMEM(kv.shape, kv.dtype),
            pltpu.SemaphoreType.DMA((z_count,)),
        ],
        cost_estimate=pl.CostEstimate(
            flops=4 * 2 * heads * rows * keys * size,
            bytes_accessed=4 << 20,
            transcendentals=2 * heads * rows * keys,
        ),
        name="attention",
    )(place, group, kv, *(() if earlier is None else (earlier,)))


def finish_kernel(place, lam, lam_theirs, parts, gain, lru_mine, lru_theirs, w_mine, w_theirs, out):
    count, _, lines, _ = parts.shape
    size = (lines - 16) // 2
    core = place[3]

    def head_output(owner, factor):
        joined = []
        for m in range(2):
            tails = [parts[i, owner, 2 * size :, :].astype(jnp.float32) for i in range(count)]
            levels = [t[2 * m : 2 * m + 1] + t[2 * m + 1 : 2 * m + 2] for t in tails]
            top = functools.reduce(jnp.maximum, levels)
            shares = [jnp.exp2(level - top) for level in levels]
            inverse = 1.0 / functools.reduce(jnp.add, shares)
            weighted = [
                parts[i, owner, m * size : (m + 1) * size, :].astype(jnp.float32)
                * (shares[i] * inverse)
                for i in range(count)
            ]
            joined.append(functools.reduce(jnp.add, weighted))
        diff = joined[0] - factor * joined[1]
        level = lax.rsqrt(jnp.mean(diff * diff, axis=0, keepdims=True) + head_eps)
        return ((diff * level).T * gain[...]).astype(jnp.bfloat16)

    mine = jnp.concatenate([lru_mine[...], head_output(core, lam[0])], axis=1)
    theirs = jnp.concatenate([lru_theirs[...], head_output(1 - core, lam_theirs[0])], axis=1)
    result = jnp.dot(mine, w_mine[...], preferred_element_type=jnp.float32)
    result = result + jnp.dot(theirs, w_theirs[...], preferred_element_type=jnp.float32)
    out[...] = result.astype(jnp.bfloat16)


def finish(place, lam, lam_theirs, parts, gain, lru_mine, lru_theirs, w_mine, w_theirs):
    rows, wide = (lru_mine.shape[0], w_mine.shape[1])
    return pl.pallas_call(
        finish_kernel,
        out_shape=jax.ShapeDtypeStruct((rows, wide), jnp.bfloat16),
        in_specs=[smem()] * 3 + [vmem()] * 6,
        out_specs=vmem(),
        cost_estimate=pl.CostEstimate(
            flops=2 * rows * wide * 512, bytes_accessed=3 << 20, transcendentals=rows * 16
        ),
        name="finish",
    )(place, lam, lam_theirs, parts, gain, lru_mine, lru_theirs, w_mine, w_theirs)


def body(
    tokens,
    norm_gain,
    query_weight,
    w_key,
    w_value,
    w_input,
    w_gate,
    conv_kernel,
    w_recur,
    w_admit,
    decay_param,
    decay_scale,
    init_state,
    diff_lambda,
    head_gain,
    w_out_lru,
    w_out_attn,
):
    member_rows, wide = tokens.shape
    fs_count = lax.axis_size("fs")
    tp_count = lax.axis_size("tp")
    row_count = member_rows * fs_count * tp_count
    share_rows = member_rows * tp_count
    member = lax.axis_index("fs")
    core = lax.axis_index("tp")
    z_count, z = (lax.axis_size("sp_0"), lax.axis_index("sp_0"))
    y_count, y = (lax.axis_size("sp_1"), lax.axis_index("sp_1"))

    normed, last_rows = normalized(tokens, norm_gain[None], 8)

    before_rows = passed_along(last_rows, SP, 1)

    chip_rows = lax.all_gather(normed, "tp", axis=0, tiled=True)
    kv_here = jnp.concatenate(
        [
            jnp.dot(chip_rows, weight, preferred_element_type=jnp.float32).astype(jnp.bfloat16)
            for weight in (w_key, w_value)
        ],
        axis=1,
    )
    kv_here, normed = lax.optimization_barrier((kv_here, normed))
    everyone = from_everyone(kv_here, SP)
    everyone = everyone.reshape(z_count, y_count * share_rows, kv_here.shape[1])

    sent = jnp.concatenate([normed, before_rows], axis=0)
    mine = lax.all_gather(sent, "fs", axis=0, tiled=True)
    swap = [(0, 1), (1, 0)]
    theirs = lax.ppermute(mine, "tp", swap)

    place = jnp.stack([z, y, member, core]).astype(jnp.int32)
    rate = gate_scale * jax.nn.softplus(-decay_param)
    query_t, decays, states, gates, ends = project(
        place,
        mine,
        theirs,
        (query_weight, w_input, w_gate),
        conv_kernel,
        w_recur,
        w_admit,
        rate[None],
        decay_scale,
        z_count * y_count,
        fs_count,
        member_rows,
    )

    group = lax.all_gather(query_t, "fs")

    w_mine = jnp.concatenate([w_out_lru, w_out_attn], axis=0)
    w_theirs = lax.ppermute(w_mine, "tp", swap)
    lam_theirs = lax.ppermute(diff_lambda, "tp", swap)

    half_heads = fs_count // 2
    part = attention(place, group, everyone, None, half_heads, row_count, share_rows)
    ends, part = lax.optimization_barrier((ends, part))
    everywhere = lax.all_to_all(ends, SP, split_axis=0, concat_axis=0, tiled=True)
    carried = attention(place, group, everyone, part, fs_count, row_count, share_rows)
    lines, half_rows = carried.shape[2:]
    carried = carried.reshape(fs_count * tp_count, lines, half_rows)
    packed = lax.all_to_all(carried, ("fs", "tp"), split_axis=0, concat_axis=0, tiled=True)
    packed = packed.reshape(fs_count, tp_count, lines, half_rows)

    lru_mine, lru_other = final_states(
        place, everywhere, init_state[None], decays, states, gates, y_count, fs_count, member_rows
    )
    lru_theirs = lax.ppermute(lru_other, "tp", swap)

    partial = finish(
        place,
        diff_lambda,
        lam_theirs,
        packed,
        head_gain[None],
        lru_mine,
        lru_theirs,
        w_mine,
        w_theirs,
    )
    partial = partial.reshape(fs_count, member_rows, wide)
    arrived = lax.all_to_all(partial, "fs", split_axis=0, concat_axis=0, tiled=True)
    return arrived.astype(jnp.float32).sum(axis=0).astype(jnp.bfloat16)


def solution(mesh):
    torus = Mesh(
        mesh.devices.reshape(8, 8, mesh.shape["fs"], mesh.shape["tp"]), ("sp_0", "sp_1", "fs", "tp")
    )

    return jax.shard_map(
        body,
        mesh=torus,
        in_specs=(
            P(SP_FS_TP, None),
            P(),
            P(None, ("fs", "tp")),
            P(None, "tp"),
            P(None, "tp"),
            P(None, ("fs", "tp")),
            P(None, ("fs", "tp")),
            P(None, ("fs", "tp")),
            P(("fs", "tp"), None, None),
            P(("fs", "tp"), None, None),
            P(("fs", "tp")),
            P(SP, ("fs", "tp")),
            P(("fs", "tp")),
            P(("fs", "tp")),
            P(),
            P(("fs", "tp"), None),
            P(("fs", "tp"), None),
        ),
        out_specs=P(SP_FS_TP, None),
        check_vma=False,
    )
```

```python
import functools

import jax
import jax.numpy as jnp
from jax import lax
from jax.experimental import pallas as pl
from jax.experimental.pallas import tpu as pltpu
from jax.sharding import Mesh
from jax.sharding import PartitionSpec as P


SP = ("sp_0", "sp_1")
SP_FS_TP = ("sp_0", "sp_1", "fs", "tp")


gate_scale = 8.0
input_eps = 1e-06
head_eps = 1e-05
far_below = -1e30
log2_e = 1.4426950408889634


def from_everyone(value, axis):
    copies = jnp.broadcast_to(value, (lax.axis_size(axis), *value.shape))
    return lax.all_to_all(copies, axis, split_axis=0, concat_axis=0, tiled=True)


def passed_along(value, axis, by):
    devices = lax.axis_size(axis)
    pairs = [(i, i + by) for i in range(devices) if 0 <= i + by < devices]
    return lax.ppermute(value, axis, pairs)


def pair_combine(earlier, later):
    decay_early, state_early = earlier
    decay_late, state_late = later
    return (decay_early * decay_late, decay_late * state_early + state_late)


def vmem():
    return pl.BlockSpec(memory_space=pltpu.VMEM)


def anywhere():
    return pl.BlockSpec(memory_space=pl.ANY)


def smem():
    return pl.BlockSpec(memory_space=pltpu.SMEM)


def norm_kernel(tokens, gain, out, last):
    floats = tokens[...].astype(jnp.float32)
    level = lax.rsqrt(jnp.mean(floats * floats, axis=1, keepdims=True) + input_eps)
    out[...] = (floats * level * gain[...]).astype(jnp.bfloat16)
    last[...] = out[out.shape[0] - last.shape[0] :, :]


def normalized(tokens, gain, margin):
    return pl.pallas_call(
        norm_kernel,
        out_shape=(
            jax.ShapeDtypeStruct(tokens.shape, jnp.bfloat16),
            jax.ShapeDtypeStruct((margin, tokens.shape[1]), jnp.bfloat16),
        ),
        in_specs=[vmem(), vmem()],
        out_specs=(vmem(), vmem()),
        cost_estimate=pl.CostEstimate(
            flops=4 * tokens.size, bytes_accessed=1 << 18, transcendentals=0
        ),
        name="normalized",
    )(tokens, gain)


def one_minus_exp(x):
    series = jnp.full_like(x, 1.0)
    for k in range(7, 1, -1):
        series = 1.0 - series * x * (1.0 / k)
    return jnp.where(x < 0.35, x * series, 1.0 - jnp.exp(-x))


def project_kernel(
    place, mine, theirs, w_query, w_input, w_gate, taps, w_recur, w_admit, rate, scale,
    query_t, decays, states, gates, ends, *, fs_count, member_rows,
):
    core = place[3]
    sent_rows = mine.shape[0] // fs_count
    first = jnp.where(core == 0, mine[...], theirs[...])
    second = jnp.where(core == 0, theirs[...], mine[...])
    rows = jnp.concatenate([first, second], axis=0)

    def project(weight):
        return jnp.dot(rows, weight[...], preferred_element_type=jnp.float32)

    def piece(value, t, f):
        at = (t * fs_count + f) * sent_rows
        return value[at : at + member_rows]

    def in_order(value):
        pieces = [piece(value, t, f) for f in range(fs_count) for t in range(2)]
        return jnp.concatenate(pieces, axis=0)

    query = project(w_query)
    query = jnp.concatenate([piece(query, t, f) for t in range(2) for f in range(fs_count)], axis=0)
    score_scale = (query.shape[1] // 2) ** (-0.5) * log2_e
    query_t[...] = (query * score_scale).astype(jnp.bfloat16).T

    gate = in_order(project(w_gate).astype(jnp.bfloat16)).astype(jnp.float32)
    gates[...] = jax.nn.gelu(gate)

    lru_all = project(w_input).astype(jnp.bfloat16).astype(jnp.float32)
    margin = sent_rows - member_rows
    before = lru_all[2 * fs_count * sent_rows - margin :]
    padded = jnp.concatenate([before, in_order(lru_all)], axis=0)
    count = taps.shape[0]
    conv_sum = padded[margin:] * taps[count - 1 : count, :]
    for back in range(1, count):
        moved = pltpu.roll(padded, back, 0)[margin:]
        conv_sum = conv_sum + moved * taps[count - 1 - back : count - back, :]
    conv_out = conv_sum.astype(jnp.bfloat16)

    def gate_of(weight):
        zero = jnp.zeros(weight.shape[1:], weight.dtype)
        whole = jnp.concatenate(
            [
                jnp.concatenate([weight[0], zero], axis=1),
                jnp.concatenate([zero, weight[1]], axis=1),
            ],
            axis=0,
        )
        return jax.nn.sigmoid(jnp.dot(conv_out, whole, preferred_element_type=jnp.float32))

    log_decay = -gate_of(w_recur) * rate[...] * scale[...]
    decay = jnp.exp(log_decay)
    drive = jnp.sqrt(one_minus_exp(-2.0 * log_decay)) * gate_of(w_admit) * conv_out.astype(jnp.float32)

    row = lax.broadcasted_iota(jnp.int32, decay.shape, 0)
    by = 1
    while by < decay.shape[0]:
        inside = row >= by
        decay_before = jnp.where(inside, pltpu.roll(decay, by, 0), 1.0)
        state_before = jnp.where(inside, pltpu.roll(drive, by, 0), 0.0)
        drive = decay * state_before + drive
        decay = decay * decay_before
        by *= 2
    decays[...] = decay
    states[...] = drive
    last = decay.shape[0] - 1
    ends[0:1, :] = decay[last:]
    ends[1:2, :] = drive[last:]


def project(
    place, mine, theirs, weights, taps, w_recur, w_admit, rate, scale, fs_count, rows
):
    channels = scale.shape[1]
    block = jax.ShapeDtypeStruct(scale.shape, jnp.float32)
    return pl.pallas_call(
        functools.partial(project_kernel, fs_count=fs_count, member_rows=rows),
        out_shape=(
            jax.ShapeDtypeStruct((channels, scale.shape[0]), jnp.bfloat16),
            block,
            block,
            block,
            jax.ShapeDtypeStruct((2, channels), jnp.float32),
        ),
        in_specs=[smem()] + [vmem()] * 10,
        out_specs=(vmem(),) * 5,
        cost_estimate=pl.CostEstimate(
            flops=2 * scale.shape[0] * mine.shape[1] * 3 * channels,
            bytes_accessed=4 << 20,
            transcendentals=1 << 18,
        ),
        name="project",
    )(place, mine, theirs, *weights, taps, w_recur, w_admit, rate, scale)


def states_kernel(
    place, near, far, start, decays, states, gates, mine, theirs, *, fs_count, member_rows
):
    z, y, core = (place[0], place[1], place[3])

    def before(pieces, here):
        decay, state = (jnp.ones_like(pieces[0, 0:1]), jnp.zeros_like(pieces[0, 1:2]))
        for k in range(pieces.shape[0]):
            passed = k < here
            new_decay, new_state = pair_combine((decay, state), (pieces[k, 0:1], pieces[k, 1:2]))
            decay = jnp.where(passed, new_decay, decay)
            state = jnp.where(passed, new_state, state)
        return decay, state

    decay, state = pair_combine(before(far, z), before(near, y))
    entering = decay * start[...] + state
    out = ((states[...] + decays[...] * entering) * gates[...]).astype(jnp.bfloat16)
    for f in range(fs_count):
        at = 2 * f * member_rows
        even = out[at : at + member_rows]
        odd = out[at + member_rows : at + 2 * member_rows]
        mine[f * member_rows : (f + 1) * member_rows] = jnp.where(core == 0, even, odd)
        theirs[f * member_rows : (f + 1) * member_rows] = jnp.where(core == 0, odd, even)


def final_states(place, near, far, start, decays, states, gates, fs_count, member_rows):
    half = jax.ShapeDtypeStruct((fs_count * member_rows, decays.shape[1]), jnp.bfloat16)
    return pl.pallas_call(
        functools.partial(states_kernel, fs_count=fs_count, member_rows=member_rows),
        out_shape=(half, half),
        in_specs=[smem()] + [vmem()] * 6,
        out_specs=(vmem(), vmem()),
        cost_estimate=pl.CostEstimate(
            flops=1 << 20, bytes_accessed=1 << 19, transcendentals=0
        ),
        name="final_states",
    )(place, near, far, start, decays, states, gates)


def attention_kernel(
    place, group, kv_far, *refs, block_rows, part_rows, start, stop
):
    packed, query, peak, values, value_t, kv, arrivals = refs[-7:]
    heads = stop - start
    _, size, rows = group.shape
    chunk_keys = kv.shape[1]
    z, y, member = (place[0], place[1], place[2])

    def arrival(at):
        return pltpu.make_async_copy(kv_far.at[at], kv.at[at], arrivals.at[at])

    arrival(z).start()

    def begin(at, _):
        arrival(at).start()
        return 0

    lax.fori_loop(0, z, begin, 0)
    line = lax.broadcasted_iota(jnp.int32, (size, rows), 0)
    for h in range(heads):
        whole = group[start + h]
        zero = jnp.zeros_like(whole)
        query[2 * h] = jnp.where(line < size // 2, whole, zero)
        query[2 * h + 1] = jnp.where(line < size // 2, zero, whole)
    peak[...] = jnp.full(peak.shape, far_below, jnp.float32)
    value_t[size:, :] = jnp.ones((16, chunk_keys), jnp.bfloat16)
    values[...] = jnp.zeros(values.shape, jnp.float32)

    def visible_keys():
        row = lax.broadcasted_iota(jnp.int32, (chunk_keys, rows), 0)
        lane = lax.broadcasted_iota(jnp.int32, (chunk_keys, rows), 1)
        key_pos = (row // part_rows) * block_rows + member * part_rows + row % part_rows
        half, piece = (rows // 2, part_rows // 2)
        inside = (lane % half) // piece * part_rows + lane // half * piece + lane % piece
        return key_pos <= inside + y * block_rows

    def one_chunk(at, masked):
        arrival(at).wait()
        both = kv[at]
        keys = both[:, :size]
        value_t[:size, :] = both[:, size:].T
        visible = visible_keys() if masked else None

        def scores_of(i):
            found = jnp.dot(keys, query[i], preferred_element_type=jnp.float32)
            return jnp.where(visible, found, far_below) if masked else found

        scores = scores_of(0)
        for i in range(2 * heads):
            following = scores_of(i + 1) if i + 1 < 2 * heads else None
            old = peak[i]
            now = jnp.maximum(old, jnp.max(scores, axis=0, keepdims=True))
            expos = jnp.exp2(scores - now)
            if masked:
                expos = jnp.where(visible, expos, 0.0)
            fade = jnp.exp2(old - now)
            peak[i] = now
            values[i] = values[i] * fade + jnp.dot(
                value_t[...], expos.astype(jnp.bfloat16), preferred_element_type=jnp.float32
            )
            scores = following

    one_chunk(z, True)

    def earlier(at, _):
        one_chunk(at, False)
        return 0

    lax.fori_loop(0, z, earlier, 0)

    if start:
        packed[:start] = refs[0][...]
    half = rows // 2
    line = lax.broadcasted_iota(jnp.int32, (16, rows), 0)
    for h in range(heads):
        tail = jnp.zeros((16, rows), jnp.float32)
        for m in range(2):
            amount = values[2 * h + m, size : size + 1, :]
            some = amount > 0.0
            safe = jnp.where(some, amount, 1.0)
            shares = (values[2 * h + m, :size, :] * jnp.where(some, 1.0 / safe, 0.0)).astype(jnp.bfloat16)
            level = jnp.where(some, peak[2 * h + m] + jnp.log2(safe), far_below)
            coarse = level.astype(jnp.bfloat16).astype(jnp.float32)
            tail = jnp.where(line == 2 * m, coarse, tail)
            tail = jnp.where(line == 2 * m + 1, level - coarse, tail)
            for t in range(2):
                packed[start + h, t, m * size : (m + 1) * size, :] = shares[:, t * half : (t + 1) * half]
        rounded = tail.astype(jnp.bfloat16)
        for t in range(2):
            packed[start + h, t, 2 * size : 2 * size + 16, :] = rounded[:, t * half : (t + 1) * half]


def attention(place, group, kv, earlier, stop, block_rows, part_rows):
    start = 0 if earlier is None else earlier.shape[0]
    heads = stop - start
    _, size, rows = group.shape
    z_count, chunk_keys, _ = kv.shape
    keys = chunk_keys * z_count
    return pl.pallas_call(
        functools.partial(
            attention_kernel, block_rows=block_rows, part_rows=part_rows, start=start, stop=stop
        ),
        out_shape=jax.ShapeDtypeStruct((stop, 2, 2 * size + 16, rows // 2), jnp.bfloat16),
        in_specs=[smem(), vmem(), anywhere()] + [vmem()] * (start > 0),
        out_specs=vmem(),
        scratch_shapes=[
            pltpu.VMEM((2 * heads, size, rows), jnp.bfloat16),
            pltpu.VMEM((2 * heads, 1, rows), jnp.float32),
            pltpu.VMEM((2 * heads, size + 16, rows), jnp.float32),
            pltpu.VMEM((size + 16, chunk_keys), jnp.bfloat16),
            pltpu.VMEM(kv.shape, kv.dtype),
            pltpu.SemaphoreType.DMA((z_count,)),
        ],
        cost_estimate=pl.CostEstimate(
            flops=4 * 2 * heads * rows * keys * size,
            bytes_accessed=4 << 20,
            transcendentals=2 * heads * rows * keys,
        ),
        name="attention",
    )(place, group, kv, *(() if earlier is None else (earlier,)))


def finish_kernel(place, lam, lam_theirs, parts, gain, lru_mine, lru_theirs, w_mine, w_theirs, out):
    count, _, lines, _ = parts.shape
    size = (lines - 16) // 2
    core = place[3]

    def head_output(owner, factor):
        joined = []
        for m in range(2):
            tails = [parts[i, owner, 2 * size :, :].astype(jnp.float32) for i in range(count)]
            levels = [t[2 * m : 2 * m + 1] + t[2 * m + 1 : 2 * m + 2] for t in tails]
            top = functools.reduce(jnp.maximum, levels)
            shares = [jnp.exp2(level - top) for level in levels]
            inverse = 1.0 / functools.reduce(jnp.add, shares)
            weighted = [
                parts[i, owner, m * size : (m + 1) * size, :].astype(jnp.float32)
                * (shares[i] * inverse)
                for i in range(count)
            ]
            joined.append(functools.reduce(jnp.add, weighted))
        diff = joined[0] - factor * joined[1]
        level = lax.rsqrt(jnp.mean(diff * diff, axis=0, keepdims=True) + head_eps)
        return ((diff * level).T * gain[...]).astype(jnp.bfloat16)

    mine = jnp.concatenate([lru_mine[...], head_output(core, lam[0])], axis=1)
    theirs = jnp.concatenate([lru_theirs[...], head_output(1 - core, lam_theirs[0])], axis=1)
    result = jnp.dot(mine, w_mine[...], preferred_element_type=jnp.float32)
    result = result + jnp.dot(theirs, w_theirs[...], preferred_element_type=jnp.float32)
    out[...] = result.astype(jnp.bfloat16)


def finish(place, lam, lam_theirs, parts, gain, lru_mine, lru_theirs, w_mine, w_theirs):
    rows, wide = (lru_mine.shape[0], w_mine.shape[1])
    return pl.pallas_call(
        finish_kernel,
        out_shape=jax.ShapeDtypeStruct((rows, wide), jnp.bfloat16),
        in_specs=[smem()] * 3 + [vmem()] * 6,
        out_specs=vmem(),
        cost_estimate=pl.CostEstimate(
            flops=2 * rows * wide * 512, bytes_accessed=3 << 20, transcendentals=rows * 16
        ),
        name="finish",
    )(place, lam, lam_theirs, parts, gain, lru_mine, lru_theirs, w_mine, w_theirs)


def body(
    tokens,
    norm_gain,
    query_weight,
    w_key,
    w_value,
    w_input,
    w_gate,
    conv_kernel,
    w_recur,
    w_admit,
    decay_param,
    decay_scale,
    init_state,
    diff_lambda,
    head_gain,
    w_out_lru,
    w_out_attn,
):
    member_rows, wide = tokens.shape
    fs_count = lax.axis_size("fs")
    tp_count = lax.axis_size("tp")
    row_count = member_rows * fs_count * tp_count
    share_rows = member_rows * tp_count
    member = lax.axis_index("fs")
    core = lax.axis_index("tp")
    z = lax.axis_index("sp_0")
    y_count, y = (lax.axis_size("sp_1"), lax.axis_index("sp_1"))

    normed, last_rows = normalized(tokens, norm_gain[None], 8)

    before_rows = passed_along(last_rows, SP, 1)

    chip_rows = lax.all_gather(normed, "tp", axis=0, tiled=True)
    kv_here = jnp.concatenate(
        [
            jnp.dot(chip_rows, weight, preferred_element_type=jnp.float32).astype(jnp.bfloat16)
            for weight in (w_key, w_value)
        ],
        axis=1,
    )
    chunk = from_everyone(kv_here, "sp_1").reshape(y_count * share_rows, kv_here.shape[1])

    sent = jnp.concatenate([normed, before_rows], axis=0)
    sent, chunk = lax.optimization_barrier((sent, chunk))
    everyone = lax.all_gather(chunk, "sp_0")
    mine = lax.all_gather(sent, "fs", axis=0, tiled=True)
    swap = [(0, 1), (1, 0)]
    theirs = lax.ppermute(mine, "tp", swap)

    place = jnp.stack([z, y, member, core]).astype(jnp.int32)
    rate = gate_scale * jax.nn.softplus(-decay_param)
    query_t, decays, states, gates, ends = project(
        place,
        mine,
        theirs,
        (query_weight, w_input, w_gate),
        conv_kernel,
        w_recur,
        w_admit,
        rate[None],
        decay_scale,
        fs_count,
        member_rows,
    )

    group = lax.all_gather(query_t, "fs")

    w_mine = jnp.concatenate([w_out_lru, w_out_attn], axis=0)
    w_theirs = lax.ppermute(w_mine, "tp", swap)
    lam_theirs = lax.ppermute(diff_lambda, "tp", swap)

    near = lax.all_gather(ends, "sp_1")
    row = (near[0, 0], near[0, 1])
    for k in range(1, y_count):
        row = pair_combine(row, (near[k, 0], near[k, 1]))
    far = from_everyone(jnp.stack(row), "sp_0")

    carried = attention(place, group, everyone, None, fs_count, row_count, share_rows)
    lines, half_rows = carried.shape[2:]
    carried = carried.reshape(fs_count * tp_count, lines, half_rows)
    packed = lax.all_to_all(carried, ("fs", "tp"), split_axis=0, concat_axis=0, tiled=True)
    packed = packed.reshape(fs_count, tp_count, lines, half_rows)

    lru_mine, lru_other = final_states(
        place, near, far, init_state[None], decays, states, gates, fs_count, member_rows
    )
    lru_theirs = lax.ppermute(lru_other, "tp", swap)

    partial = finish(
        place,
        diff_lambda,
        lam_theirs,
        packed,
        head_gain[None],
        lru_mine,
        lru_theirs,
        w_mine,
        w_theirs,
    )
    partial = partial.reshape(fs_count, member_rows, wide)
    arrived = lax.all_to_all(partial, "fs", split_axis=0, concat_axis=0, tiled=True)
    return arrived.astype(jnp.float32).sum(axis=0).astype(jnp.bfloat16)


def solution(mesh):
    torus = Mesh(
        mesh.devices.reshape(8, 8, mesh.shape["fs"], mesh.shape["tp"]), ("sp_0", "sp_1", "fs", "tp")
    )

    return jax.shard_map(
        body,
        mesh=torus,
        in_specs=(
            P(SP_FS_TP, None),
            P(),
            P(None, ("fs", "tp")),
            P(None, "tp"),
            P(None, "tp"),
            P(None, ("fs", "tp")),
            P(None, ("fs", "tp")),
            P(None, ("fs", "tp")),
            P(("fs", "tp"), None, None),
            P(("fs", "tp"), None, None),
            P(("fs", "tp")),
            P(SP, ("fs", "tp")),
            P(("fs", "tp")),
            P(("fs", "tp")),
            P(),
            P(("fs", "tp"), None),
            P(("fs", "tp"), None),
        ),
        out_specs=P(SP_FS_TP, None),
        check_vma=False,
    )
```

```python
import functools

import jax
import jax.numpy as jnp
from jax import lax
from jax.experimental import pallas as pl
from jax.experimental.pallas import tpu as pltpu
from jax.sharding import Mesh
from jax.sharding import PartitionSpec as P


SP = ("sp_0", "sp_1")
SP_FS_TP = ("sp_0", "sp_1", "fs", "tp")


gate_scale = 8.0
input_eps = 1e-06
head_eps = 1e-05
far_below = -1e30
log2_e = 1.4426950408889634


def from_everyone(value, axis):
    copies = jnp.broadcast_to(value, (lax.axis_size(axis), *value.shape))
    return lax.all_to_all(copies, axis, split_axis=0, concat_axis=0, tiled=True)


def passed_along(value, axis, by):
    devices = lax.axis_size(axis)
    pairs = [(i, i + by) for i in range(devices) if 0 <= i + by < devices]
    return lax.ppermute(value, axis, pairs)


def vmem():
    return pl.BlockSpec(memory_space=pltpu.VMEM)


def anywhere():
    return pl.BlockSpec(memory_space=pl.ANY)


def smem():
    return pl.BlockSpec(memory_space=pltpu.SMEM)


def norm_kernel(tokens, gain, out, last):
    floats = tokens[...].astype(jnp.float32)
    level = lax.rsqrt(jnp.mean(floats * floats, axis=1, keepdims=True) + input_eps)
    out[...] = (floats * level * gain[...]).astype(jnp.bfloat16)
    last[...] = out[out.shape[0] - last.shape[0] :, :]


def normalized(tokens, gain, margin):
    return pl.pallas_call(
        norm_kernel,
        out_shape=(
            jax.ShapeDtypeStruct(tokens.shape, jnp.bfloat16),
            jax.ShapeDtypeStruct((margin, tokens.shape[1]), jnp.bfloat16),
        ),
        in_specs=[vmem(), vmem()],
        out_specs=(vmem(), vmem()),
        cost_estimate=pl.CostEstimate(
            flops=4 * tokens.size, bytes_accessed=1 << 18, transcendentals=0
        ),
        name="normalized",
    )(tokens, gain)


def one_minus_exp(x):
    series = jnp.full_like(x, 1.0)
    for k in range(7, 1, -1):
        series = 1.0 - series * x * (1.0 / k)
    return jnp.where(x < 0.35, x * series, 1.0 - jnp.exp(-x))


def project_kernel(
    place, mine, theirs, w_query, w_input, w_gate, taps, w_recur, w_admit, rate, scale,
    query_t, decays, states, gates, ends, *, fs_count, member_rows,
):
    core = place[3]
    sent_rows = mine.shape[0] // fs_count
    first = jnp.where(core == 0, mine[...], theirs[...])
    second = jnp.where(core == 0, theirs[...], mine[...])
    rows = jnp.concatenate([first, second], axis=0)

    def project(weight):
        return jnp.dot(rows, weight[...], preferred_element_type=jnp.float32)

    def piece(value, t, f):
        at = (t * fs_count + f) * sent_rows
        return value[at : at + member_rows]

    def in_order(value):
        pieces = [piece(value, t, f) for f in range(fs_count) for t in range(2)]
        return jnp.concatenate(pieces, axis=0)

    query = project(w_query)
    query = jnp.concatenate([piece(query, t, f) for t in range(2) for f in range(fs_count)], axis=0)
    score_scale = (query.shape[1] // 2) ** (-0.5) * log2_e
    query_t[...] = (query * score_scale).astype(jnp.bfloat16).T

    gate = in_order(project(w_gate).astype(jnp.bfloat16)).astype(jnp.float32)
    gates[...] = jax.nn.gelu(gate)

    lru_all = project(w_input).astype(jnp.bfloat16).astype(jnp.float32)
    margin = sent_rows - member_rows
    before = lru_all[2 * fs_count * sent_rows - margin :]
    padded = jnp.concatenate([before, in_order(lru_all)], axis=0)
    count = taps.shape[0]
    conv_sum = padded[margin:] * taps[count - 1 : count, :]
    for back in range(1, count):
        moved = pltpu.roll(padded, back, 0)[margin:]
        conv_sum = conv_sum + moved * taps[count - 1 - back : count - back, :]
    conv_out = conv_sum.astype(jnp.bfloat16)

    def gate_of(weight):
        zero = jnp.zeros(weight.shape[1:], weight.dtype)
        whole = jnp.concatenate(
            [
                jnp.concatenate([weight[0], zero], axis=1),
                jnp.concatenate([zero, weight[1]], axis=1),
            ],
            axis=0,
        )
        return jax.nn.sigmoid(jnp.dot(conv_out, whole, preferred_element_type=jnp.float32))

    log_decay = -gate_of(w_recur) * rate[...] * scale[...]
    decay = jnp.exp(log_decay)
    drive = jnp.sqrt(one_minus_exp(-2.0 * log_decay)) * gate_of(w_admit) * conv_out.astype(jnp.float32)

    row = lax.broadcasted_iota(jnp.int32, decay.shape, 0)
    by = 1
    while by < decay.shape[0]:
        inside = row >= by
        decay_before = jnp.where(inside, pltpu.roll(decay, by, 0), 1.0)
        state_before = jnp.where(inside, pltpu.roll(drive, by, 0), 0.0)
        drive = decay * state_before + drive
        decay = decay * decay_before
        by *= 2
    decays[...] = decay
    states[...] = drive
    last = decay.shape[0] - 1
    both = jnp.concatenate([decay[last:], drive[last:]], axis=0)
    ends[...] = jnp.broadcast_to(both[None], ends.shape)


def project(
    place, mine, theirs, weights, taps, w_recur, w_admit, rate, scale, blocks, fs_count, rows
):
    channels = scale.shape[1]
    block = jax.ShapeDtypeStruct(scale.shape, jnp.float32)
    return pl.pallas_call(
        functools.partial(project_kernel, fs_count=fs_count, member_rows=rows),
        out_shape=(
            jax.ShapeDtypeStruct((channels, scale.shape[0]), jnp.bfloat16),
            block,
            block,
            block,
            jax.ShapeDtypeStruct((blocks, 2, channels), jnp.float32),
        ),
        in_specs=[smem()] + [vmem()] * 10,
        out_specs=(vmem(),) * 5,
        cost_estimate=pl.CostEstimate(
            flops=2 * scale.shape[0] * mine.shape[1] * 3 * channels,
            bytes_accessed=4 << 20,
            transcendentals=1 << 18,
        ),
        name="project",
    )(place, mine, theirs, *weights, taps, w_recur, w_admit, rate, scale)


def states_kernel(
    place, pieces, start, decays, states, gates, mine, theirs, *, y_count, fs_count, member_rows
):
    here, core = (place[0] * y_count + place[1], place[3])

    count = pieces.shape[0]
    decay, state = (pieces[:, 0, :], pieces[:, 1, :])
    row = lax.broadcasted_iota(jnp.int32, decay.shape, 0)
    decay = jnp.where(row < here, decay, 1.0)
    state = jnp.where(row < here, state, 0.0)
    by = 1
    while by < count:
        inside = row >= by
        decay_before = jnp.where(inside, pltpu.roll(decay, by, 0), 1.0)
        state_before = jnp.where(inside, pltpu.roll(state, by, 0), 0.0)
        state = decay * state_before + state
        decay = decay * decay_before
        by *= 2
    entering = decay[count - 1 :] * start[...] + state[count - 1 :]
    out = ((states[...] + decays[...] * entering) * gates[...]).astype(jnp.bfloat16)
    for f in range(fs_count):
        at = 2 * f * member_rows
        even = out[at : at + member_rows]
        odd = out[at + member_rows : at + 2 * member_rows]
        mine[f * member_rows : (f + 1) * member_rows] = jnp.where(core == 0, even, odd)
        theirs[f * member_rows : (f + 1) * member_rows] = jnp.where(core == 0, odd, even)


def final_states(place, pieces, start, decays, states, gates, y_count, fs_count, member_rows):
    half = jax.ShapeDtypeStruct((fs_count * member_rows, decays.shape[1]), jnp.bfloat16)
    return pl.pallas_call(
        functools.partial(
            states_kernel, y_count=y_count, fs_count=fs_count, member_rows=member_rows
        ),
        out_shape=(half, half),
        in_specs=[smem()] + [vmem()] * 5,
        out_specs=(vmem(), vmem()),
        cost_estimate=pl.CostEstimate(
            flops=1 << 20, bytes_accessed=1 << 19, transcendentals=0
        ),
        name="final_states",
    )(place, pieces, start, decays, states, gates)


def attention_kernel(
    place, group, kv_far, *refs, block_rows, part_rows, start, stop
):
    packed, query, peak, values, value_t, kv, arrivals = refs[-10:-3]
    plain, held = (refs[-3], refs[-2:])
    heads = stop - start
    _, size, rows = group.shape
    z_count, chunk_keys, _ = kv.shape
    z, y, member = (place[0], place[1], place[2])

    def arrival(at):
        return pltpu.make_async_copy(kv_far.at[at], kv.at[at], arrivals.at[at])

    queries = pltpu.make_async_copy(group.at[pl.ds(start, heads)], plain, arrivals.at[z_count])
    queries.start()
    arrival(z).start()

    def begin(at, _):
        arrival(at).start()
        return 0

    lax.fori_loop(0, z, begin, 0)
    peak[...] = jnp.full(peak.shape, far_below, jnp.float32)
    value_t[size:, :] = jnp.ones((16, chunk_keys), jnp.bfloat16)
    values[...] = jnp.zeros(values.shape, jnp.float32)

    def visible_keys():
        row = lax.broadcasted_iota(jnp.int32, (chunk_keys, rows), 0)
        lane = lax.broadcasted_iota(jnp.int32, (chunk_keys, rows), 1)
        key_pos = (row // part_rows) * block_rows + member * part_rows + row % part_rows
        half, piece = (rows // 2, part_rows // 2)
        inside = (lane % half) // piece * part_rows + lane // half * piece + lane % piece
        return key_pos <= inside + y * block_rows

    def one_chunk(at, masked):
        arrival(at).wait()
        both = kv[at]
        keys = both[:, :size]
        value_t[:size, :] = both[:, size:].T
        visible = visible_keys() if masked else None

        def scores_of(i):
            found = jnp.dot(keys, query[i], preferred_element_type=jnp.float32)
            return jnp.where(visible, found, far_below) if masked else found

        held[0][...] = scores_of(0)
        for i in range(2 * heads):
            if i + 1 < 2 * heads:
                held[(i + 1) % 2][...] = scores_of(i + 1)
            scores = held[i % 2][...]
            old = peak[i]
            now = jnp.maximum(old, jnp.max(scores, axis=0, keepdims=True))
            expos = jnp.exp2(scores - now)
            if masked:
                expos = jnp.where(visible, expos, 0.0)
            fade = jnp.exp2(old - now)
            peak[i] = now
            values[i] = values[i] * fade + jnp.dot(
                value_t[...], expos.astype(jnp.bfloat16), preferred_element_type=jnp.float32
            )

    queries.wait()
    line = lax.broadcasted_iota(jnp.int32, (size, rows), 0)
    for h in range(heads):
        whole = plain[h]
        zero = jnp.zeros_like(whole)
        query[2 * h] = jnp.where(line < size // 2, whole, zero)
        query[2 * h + 1] = jnp.where(line < size // 2, zero, whole)
    one_chunk(z, True)

    def earlier(at, _):
        one_chunk(at, False)
        return 0

    lax.fori_loop(0, z, earlier, 0)

    if start:
        packed[:start] = refs[0][...]
    half = rows // 2
    line = lax.broadcasted_iota(jnp.int32, (16, rows), 0)
    for h in range(heads):
        tail = jnp.zeros((16, rows), jnp.float32)
        for m in range(2):
            amount = values[2 * h + m, size : size + 1, :]
            some = amount > 0.0
            safe = jnp.where(some, amount, 1.0)
            shares = (values[2 * h + m, :size, :] * jnp.where(some, 1.0 / safe, 0.0)).astype(jnp.bfloat16)
            level = jnp.where(some, peak[2 * h + m] + jnp.log2(safe), far_below)
            coarse = level.astype(jnp.bfloat16).astype(jnp.float32)
            tail = jnp.where(line == 2 * m, coarse, tail)
            tail = jnp.where(line == 2 * m + 1, level - coarse, tail)
            for t in range(2):
                packed[start + h, t, m * size : (m + 1) * size, :] = shares[:, t * half : (t + 1) * half]
        rounded = tail.astype(jnp.bfloat16)
        for t in range(2):
            packed[start + h, t, 2 * size : 2 * size + 16, :] = rounded[:, t * half : (t + 1) * half]


def attention(place, group, kv, earlier, stop, block_rows, part_rows):
    start = 0 if earlier is None else earlier.shape[0]
    heads = stop - start
    _, size, rows = group.shape
    z_count, chunk_keys, _ = kv.shape
    keys = chunk_keys * z_count
    return pl.pallas_call(
        functools.partial(
            attention_kernel, block_rows=block_rows, part_rows=part_rows, start=start, stop=stop
        ),
        out_shape=jax.ShapeDtypeStruct((stop, 2, 2 * size + 16, rows // 2), jnp.bfloat16),
        in_specs=[smem(), anywhere(), anywhere()] + [vmem()] * (start > 0),
        out_specs=vmem(),
        scratch_shapes=[
            pltpu.VMEM((2 * heads, size, rows), jnp.bfloat16),
            pltpu.VMEM((2 * heads, 1, rows), jnp.float32),
            pltpu.VMEM((2 * heads, size + 16, rows), jnp.float32),
            pltpu.VMEM((size + 16, chunk_keys), jnp.bfloat16),
            pltpu.VMEM(kv.shape, kv.dtype),
            pltpu.SemaphoreType.DMA((z_count + 1,)),
            pltpu.VMEM((heads, size, rows), jnp.bfloat16),
            pltpu.VMEM((chunk_keys, rows), jnp.float32),
            pltpu.VMEM((chunk_keys, rows), jnp.float32),
        ],
        cost_estimate=pl.CostEstimate(
            flops=4 * 2 * heads * rows * keys * size,
            bytes_accessed=4 << 20,
            transcendentals=2 * heads * rows * keys,
        ),
        name="attention",
    )(place, group, kv, *(() if earlier is None else (earlier,)))


def finish_kernel(place, lam, lam_theirs, parts, gain, lru_mine, lru_theirs, w_mine, w_theirs, out):
    count, _, lines, _ = parts.shape
    size = (lines - 16) // 2
    core = place[3]

    def head_output(owner, factor):
        joined = []
        for m in range(2):
            tails = [parts[i, owner, 2 * size :, :].astype(jnp.float32) for i in range(count)]
            levels = [t[2 * m : 2 * m + 1] + t[2 * m + 1 : 2 * m + 2] for t in tails]
            top = functools.reduce(jnp.maximum, levels)
            shares = [jnp.exp2(level - top) for level in levels]
            inverse = 1.0 / functools.reduce(jnp.add, shares)
            weighted = [
                parts[i, owner, m * size : (m + 1) * size, :].astype(jnp.float32)
                * (shares[i] * inverse)
                for i in range(count)
            ]
            joined.append(functools.reduce(jnp.add, weighted))
        diff = joined[0] - factor * joined[1]
        level = lax.rsqrt(jnp.mean(diff * diff, axis=0, keepdims=True) + head_eps)
        return ((diff * level).T * gain[...]).astype(jnp.bfloat16)

    mine = jnp.concatenate([lru_mine[...], head_output(core, lam[0])], axis=1)
    theirs = jnp.concatenate([lru_theirs[...], head_output(1 - core, lam_theirs[0])], axis=1)
    result = jnp.dot(mine, w_mine[...], preferred_element_type=jnp.float32)
    result = result + jnp.dot(theirs, w_theirs[...], preferred_element_type=jnp.float32)
    out[...] = result.astype(jnp.bfloat16)


def finish(place, lam, lam_theirs, parts, gain, lru_mine, lru_theirs, w_mine, w_theirs):
    rows, wide = (lru_mine.shape[0], w_mine.shape[1])
    return pl.pallas_call(
        finish_kernel,
        out_shape=jax.ShapeDtypeStruct((rows, wide), jnp.bfloat16),
        in_specs=[smem()] * 3 + [vmem()] * 6,
        out_specs=vmem(),
        cost_estimate=pl.CostEstimate(
            flops=2 * rows * wide * 512, bytes_accessed=3 << 20, transcendentals=rows * 16
        ),
        name="finish",
    )(place, lam, lam_theirs, parts, gain, lru_mine, lru_theirs, w_mine, w_theirs)


def body(
    tokens,
    norm_gain,
    query_weight,
    w_key,
    w_value,
    w_input,
    w_gate,
    conv_kernel,
    w_recur,
    w_admit,
    decay_param,
    decay_scale,
    init_state,
    diff_lambda,
    head_gain,
    w_out_lru,
    w_out_attn,
):
    member_rows, wide = tokens.shape
    fs_count = lax.axis_size("fs")
    tp_count = lax.axis_size("tp")
    row_count = member_rows * fs_count * tp_count
    share_rows = member_rows * tp_count
    member = lax.axis_index("fs")
    core = lax.axis_index("tp")
    z_count, z = (lax.axis_size("sp_0"), lax.axis_index("sp_0"))
    y_count, y = (lax.axis_size("sp_1"), lax.axis_index("sp_1"))

    normed, last_rows = normalized(tokens, norm_gain[None], 8)

    before_rows = passed_along(last_rows, SP, 1)

    chip_rows = lax.all_gather(normed, "tp", axis=0, tiled=True)
    kv_here = jnp.concatenate(
        [
            jnp.dot(chip_rows, weight, preferred_element_type=jnp.float32).astype(jnp.bfloat16)
            for weight in (w_key, w_value)
        ],
        axis=1,
    )
    kv_here, normed = lax.optimization_barrier((kv_here, normed))
    everyone = from_everyone(kv_here, SP)
    everyone = everyone.reshape(z_count, y_count * share_rows, kv_here.shape[1])

    sent = jnp.concatenate([normed, before_rows], axis=0)
    mine = lax.all_gather(sent, "fs", axis=0, tiled=True)
    swap = [(0, 1), (1, 0)]
    theirs = lax.ppermute(mine, "tp", swap)

    place = jnp.stack([z, y, member, core]).astype(jnp.int32)
    rate = gate_scale * jax.nn.softplus(-decay_param)
    query_t, decays, states, gates, ends = project(
        place,
        mine,
        theirs,
        (query_weight, w_input, w_gate),
        conv_kernel,
        w_recur,
        w_admit,
        rate[None],
        decay_scale,
        z_count * y_count,
        fs_count,
        member_rows,
    )

    group = lax.all_gather(query_t, "fs")

    w_mine = jnp.concatenate([w_out_lru, w_out_attn], axis=0)
    w_theirs = lax.ppermute(w_mine, "tp", swap)
    lam_theirs = lax.ppermute(diff_lambda, "tp", swap)

    everywhere = lax.all_to_all(ends, SP, split_axis=0, concat_axis=0, tiled=True)

    carried = attention(place, group, everyone, None, fs_count, row_count, share_rows)
    lines, half_rows = carried.shape[2:]
    carried = carried.reshape(fs_count * tp_count, lines, half_rows)
    packed = lax.all_to_all(carried, ("fs", "tp"), split_axis=0, concat_axis=0, tiled=True)
    packed = packed.reshape(fs_count, tp_count, lines, half_rows)

    lru_mine, lru_other = final_states(
        place, everywhere, init_state[None], decays, states, gates, y_count, fs_count, member_rows
    )
    lru_theirs = lax.ppermute(lru_other, "tp", swap)

    partial = finish(
        place,
        diff_lambda,
        lam_theirs,
        packed,
        head_gain[None],
        lru_mine,
        lru_theirs,
        w_mine,
        w_theirs,
    )
    partial = partial.reshape(fs_count, member_rows, wide)
    arrived = lax.all_to_all(partial, "fs", split_axis=0, concat_axis=0, tiled=True)
    return arrived.astype(jnp.float32).sum(axis=0).astype(jnp.bfloat16)


def solution(mesh):
    torus = Mesh(
        mesh.devices.reshape(8, 8, mesh.shape["fs"], mesh.shape["tp"]), ("sp_0", "sp_1", "fs", "tp")
    )

    return jax.shard_map(
        body,
        mesh=torus,
        in_specs=(
            P(SP_FS_TP, None),
            P(),
            P(None, ("fs", "tp")),
            P(None, "tp"),
            P(None, "tp"),
            P(None, ("fs", "tp")),
            P(None, ("fs", "tp")),
            P(None, ("fs", "tp")),
            P(("fs", "tp"), None, None),
            P(("fs", "tp"), None, None),
            P(("fs", "tp")),
            P(SP, ("fs", "tp")),
            P(("fs", "tp")),
            P(("fs", "tp")),
            P(),
            P(("fs", "tp"), None),
            P(("fs", "tp"), None),
        ),
        out_specs=P(SP_FS_TP, None),
        check_vma=False,
    )
```

```python
import functools

import jax
import jax.numpy as jnp
from jax import lax
from jax.experimental import pallas as pl
from jax.experimental.pallas import tpu as pltpu
from jax.sharding import Mesh
from jax.sharding import PartitionSpec as P


SP = ("sp_0", "sp_1")
SP_FS_TP = ("sp_0", "sp_1", "fs", "tp")


gate_scale = 8.0
input_eps = 1e-06
head_eps = 1e-05
far_below = -1e30
log2_e = 1.4426950408889634


def from_everyone(value, axis):
    copies = jnp.broadcast_to(value, (lax.axis_size(axis), *value.shape))
    return lax.all_to_all(copies, axis, split_axis=0, concat_axis=0, tiled=True)


def passed_along(value, axis, by):
    devices = lax.axis_size(axis)
    pairs = [(i, i + by) for i in range(devices) if 0 <= i + by < devices]
    return lax.ppermute(value, axis, pairs)


def vmem():
    return pl.BlockSpec(memory_space=pltpu.VMEM)


def anywhere():
    return pl.BlockSpec(memory_space=pl.ANY)


def smem():
    return pl.BlockSpec(memory_space=pltpu.SMEM)


def norm_kernel(tokens, gain, out, last):
    floats = tokens[...].astype(jnp.float32)
    level = lax.rsqrt(jnp.mean(floats * floats, axis=1, keepdims=True) + input_eps)
    out[...] = (floats * level * gain[...]).astype(jnp.bfloat16)
    last[...] = out[out.shape[0] - last.shape[0] :, :]


def normalized(tokens, gain, margin):
    return pl.pallas_call(
        norm_kernel,
        out_shape=(
            jax.ShapeDtypeStruct(tokens.shape, jnp.bfloat16),
            jax.ShapeDtypeStruct((margin, tokens.shape[1]), jnp.bfloat16),
        ),
        in_specs=[vmem(), vmem()],
        out_specs=(vmem(), vmem()),
        cost_estimate=pl.CostEstimate(
            flops=4 * tokens.size, bytes_accessed=1 << 18, transcendentals=0
        ),
        name="normalized",
    )(tokens, gain)


def one_minus_exp(x):
    series = jnp.full_like(x, 1.0)
    for k in range(7, 1, -1):
        series = 1.0 - series * x * (1.0 / k)
    return jnp.where(x < 0.35, x * series, 1.0 - jnp.exp(-x))


def project_kernel(
    place, mine, theirs, w_query, w_input, w_gate, taps, w_recur, w_admit, rate, scale,
    query_t, decays, states, gates, ends, *, fs_count, member_rows,
):
    core = place[3]
    sent_rows = mine.shape[0] // fs_count
    first = jnp.where(core == 0, mine[...], theirs[...])
    second = jnp.where(core == 0, theirs[...], mine[...])
    rows = jnp.concatenate([first, second], axis=0)

    def project(weight):
        return jnp.dot(rows, weight[...], preferred_element_type=jnp.float32)

    def piece(value, t, f):
        at = (t * fs_count + f) * sent_rows
        return value[at : at + member_rows]

    def in_order(value):
        pieces = [piece(value, t, f) for f in range(fs_count) for t in range(2)]
        return jnp.concatenate(pieces, axis=0)

    query = project(w_query)
    query = jnp.concatenate([piece(query, t, f) for t in range(2) for f in range(fs_count)], axis=0)
    score_scale = (query.shape[1] // 2) ** (-0.5) * log2_e
    query_t[...] = (query * score_scale).astype(jnp.bfloat16).T

    gate = in_order(project(w_gate).astype(jnp.bfloat16)).astype(jnp.float32)
    gates[...] = jax.nn.gelu(gate)

    lru_all = project(w_input).astype(jnp.bfloat16).astype(jnp.float32)
    margin = sent_rows - member_rows
    before = lru_all[2 * fs_count * sent_rows - margin :]
    padded = jnp.concatenate([before, in_order(lru_all)], axis=0)
    count = taps.shape[0]
    conv_sum = padded[margin:] * taps[count - 1 : count, :]
    for back in range(1, count):
        moved = pltpu.roll(padded, back, 0)[margin:]
        conv_sum = conv_sum + moved * taps[count - 1 - back : count - back, :]
    conv_out = conv_sum.astype(jnp.bfloat16)

    def gate_of(weight):
        zero = jnp.zeros(weight.shape[1:], weight.dtype)
        whole = jnp.concatenate(
            [
                jnp.concatenate([weight[0], zero], axis=1),
                jnp.concatenate([zero, weight[1]], axis=1),
            ],
            axis=0,
        )
        return jax.nn.sigmoid(jnp.dot(conv_out, whole, preferred_element_type=jnp.float32))

    log_decay = -gate_of(w_recur) * rate[...] * scale[...]
    decay = jnp.exp(log_decay)
    drive = jnp.sqrt(one_minus_exp(-2.0 * log_decay)) * gate_of(w_admit) * conv_out.astype(jnp.float32)

    row = lax.broadcasted_iota(jnp.int32, decay.shape, 0)
    by = 1
    while by < decay.shape[0]:
        inside = row >= by
        decay_before = jnp.where(inside, pltpu.roll(decay, by, 0), 1.0)
        state_before = jnp.where(inside, pltpu.roll(drive, by, 0), 0.0)
        drive = decay * state_before + drive
        decay = decay * decay_before
        by *= 2
    decays[...] = decay
    states[...] = drive
    last = decay.shape[0] - 1
    both = jnp.concatenate([decay[last:], drive[last:]], axis=0)
    ends[...] = jnp.broadcast_to(both[None], ends.shape)


def project(
    place, mine, theirs, weights, taps, w_recur, w_admit, rate, scale, blocks, fs_count, rows
):
    channels = scale.shape[1]
    block = jax.ShapeDtypeStruct(scale.shape, jnp.float32)
    return pl.pallas_call(
        functools.partial(project_kernel, fs_count=fs_count, member_rows=rows),
        out_shape=(
            jax.ShapeDtypeStruct((channels, scale.shape[0]), jnp.bfloat16),
            block,
            block,
            block,
            jax.ShapeDtypeStruct((blocks, 2, channels), jnp.float32),
        ),
        in_specs=[smem()] + [vmem()] * 10,
        out_specs=(vmem(),) * 5,
        cost_estimate=pl.CostEstimate(
            flops=2 * scale.shape[0] * mine.shape[1] * 3 * channels,
            bytes_accessed=4 << 20,
            transcendentals=1 << 18,
        ),
        name="project",
    )(place, mine, theirs, *weights, taps, w_recur, w_admit, rate, scale)


def states_kernel(
    place, pieces, start, decays, states, gates, mine, theirs, *, y_count, fs_count, member_rows
):
    here, core = (place[0] * y_count + place[1], place[3])

    count = pieces.shape[0]
    decay, state = (pieces[:, 0, :], pieces[:, 1, :])
    row = lax.broadcasted_iota(jnp.int32, decay.shape, 0)
    decay = jnp.where(row < here, decay, 1.0)
    state = jnp.where(row < here, state, 0.0)
    by = 1
    while by < count:
        inside = row >= by
        decay_before = jnp.where(inside, pltpu.roll(decay, by, 0), 1.0)
        state_before = jnp.where(inside, pltpu.roll(state, by, 0), 0.0)
        state = decay * state_before + state
        decay = decay * decay_before
        by *= 2
    entering = decay[count - 1 :] * start[...] + state[count - 1 :]
    out = ((states[...] + decays[...] * entering) * gates[...]).astype(jnp.bfloat16)
    for f in range(fs_count):
        at = 2 * f * member_rows
        even = out[at : at + member_rows]
        odd = out[at + member_rows : at + 2 * member_rows]
        mine[f * member_rows : (f + 1) * member_rows] = jnp.where(core == 0, even, odd)
        theirs[f * member_rows : (f + 1) * member_rows] = jnp.where(core == 0, odd, even)


def final_states(place, pieces, start, decays, states, gates, y_count, fs_count, member_rows):
    half = jax.ShapeDtypeStruct((fs_count * member_rows, decays.shape[1]), jnp.bfloat16)
    return pl.pallas_call(
        functools.partial(
            states_kernel, y_count=y_count, fs_count=fs_count, member_rows=member_rows
        ),
        out_shape=(half, half),
        in_specs=[smem()] + [vmem()] * 5,
        out_specs=(vmem(), vmem()),
        cost_estimate=pl.CostEstimate(
            flops=1 << 20, bytes_accessed=1 << 19, transcendentals=0
        ),
        name="final_states",
    )(place, pieces, start, decays, states, gates)


def attention_kernel(
    place, group, kv_far, *refs, block_rows, part_rows, start, stop
):
    packed, query, peak, values, value_t, kv, arrivals = refs[-9:-2]
    held = refs[-2:]
    heads = stop - start
    _, size, rows = group.shape
    chunk_keys = kv.shape[1]
    z, y, member = (place[0], place[1], place[2])

    def arrival(at):
        return pltpu.make_async_copy(kv_far.at[at], kv.at[at], arrivals.at[at])

    arrival(z).start()

    def begin(at, _):
        arrival(at).start()
        return 0

    lax.fori_loop(0, z, begin, 0)
    line = lax.broadcasted_iota(jnp.int32, (size, rows), 0)
    for h in range(heads):
        whole = group[start + h]
        zero = jnp.zeros_like(whole)
        query[2 * h] = jnp.where(line < size // 2, whole, zero)
        query[2 * h + 1] = jnp.where(line < size // 2, zero, whole)
    peak[...] = jnp.full(peak.shape, far_below, jnp.float32)
    value_t[size:, :] = jnp.ones((16, chunk_keys), jnp.bfloat16)
    values[...] = jnp.zeros(values.shape, jnp.float32)

    def visible_keys():
        row = lax.broadcasted_iota(jnp.int32, (chunk_keys, rows), 0)
        lane = lax.broadcasted_iota(jnp.int32, (chunk_keys, rows), 1)
        key_pos = (row // part_rows) * block_rows + member * part_rows + row % part_rows
        half, piece = (rows // 2, part_rows // 2)
        inside = (lane % half) // piece * part_rows + lane // half * piece + lane % piece
        return key_pos <= inside + y * block_rows

    def one_chunk(at, masked):
        arrival(at).wait()
        both = kv[at]
        keys = both[:, :size]
        value_t[:size, :] = both[:, size:].T
        visible = visible_keys() if masked else None

        def scores_of(i):
            found = jnp.dot(keys, query[i], preferred_element_type=jnp.float32)
            return jnp.where(visible, found, far_below) if masked else found

        held[0][...] = scores_of(0)
        for i in range(2 * heads):
            if i + 1 < 2 * heads:
                held[(i + 1) % 2][...] = scores_of(i + 1)
            scores = held[i % 2][...]
            old = peak[i]
            now = jnp.maximum(old, jnp.max(scores, axis=0, keepdims=True))
            expos = jnp.exp2(scores - now)
            if masked:
                expos = jnp.where(visible, expos, 0.0)
            fade = jnp.exp2(old - now)
            peak[i] = now
            values[i] = values[i] * fade + jnp.dot(
                value_t[...], expos.astype(jnp.bfloat16), preferred_element_type=jnp.float32
            )

    one_chunk(z, True)

    def earlier(at, _):
        one_chunk(at, False)
        return 0

    lax.fori_loop(0, z, earlier, 0)

    if start:
        packed[:start] = refs[0][...]
    half = rows // 2
    line = lax.broadcasted_iota(jnp.int32, (16, rows), 0)
    for h in range(heads):
        tail = jnp.zeros((16, rows), jnp.float32)
        for m in range(2):
            amount = values[2 * h + m, size : size + 1, :]
            some = amount > 0.0
            safe = jnp.where(some, amount, 1.0)
            shares = (values[2 * h + m, :size, :] * jnp.where(some, 1.0 / safe, 0.0)).astype(jnp.bfloat16)
            level = jnp.where(some, peak[2 * h + m] + jnp.log2(safe), far_below)
            coarse = level.astype(jnp.bfloat16).astype(jnp.float32)
            tail = jnp.where(line == 2 * m, coarse, tail)
            tail = jnp.where(line == 2 * m + 1, level - coarse, tail)
            for t in range(2):
                packed[start + h, t, m * size : (m + 1) * size, :] = shares[:, t * half : (t + 1) * half]
        rounded = tail.astype(jnp.bfloat16)
        for t in range(2):
            packed[start + h, t, 2 * size : 2 * size + 16, :] = rounded[:, t * half : (t + 1) * half]


def attention(place, group, kv, earlier, stop, block_rows, part_rows):
    start = 0 if earlier is None else earlier.shape[0]
    heads = stop - start
    _, size, rows = group.shape
    z_count, chunk_keys, _ = kv.shape
    keys = chunk_keys * z_count
    return pl.pallas_call(
        functools.partial(
            attention_kernel, block_rows=block_rows, part_rows=part_rows, start=start, stop=stop
        ),
        out_shape=jax.ShapeDtypeStruct((stop, 2, 2 * size + 16, rows // 2), jnp.bfloat16),
        in_specs=[smem(), vmem(), anywhere()] + [vmem()] * (start > 0),
        out_specs=vmem(),
        scratch_shapes=[
            pltpu.VMEM((2 * heads, size, rows), jnp.bfloat16),
            pltpu.VMEM((2 * heads, 1, rows), jnp.float32),
            pltpu.VMEM((2 * heads, size + 16, rows), jnp.float32),
            pltpu.VMEM((size + 16, chunk_keys), jnp.bfloat16),
            pltpu.VMEM(kv.shape, kv.dtype),
            pltpu.SemaphoreType.DMA((z_count,)),
            pltpu.VMEM((chunk_keys, rows), jnp.float32),
            pltpu.VMEM((chunk_keys, rows), jnp.float32),
        ],
        cost_estimate=pl.CostEstimate(
            flops=4 * 2 * heads * rows * keys * size,
            bytes_accessed=4 << 20,
            transcendentals=2 * heads * rows * keys,
        ),
        name="attention",
    )(place, group, kv, *(() if earlier is None else (earlier,)))


def finish_kernel(place, lam, lam_theirs, parts, gain, lru_mine, lru_theirs, w_mine, w_theirs, out):
    count, _, lines, _ = parts.shape
    size = (lines - 16) // 2
    core = place[3]

    def head_output(owner, factor):
        joined = []
        for m in range(2):
            tails = [parts[i, owner, 2 * size :, :].astype(jnp.float32) for i in range(count)]
            levels = [t[2 * m : 2 * m + 1] + t[2 * m + 1 : 2 * m + 2] for t in tails]
            top = functools.reduce(jnp.maximum, levels)
            shares = [jnp.exp2(level - top) for level in levels]
            inverse = 1.0 / functools.reduce(jnp.add, shares)
            weighted = [
                parts[i, owner, m * size : (m + 1) * size, :].astype(jnp.float32)
                * (shares[i] * inverse)
                for i in range(count)
            ]
            joined.append(functools.reduce(jnp.add, weighted))
        diff = joined[0] - factor * joined[1]
        level = lax.rsqrt(jnp.mean(diff * diff, axis=0, keepdims=True) + head_eps)
        return ((diff * level).T * gain[...]).astype(jnp.bfloat16)

    mine = jnp.concatenate([lru_mine[...], head_output(core, lam[0])], axis=1)
    theirs = jnp.concatenate([lru_theirs[...], head_output(1 - core, lam_theirs[0])], axis=1)
    result = jnp.dot(mine, w_mine[...], preferred_element_type=jnp.float32)
    result = result + jnp.dot(theirs, w_theirs[...], preferred_element_type=jnp.float32)
    out[...] = result.astype(jnp.bfloat16)


def finish(place, lam, lam_theirs, parts, gain, lru_mine, lru_theirs, w_mine, w_theirs):
    rows, wide = (lru_mine.shape[0], w_mine.shape[1])
    return pl.pallas_call(
        finish_kernel,
        out_shape=jax.ShapeDtypeStruct((rows, wide), jnp.bfloat16),
        in_specs=[smem()] * 3 + [vmem()] * 6,
        out_specs=vmem(),
        cost_estimate=pl.CostEstimate(
            flops=2 * rows * wide * 512, bytes_accessed=3 << 20, transcendentals=rows * 16
        ),
        name="finish",
    )(place, lam, lam_theirs, parts, gain, lru_mine, lru_theirs, w_mine, w_theirs)


def body(
    tokens,
    norm_gain,
    query_weight,
    w_key,
    w_value,
    w_input,
    w_gate,
    conv_kernel,
    w_recur,
    w_admit,
    decay_param,
    decay_scale,
    init_state,
    diff_lambda,
    head_gain,
    w_out_lru,
    w_out_attn,
):
    member_rows, wide = tokens.shape
    fs_count = lax.axis_size("fs")
    tp_count = lax.axis_size("tp")
    row_count = member_rows * fs_count * tp_count
    share_rows = member_rows * tp_count
    member = lax.axis_index("fs")
    core = lax.axis_index("tp")
    z_count, z = (lax.axis_size("sp_0"), lax.axis_index("sp_0"))
    y_count, y = (lax.axis_size("sp_1"), lax.axis_index("sp_1"))

    normed, last_rows = normalized(tokens, norm_gain[None], 8)

    before_rows = passed_along(last_rows, SP, 1)

    chip_rows = lax.all_gather(normed, "tp", axis=0, tiled=True)
    kv_here = jnp.concatenate(
        [
            jnp.dot(chip_rows, weight, preferred_element_type=jnp.float32).astype(jnp.bfloat16)
            for weight in (w_key, w_value)
        ],
        axis=1,
    )
    kv_here, normed = lax.optimization_barrier((kv_here, normed))
    everyone = from_everyone(kv_here, SP)
    everyone = everyone.reshape(z_count, y_count * share_rows, kv_here.shape[1])

    sent = jnp.concatenate([normed, before_rows], axis=0)
    mine = lax.all_gather(sent, "fs", axis=0, tiled=True)
    swap = [(0, 1), (1, 0)]
    theirs = lax.ppermute(mine, "tp", swap)

    place = jnp.stack([z, y, member, core]).astype(jnp.int32)
    rate = gate_scale * jax.nn.softplus(-decay_param)
    query_t, decays, states, gates, ends = project(
        place,
        mine,
        theirs,
        (query_weight, w_input, w_gate),
        conv_kernel,
        w_recur,
        w_admit,
        rate[None],
        decay_scale,
        z_count * y_count,
        fs_count,
        member_rows,
    )

    group = lax.all_gather(query_t, "fs")

    w_mine = jnp.concatenate([w_out_lru, w_out_attn], axis=0)
    w_theirs = lax.ppermute(w_mine, "tp", swap)
    lam_theirs = lax.ppermute(diff_lambda, "tp", swap)

    everywhere = lax.all_to_all(ends, SP, split_axis=0, concat_axis=0, tiled=True)

    carried = attention(place, group, everyone, None, fs_count, row_count, share_rows)
    lines, half_rows = carried.shape[2:]
    carried = carried.reshape(fs_count * tp_count, lines, half_rows)
    packed = lax.all_to_all(carried, ("fs", "tp"), split_axis=0, concat_axis=0, tiled=True)
    packed = packed.reshape(fs_count, tp_count, lines, half_rows)

    lru_mine, lru_other = final_states(
        place, everywhere, init_state[None], decays, states, gates, y_count, fs_count, member_rows
    )
    lru_theirs = lax.ppermute(lru_other, "tp", swap)

    partial = finish(
        place,
        diff_lambda,
        lam_theirs,
        packed,
        head_gain[None],
        lru_mine,
        lru_theirs,
        w_mine,
        w_theirs,
    )
    partial = partial.reshape(fs_count, member_rows, wide)
    arrived = lax.all_to_all(partial, "fs", split_axis=0, concat_axis=0, tiled=True)
    return arrived.astype(jnp.float32).sum(axis=0).astype(jnp.bfloat16)


def solution(mesh):
    torus = Mesh(
        mesh.devices.reshape(8, 8, mesh.shape["fs"], mesh.shape["tp"]), ("sp_0", "sp_1", "fs", "tp")
    )

    return jax.shard_map(
        body,
        mesh=torus,
        in_specs=(
            P(SP_FS_TP, None),
            P(),
            P(None, ("fs", "tp")),
            P(None, "tp"),
            P(None, "tp"),
            P(None, ("fs", "tp")),
            P(None, ("fs", "tp")),
            P(None, ("fs", "tp")),
            P(("fs", "tp"), None, None),
            P(("fs", "tp"), None, None),
            P(("fs", "tp")),
            P(SP, ("fs", "tp")),
            P(("fs", "tp")),
            P(("fs", "tp")),
            P(),
            P(("fs", "tp"), None),
            P(("fs", "tp"), None),
        ),
        out_specs=P(SP_FS_TP, None),
        check_vma=False,
    )
```
